32 devices in a mesh: ep: 8 (over z, x), tp: 4 (over y, core).
Axes of the slice: x: 2, y: 2, z: 4, core: 2. Of those that a mesh axis runs over, the one named last changes fastest.
Arguments:
- receptance: bfloat16 [2048, 1024], P('ep', 'tp'), may hold values from -6 to 6
- head_key_input: bfloat16 [2048, 1024], P('ep', 'tp'), may hold values from -12 to 12
- head_value_input: bfloat16 [2048, 1024], P('ep', 'tp'), may hold values from -6 to 6
- decay_input_part: bfloat16 [2048, 1024], P('ep', 'tp'), may hold values from -4 to 4
- learning_rate_input: bfloat16 [2048, 1024], P('ep', 'tp'), may hold values from -7 to 1
- output_gate_input: bfloat16 [2048, 1024], P('ep', 'tp'), may hold values from -6 to 6
- decay_channel_offset: float32 [1024], P('tp'), may hold values from -12.5 to -2
- spike_log_decay: float32 [2048, 1024], P('ep', 'tp'), may hold values from -0.7 to 0
- head_norm_gain: float32 [1024], P('tp'), may hold values from 0.1 to 1.9
- head_output_weight: bfloat16 [1024, 2048], P('tp'), may hold values from -0.25 to 0.25
- projection_norm_gain: float32 [2048], replicated, may hold values from 0.1 to 1.9
- expert_input_rows: bfloat16 [1024, 2048], P('ep'), may hold values from -6 to 6
- expert_norm_gain: float32 [2048], replicated, may hold values from 0.1 to 1.9
- selected_expert_index: int32 [1024, 2], P('ep'), may hold values from 0 to 15, all different within a row; in each aligned block of 128 rows (0 to 127, 128 to 255, ...) at most 32 rows name the same one
- selected_expert_weight: float32 [1024, 2], P('ep'), may hold values from 0.3 to 1.5
- routed_gate_weight: bfloat16 [32, 2048, 256], P(('ep', 'tp')), may hold values from -0.125 to 0.125
- routed_up_weight: bfloat16 [32, 2048, 256], P(('ep', 'tp')), may hold values from -0.125 to 0.125
- routed_down_weight: bfloat16 [32, 256, 2048], P(('ep', 'tp')), may hold values from -0.25 to 0.25
- common_gate_weight: bfloat16 [2048, 1024], P(None, 'tp'), may hold values from -0.125 to 0.125
- common_up_weight: bfloat16 [2048, 1024], P(None, 'tp'), may hold values from -0.125 to 0.125
- common_down_weight: bfloat16 [1024, 2048], P('tp'), may hold values from -0.25 to 0.25
Outputs:
- attention_output: bfloat16 [2048, 2048], P(('ep', 'tp'))
- expert_output: bfloat16 [1024, 2048], P('ep', 'tp')
The draws below stay inside these ranges and needn't reach their ends.
Inputs may be any that keep to these rules, and one draw needn't show every extreme that they name: `selected_expert_index`: each row names 2 different experts. Among the rows of one index of ep (aligned blocks of 128 rows) no expert is named by more than 32 rows, a bound that some block reaches.
All inputs are finite; a program needn't handle non-finite values.
Results may differ from the reference program's by a relative error of at most 0.023.
Values may be sent and summed in bfloat16 or wider, within the bound.
A program may use at most 128 MiB of HBM per device.

```python
import math
import jax
import jax.numpy as jnp
import numpy as np
from jax import lax

D = 2048
HEADS = 16
HEAD_CHANNELS = 64
FF = 512
SHARED_FF = 1024
TOPK = 2
TOK_A = 256
TOK_B = 128
WIDTH = 1024
EXPERTS = 16
CAP = 32
TOKENS_A = 2048
TOKENS_B = 1024
N_EP = 8
N_TP = 4


def draw_decay_channel_offset(key, part):
    head_key, fast_key, slow_key = jax.random.split(jax.random.fold_in(key, 11), 3)
    fast_share = 0.5
    fast_heads = jax.random.uniform(head_key, (HEADS,), jnp.float32) < fast_share
    fast_values = jax.random.uniform(fast_key, (WIDTH,), jnp.float32, minval=-3.0, maxval=-2.0)
    slow_values = jax.random.uniform(slow_key, (WIDTH,), jnp.float32, minval=-12.5, maxval=-11.0)
    fast_channels = jnp.repeat(fast_heads, HEAD_CHANNELS)
    return jnp.where(fast_channels, fast_values, slow_values).astype(jnp.float32)


def draw_spike_log_decay(key, part):
    spot_key, depth_key = jax.random.split(jax.random.fold_in(key, 23))
    struck = jax.random.uniform(spot_key, (TOKENS_A, HEADS), jnp.float32) < 3.0 / TOKENS_A
    depth = jax.random.uniform(depth_key, (TOKENS_A, HEADS), jnp.float32, minval=-0.7, maxval=-0.22)
    per_head = jnp.where(struck, depth, jnp.zeros_like(depth))
    return jnp.repeat(per_head, HEAD_CHANNELS, axis=1).astype(jnp.float32)


def draw_decay_input_part(key, part):
    noise_key, offset_key = jax.random.split(jax.random.fold_in(key, 37))
    groups = TOKENS_A // TOK_A
    noise = jax.random.normal(noise_key, (groups, TOK_A, WIDTH), jnp.float32) * 0.7
    offset = jax.random.uniform(offset_key, (groups, 1, 1), jnp.float32, minval=-0.8, maxval=0.8)
    values = jnp.clip(noise + offset, -4.0, 4.0).reshape(TOKENS_A, WIDTH)
    return values.astype(jnp.bfloat16)


def draw_head_key_input(key, part):
    common_key, noise_key = jax.random.split(jax.random.fold_in(key, 41))
    common = jnp.clip(jax.random.normal(common_key, (WIDTH,), jnp.float32), -2.7, 2.7) * 3.0
    noise = jnp.clip(jax.random.normal(noise_key, (TOKENS_A, WIDTH), jnp.float32), -3.5, 3.5)
    values = jnp.clip(common[None, :] + noise, -12.0, 12.0)
    return values.astype(jnp.bfloat16)


def draw_learning_rate_input(key, part):
    rate_key = jax.random.fold_in(key, 53)
    values = jax.random.normal(rate_key, (TOKENS_A, WIDTH), jnp.float32) - 3.0
    return jnp.clip(values, -7.0, 1.0).astype(jnp.bfloat16)


def strengthened(drawn, key, source, target, blocks, factor):
    owner, partner = [(jnp.arange(drawn.shape[position]) // (drawn.shape[position] // blocks)).reshape([-1 if axis == position else 1 for axis in range(drawn.ndim)]) for position in (source, target)]
    chosen = jax.random.permutation(key, blocks)[partner]
    strong = (owner == chosen) | (owner == (partner + blocks // 2) % blocks)
    return jnp.where(strong, factor * drawn, drawn)


def steps_of(stream_key, dims, cuts, least, top_value):
    def one(position, blocks):
        draws = jax.random.uniform(jax.random.fold_in(jax.random.fold_in(stream_key, 6), position), (blocks,), jnp.float32, least / len(cuts), top_value / len(cuts))
        return jnp.repeat(jnp.exp(draws), dims[position] // blocks).reshape((-1,) + (1,) * (len(dims) - position - 1))

    level = one(*cuts[0])
    for cut in cuts[1:]:
        level = level * one(*cut)
    return level


def assign_block(own_key, own, number, rows, number_of, top, reach, slope):
    order = jax.random.permutation(own_key, number_of)
    heavy_load, usual = portions_of(number_of, rows * top, reach, slope, True), portions_of(number_of, rows * top, reach, slope, False)
    places = jnp.arange(number_of)

    def named(tallies, offset_by):
        used = int((tallies > 0).sum())
        fixed = max(1, used // 4)
        moved = fixed + (places - fixed + offset_by * (used - fixed)) % max(1, number_of - fixed)
        return jnp.zeros((number_of,), jnp.int32).at[order[jnp.where(places < fixed, places, moved)]].set(jnp.asarray(tallies, jnp.int32))

    tallies = jnp.where(number % 4 == 0, named(heavy_load, number // 4), named(usual, number - number // 4 - 1))
    mixed = jax.random.permutation(jax.random.fold_in(own, 3), number_of)
    source_of, sink = mixed[0:number_of // 2 * 2:2], mixed[1:number_of // 2 * 2:2]
    room = jnp.minimum(tallies[source_of] - 1, reach - tallies[sink]) // 2
    room = jnp.where((source_of == order[0]) | (sink == order[0]) | (tallies[sink] == 0), 0, jnp.maximum(room, 0))
    moved = jax.random.randint(jax.random.fold_in(own, 4), (number_of // 2,), 0, 1 << 20) % (room + 1)
    tallies = tallies.at[source_of].add(-moved).at[sink].add(moved)
    labels = jnp.searchsorted(jnp.cumsum(tallies), jnp.arange(rows * top), side="right").astype(jnp.int32)
    listing = labels.reshape(top, rows).T
    listing = listing[jax.random.permutation(jax.random.fold_in(own, 1), rows)]
    offset_by = jax.random.randint(jax.random.fold_in(own, 2), (rows, 1), 0, top)
    return jnp.take_along_axis(listing, (jnp.arange(top)[None, :] + offset_by) % top, axis=1)


def portions_of(amount, total, limit, lean, full):
    weights = [(1 << 20) // math.isqrt(standing ** lean) + 1 for standing in range(1, amount + 1)]
    largest = limit if full else min(limit, max(-(-total // amount), total * weights[0] // sum(weights)))
    least = 1 if total - largest >= amount - 1 else 0
    holding, spare = [largest] + [least] * (amount - 1), total - largest - least * (amount - 1)
    while spare > 0:
        movable = [i for i in range(1, amount) if holding[i] < largest] or [i for i in range(1, amount) if holding[i] < limit]
        mass, left = sum([weights[i] for i in movable]), spare
        for i in movable:
            addition = min(limit - holding[i], max(1, left * weights[i] // mass), spare)
            holding[i] = holding[i] + addition
            spare = spare - addition
    return np.array(holding)


def scatter_about(own_key, shape, scale, reach, cuts=(), held_as=jnp.bfloat16):
    array = scale * jax.random.normal(own_key, shape, jnp.float32)
    if cuts:
        array = array * steps_of(own_key, shape, cuts, -0.22, 0.18)
    return jnp.clip(array, -reach, reach).astype(held_as)


def noise_with(stream_key, dims, spread, most, pieces, heavy, kind=jnp.bfloat16):
    result = spread * jax.random.normal(stream_key, dims, jnp.float32)
    if pieces:
        result = result * steps_of(stream_key, dims, pieces, -0.22, 0.18)
    return jnp.clip(strengthened(result, jax.random.fold_in(stream_key, 3), *heavy), -most, most).astype(kind)


def setup_inputs(seed: int = 0) -> dict:
    key_of = jax.random.split(jax.random.key(seed), 22)
    receptance = scatter_about(key_of[0], (TOKENS_A, WIDTH), 1.0, 6.0, ((0, 8), (1, 4)))
    head_key_input = draw_head_key_input(jax.random.fold_in(key_of[21], 71), 0)
    head_value_input = scatter_about(key_of[2], (TOKENS_A, WIDTH), 1.0, 6.0, ((0, 8), (1, 4)))
    decay_input_part = draw_decay_input_part(jax.random.fold_in(key_of[21], 71), 0)
    learning_rate_input = draw_learning_rate_input(jax.random.fold_in(key_of[21], 71), 0)
    output_gate_input = scatter_about(key_of[5], (TOKENS_A, WIDTH), 1.5, 6.0, ((0, 8), (1, 4)))
    decay_channel_offset = draw_decay_channel_offset(jax.random.fold_in(key_of[21], 71), 0)
    spike_log_decay = draw_spike_log_decay(jax.random.fold_in(key_of[21], 71), 0)
    head_norm_gain = jnp.clip(1.0 + 0.18 * jax.random.normal(key_of[8], (WIDTH,), jnp.float32), 0.1, 1.9)
    head_output_weight = noise_with(key_of[9], (WIDTH, D), WIDTH ** -0.5, 0.25, ((0, 4),), (0, 1, 4, 2.0))
    projection_norm_gain = jnp.clip(1.0 + 0.18 * jax.random.normal(key_of[10], (D,), jnp.float32), 0.1, 1.9)
    expert_input_rows = scatter_about(key_of[11], (TOKENS_B, D), 1.0, 6.0, ((0, 8),))
    expert_norm_gain = jnp.clip(1.0 + 0.18 * jax.random.normal(key_of[12], (D,), jnp.float32), 0.1, 1.9)
    selected_expert_index_keys = jax.random.split(jax.random.fold_in(key_of[13], 1), TOKENS_B // TOK_B)
    selected_expert_index_turns = jax.random.permutation(jax.random.fold_in(key_of[13], 3), TOKENS_B // TOK_B)
    selected_expert_index = jax.vmap(lambda own, number: assign_block(jax.random.fold_in(key_of[13], 2), own, number, TOK_B, EXPERTS, TOPK, CAP, 1))(selected_expert_index_keys, selected_expert_index_turns).reshape((TOKENS_B, TOPK))
    selected_expert_weight = jnp.clip(0.3 + 1.2 * jax.random.uniform(key_of[14], (TOKENS_B, TOPK), jnp.float32) ** steps_of(key_of[14], (TOKENS_B, TOPK), ((0, 8),), -0.2, 0.2), 0.3, 1.5)
    routed_gate_weight = scatter_about(key_of[15], (2 * EXPERTS, D, FF // 2), D ** -0.5, 0.125, ((0, 32),))
    routed_up_weight = scatter_about(key_of[16], (2 * EXPERTS, D, FF // 2), D ** -0.5, 0.125, ((0, 32),))
    routed_down_weight = scatter_about(key_of[17], (2 * EXPERTS, FF // 2, D), FF ** -0.5, 0.25, ((0, 32),))
    common_gate_weight = scatter_about(key_of[18], (D, SHARED_FF), D ** -0.5, 0.125, ((1, 4),))
    common_up_weight = scatter_about(key_of[19], (D, SHARED_FF), D ** -0.5, 0.125, ((1, 4),))
    common_down_weight = noise_with(key_of[20], (SHARED_FF, D), SHARED_FF ** -0.5, 0.25, ((0, 4),), (0, 1, 4, 2.0))
    return dict(receptance=receptance, head_key_input=head_key_input, head_value_input=head_value_input, decay_input_part=decay_input_part, learning_rate_input=learning_rate_input, output_gate_input=output_gate_input, decay_channel_offset=decay_channel_offset, spike_log_decay=spike_log_decay, head_norm_gain=head_norm_gain, head_output_weight=head_output_weight, projection_norm_gain=projection_norm_gain, expert_input_rows=expert_input_rows, expert_norm_gain=expert_norm_gain, selected_expert_index=selected_expert_index, selected_expert_weight=selected_expert_weight, routed_gate_weight=routed_gate_weight, routed_up_weight=routed_up_weight, routed_down_weight=routed_down_weight, common_gate_weight=common_gate_weight, common_up_weight=common_up_weight, common_down_weight=common_down_weight)


FULL_PRECISION = lax.Precision.HIGHEST
NORM_EPSILON = 1e-06
GROUP_EPSILON = 0.00064

def rms_scale(values, gain):
    values = values.astype(jnp.float32)
    return values * lax.rsqrt(lax.optimization_barrier(jnp.mean(values * values, axis=-1, keepdims=True)) + NORM_EPSILON) * gain.astype(jnp.float32)

def blocked_down(hidden, weight):
    block_width = hidden.shape[1] // N_TP
    summed = jnp.zeros((hidden.shape[0], weight.shape[1]), jnp.float32)
    for block_index in range(N_TP):
        lower = block_index * block_width
        upper = lower + block_width
        partial_value = jnp.dot(hidden[:, lower:upper], weight[lower:upper], preferred_element_type=jnp.float32).astype(jnp.bfloat16)
        partial_value = lax.optimization_barrier(partial_value)
        summed = summed + partial_value.astype(jnp.float32)
    return summed

def attention_mixer(receptance, head_key_input, head_value_input, decay_input_part, learning_rate_input, output_gate_input, decay_channel_offset, spike_log_decay, head_norm_gain, head_output_weight, projection_norm_gain):
    sequence_length, width = receptance.shape
    number_of_heads = width // HEAD_CHANNELS

    def split_heads(values):
        return values.astype(jnp.float32).reshape(sequence_length, number_of_heads, HEAD_CHANNELS)
    recept = split_heads(receptance)
    keys = split_heads(head_key_input)
    values = split_heads(head_value_input)
    learn_rate = jax.nn.sigmoid(split_heads(learning_rate_input))
    decay_preactivation = decay_channel_offset.astype(jnp.float32)[None, :] + jnp.tanh(decay_input_part.astype(jnp.float32))
    decay_factor = jnp.exp(spike_log_decay.astype(jnp.float32) - jnp.exp(-jax.nn.softplus(-decay_preactivation) - 0.5)).reshape(sequence_length, number_of_heads, HEAD_CHANNELS)
    removal = keys * lax.rsqrt(lax.optimization_barrier(jnp.sum(keys * keys, axis=-1, keepdims=True)) + NORM_EPSILON)
    insertion = keys * learn_rate
    scaled_removal = removal * learn_rate

    def advance(state, inputs):
        recept_now, decay_now, insert_now, value_now, removal_now, scaled_now = inputs
        along = jnp.einsum('hvk,hk->hv', state, removal_now, precision=FULL_PRECISION)
        state = state * decay_now[:, None, :] - along[:, :, None] * scaled_now[:, None, :] + value_now[:, :, None] * insert_now[:, None, :]
        return (state, jnp.einsum('hvk,hk->hv', state, recept_now, precision=FULL_PRECISION))
    start = jnp.zeros((number_of_heads, HEAD_CHANNELS, HEAD_CHANNELS), jnp.float32)
    _, head_value = lax.scan(advance, start, (recept, decay_factor, insertion, values, removal, scaled_removal))
    centred = head_value - lax.optimization_barrier(jnp.mean(head_value, axis=-1, keepdims=True))
    normed = centred * lax.rsqrt(lax.optimization_barrier(jnp.mean(centred * centred, axis=-1, keepdims=True)) + GROUP_EPSILON)
    gated = normed.reshape(sequence_length, width) * head_norm_gain.astype(jnp.float32) * jax.nn.sigmoid(output_gate_input.astype(jnp.float32))
    heads_out = gated.astype(jnp.bfloat16)
    mix_sum = blocked_down(heads_out, head_output_weight)
    return rms_scale(mix_sum, projection_norm_gain).astype(jnp.bfloat16)

def expert_half(expert_input_rows, expert_norm_gain, selected_expert_index, selected_expert_weight, routed_gate_weight, routed_up_weight, routed_down_weight, common_gate_weight, common_up_weight, common_down_weight):
    normed = rms_scale(expert_input_rows, expert_norm_gain).astype(jnp.bfloat16)
    shared_hidden = (jax.nn.silu(jnp.dot(normed, common_gate_weight, preferred_element_type=jnp.float32)) * jnp.dot(normed, common_up_weight, preferred_element_type=jnp.float32)).astype(jnp.bfloat16)
    shared_sum = blocked_down(shared_hidden, common_down_weight)
    most_rows = N_EP * CAP

    def per_expert(summed, expert):
        hits = selected_expert_index == expert
        chosen = jnp.any(hits, axis=1)
        weight = lax.optimization_barrier(jnp.sum(jnp.where(hits, selected_expert_weight, jnp.zeros_like(selected_expert_weight)), axis=1))
        order = jnp.argsort(jnp.where(chosen, 0, 1).astype(jnp.int32), stable=True)[:most_rows].astype(jnp.int32)
        picked = normed[order]
        first_half = (2 * expert).astype(jnp.int32)
        gate_pair = lax.dynamic_slice_in_dim(routed_gate_weight, first_half, 2, 0)
        up_pair = lax.dynamic_slice_in_dim(routed_up_weight, first_half, 2, 0)
        down_pair = lax.dynamic_slice_in_dim(routed_down_weight, first_half, 2, 0)
        value = jnp.zeros((most_rows, normed.shape[1]), jnp.float32)
        for half in range(2):
            gate = jnp.dot(picked, gate_pair[half], preferred_element_type=jnp.float32)
            upward = jnp.dot(picked, up_pair[half], preferred_element_type=jnp.float32)
            hidden = (jax.nn.silu(gate) * upward).astype(jnp.bfloat16)
            partial_value = jnp.dot(hidden, down_pair[half], preferred_element_type=jnp.float32).astype(jnp.bfloat16)
            partial_value = lax.optimization_barrier(partial_value)
            value = value + partial_value.astype(jnp.float32)
        value = value.astype(jnp.bfloat16)
        value = lax.optimization_barrier(value)
        summed = summed.at[order].add(weight[order][:, None] * value.astype(jnp.float32))
        return (summed, None)
    start = jnp.zeros((expert_input_rows.shape[0], expert_input_rows.shape[1]), jnp.float32)
    routed, _ = lax.scan(per_expert, start, jnp.arange(EXPERTS, dtype=jnp.int32))
    return (routed + shared_sum).astype(jnp.bfloat16)

def reference(receptance, head_key_input, head_value_input, decay_input_part, learning_rate_input, output_gate_input, decay_channel_offset, spike_log_decay, head_norm_gain, head_output_weight, projection_norm_gain, expert_input_rows, expert_norm_gain, selected_expert_index, selected_expert_weight, routed_gate_weight, routed_up_weight, routed_down_weight, common_gate_weight, common_up_weight, common_down_weight):
    attention_output = attention_mixer(receptance, head_key_input, head_value_input, decay_input_part, learning_rate_input, output_gate_input, decay_channel_offset, spike_log_decay, head_norm_gain, head_output_weight, projection_norm_gain)
    expert_output = expert_half(expert_input_rows, expert_norm_gain, selected_expert_index, selected_expert_weight, routed_gate_weight, routed_up_weight, routed_down_weight, common_gate_weight, common_up_weight, common_down_weight)
    return (attention_output, expert_output)
```

```python
import functools

import jax
import jax.numpy as jnp
from jax import lax
from jax.experimental import pallas as pl
from jax.experimental.pallas import tpu as pltpu
from jax.sharding import PartitionSpec as P

HEAD_CHANNELS = 64
BLOCK = 64


MESH = pl.DeviceIdType.MESH
NORM_EPSILON = 1e-06
GROUP_EPSILON = 0.00064


def rms_scale(values, gain):
    values = values.astype(jnp.float32)
    return (
        values * lax.rsqrt(jnp.mean(values * values, axis=-1, keepdims=True) + NORM_EPSILON) * gain
    )


def split_parts(x):
    high = x.astype(jnp.bfloat16)
    return high, (x - high.astype(jnp.float32)).astype(jnp.bfloat16)


def dot3(x, y, dims):
    xh, xl = split_parts(x)
    yh, yl = split_parts(y)

    def one(p, q):
        return lax.dot_general(p, q, (dims, ((), ())), preferred_element_type=jnp.float32)

    return one(xh, yh) + (one(xh, yl) + one(xl, yh))


NN = ((1,), (0,))
NT = ((1,), (1,))
TN = ((0,), (0,))


def local_kernel(
    r_ref, k_ref, v_ref, dec_ref, lr_ref, off_ref, spike_ref, out_ref, carry_ref, map_ref
):
    rows, width = r_ref.shape
    heads = width // HEAD_CHANNELS
    blocks = rows // BLOCK
    row = lax.broadcasted_iota(jnp.int32, (rows, rows), 0)
    col = lax.broadcasted_iota(jnp.int32, (rows, rows), 1)
    strict = col < row
    inclusive = col <= row
    learn_all = jax.nn.sigmoid(lr_ref[...].astype(jnp.float32))
    pre = off_ref[...] + jnp.tanh(dec_ref[...].astype(jnp.float32))
    log_all = spike_ref[...] - jax.nn.sigmoid(pre) * jnp.exp(jnp.float32(-0.5))
    ones = jnp.where(inclusive, 1.0, 0.0).astype(jnp.bfloat16)
    p0 = log_all.astype(jnp.bfloat16)
    rest = log_all - p0.astype(jnp.float32)
    p1 = rest.astype(jnp.bfloat16)
    p2 = (rest - p1.astype(jnp.float32)).astype(jnp.bfloat16)
    cum_all = sum(jnp.dot(ones, p, preferred_element_type=jnp.float32) for p in (p0, p1, p2))
    before_all = cum_all - log_all
    for h in range(heads):
        lanes = slice(h * HEAD_CHANNELS, (h + 1) * HEAD_CHANNELS)
        r = r_ref[:, lanes].astype(jnp.float32)
        k = k_ref[:, lanes].astype(jnp.float32)
        v = v_ref[:, lanes].astype(jnp.float32)
        learn = learn_all[:, lanes]
        cum = cum_all[:, lanes]
        before = before_all[:, lanes]
        a = k * lax.rsqrt(jnp.sum(k * k, axis=-1, keepdims=True) + NORM_EPSILON)
        b = a * learn
        ins = k * learn
        parts = []
        for i in range(blocks):
            span = slice(i * BLOCK, (i + 1) * BLOCK)
            base = before[i * BLOCK : i * BLOCK + 1]
            left = jnp.concatenate(
                [a[span] * jnp.exp(before[span] - base), r[span] * jnp.exp(cum[span] - base)],
                axis=0,
            )
            back = jnp.exp(jnp.minimum(base - cum, 60.0))
            right = jnp.concatenate([b * back, ins * back], axis=0)
            parts.append(dot3(left, right, NT))
        low_b = jnp.where(strict, jnp.concatenate([p[:BLOCK, :rows] for p in parts], axis=0), 0.0)
        low_k = jnp.where(strict, jnp.concatenate([p[:BLOCK, rows:] for p in parts], axis=0), 0.0)
        out_b = jnp.where(
            inclusive, jnp.concatenate([p[BLOCK:, :rows] for p in parts], axis=0), 0.0
        )
        out_k = jnp.where(
            inclusive, jnp.concatenate([p[BLOCK:, rows:] for p in parts], axis=0), 0.0
        )
        inverse = jnp.where(row == col, 1.0, 0.0)
        size = 1
        while size < BLOCK:
            corner = (row // (2 * size) == col // (2 * size)) & (row // size != col // size)
            corner = jnp.where(corner, low_b, 0.0)
            if size == 1:
                inverse = inverse - corner
            else:
                inverse = inverse - dot3(dot3(inverse, corner, NN), inverse, NN)
            size *= 2
        right_side = jnp.concatenate([a * jnp.exp(before), dot3(low_k, v, NN)], axis=1)
        solved = []
        for i in range(blocks):
            span = slice(i * BLOCK, (i + 1) * BLOCK)
            piece = right_side[span]
            if i:
                piece = piece - dot3(
                    low_b[span, : i * BLOCK], jnp.concatenate(solved, axis=0), NN
                )
            solved.append(dot3(inverse[span, span], piece, NN))
        solved = jnp.concatenate(solved, axis=0)
        removed = dot3(out_b, solved, NN)
        out_ref[:, lanes] = dot3(out_k, v, NN) - removed[:, HEAD_CHANNELS:]
        carry_ref[:, lanes] = r * jnp.exp(cum) - removed[:, :HEAD_CHANNELS]
        last = cum[rows - 1 :]
        to_end = jnp.exp(last - cum)
        taken = dot3(solved, b * to_end, TN)
        added = dot3(v, ins * to_end, TN)
        small = (HEAD_CHANNELS, HEAD_CHANNELS)
        eye = lax.broadcasted_iota(jnp.int32, small, 0) == lax.broadcasted_iota(jnp.int32, small, 1)
        through = jnp.where(eye, jnp.exp(last), 0.0) - taken[:HEAD_CHANNELS]
        fresh = added - taken[HEAD_CHANNELS:]
        map_ref[lanes, :] = jnp.concatenate([through, fresh], axis=1).astype(jnp.bfloat16)


def join_kernel(
    count, out_ref, carry_ref, map_ref, gain_ref, gate_ref, weight_ref, mix_ref, held, state,
    send_sem, recv_sem
):
    me = lax.axis_index("ep")
    rows, width = out_ref.shape
    heads = width // HEAD_CHANNELS
    barrier = pltpu.get_barrier_semaphore()
    for step in range(1, count):
        pl.semaphore_signal(
            barrier, inc=1, device_id={"ep": lax.rem(me + step, count)}, device_id_type=MESH
        )
    pl.semaphore_wait(barrier, count - 1)

    def copy(slot, step):
        return pltpu.make_async_remote_copy(
            src_ref=map_ref,
            dst_ref=held.at[slot],
            send_sem=send_sem.at[step],
            recv_sem=recv_sem.at[slot],
            device_id={"ep": lax.rem(me + step, count)},
            device_id_type=MESH,
        )

    for step in range(1, count):

        @pl.when(me + step < count)
        def _():
            copy(me, step).start()

    state[...] = jnp.zeros_like(state)

    def one(turn, _):
        copy(turn, 1).wait_recv()
        for h in range(heads):
            lanes = slice(h * HEAD_CHANNELS, (h + 1) * HEAD_CHANNELS)
            block = held[turn, lanes, :]
            high, low = split_parts(state[lanes, :])
            through = block[:, :HEAD_CHANNELS]
            state[lanes, :] = (
                jnp.dot(high, through, preferred_element_type=jnp.float32)
                + jnp.dot(low, through, preferred_element_type=jnp.float32)
                + block[:, HEAD_CHANNELS:].astype(jnp.float32)
            )
        return 0

    lax.fori_loop(0, me, one, 0)
    normed = []
    for h in range(heads):
        lanes = slice(h * HEAD_CHANNELS, (h + 1) * HEAD_CHANNELS)
        value = out_ref[:, lanes] + dot3(carry_ref[:, lanes], state[lanes, :], NT)
        centred = value - jnp.mean(value, axis=-1, keepdims=True)
        normed.append(
            centred
            * lax.rsqrt(jnp.mean(centred * centred, axis=-1, keepdims=True) + GROUP_EPSILON)
        )
    flat = normed[0] if heads == 1 else jnp.concatenate(normed, axis=1)
    heads_out = flat * gain_ref[...] * jax.nn.sigmoid(gate_ref[...].astype(jnp.float32))
    mix_ref[...] = jnp.dot(
        heads_out.astype(jnp.bfloat16), weight_ref[...], preferred_element_type=jnp.float32
    ).astype(jnp.bfloat16)
    for step in range(1, count):

        @pl.when(me + step < count)
        def _():
            copy(me, step).wait_send()


def attention_mixer(
    receptance,
    head_key_input,
    head_value_input,
    decay_input_part,
    learning_rate_input,
    output_gate_input,
    decay_channel_offset,
    spike_log_decay,
    head_norm_gain,
    head_output_weight,
    projection_norm_gain,
):
    rows, width = receptance.shape
    count = lax.axis_size("ep")
    full = pl.BlockSpec(memory_space=pltpu.VMEM)
    out, carry, maps = pl.pallas_call(
        local_kernel,
        out_shape=(
            jax.ShapeDtypeStruct((rows, width), jnp.float32),
            jax.ShapeDtypeStruct((rows, width), jnp.float32),
            jax.ShapeDtypeStruct((width, 2 * HEAD_CHANNELS), jnp.bfloat16),
        ),
        in_specs=[full] * 7,
        out_specs=(full, full, full),
        cost_estimate=pl.CostEstimate(
            flops=rows * rows * width * 200, bytes_accessed=rows * width * 22, transcendentals=0
        ),
    )(
        receptance,
        head_key_input,
        head_value_input,
        decay_input_part,
        learning_rate_input,
        decay_channel_offset[None, :],
        spike_log_decay,
    )
    model_width = head_output_weight.shape[1]
    mix = pl.pallas_call(
        functools.partial(join_kernel, count),
        out_shape=jax.ShapeDtypeStruct((rows, model_width), jnp.bfloat16),
        in_specs=[full] * 6,
        out_specs=full,
        scratch_shapes=[
            pltpu.VMEM((count, width, 2 * HEAD_CHANNELS), jnp.bfloat16),
            pltpu.VMEM((width, HEAD_CHANNELS), jnp.float32),
            pltpu.SemaphoreType.DMA((count,)),
            pltpu.SemaphoreType.DMA((count,)),
        ],
        compiler_params=pltpu.CompilerParams(collective_id=0, has_side_effects=True),
        cost_estimate=pl.CostEstimate(
            flops=rows * width * model_width * 20,
            bytes_accessed=width * model_width * 2,
            transcendentals=0,
        ),
    )(out, carry, maps, head_norm_gain[None, :], output_gate_input, head_output_weight)
    mix_sum = lax.psum_scatter(mix, "tp", scatter_dimension=0, tiled=True).astype(jnp.float32)
    return rms_scale(mix_sum, projection_norm_gain).astype(jnp.bfloat16)


def expert_kernel(
    count, pairs, arrived, gate_ref, up_ref, down_ref, result_ref, crossing, halves, paired,
    final, back, half_send, half_recv, pair_send, pair_recv, back_send, back_recv
):
    me = lax.axis_index("ep")
    place = lax.axis_index("tp")
    group = place // 2
    half = place % 2
    capacity = arrived.shape[0] // count
    columns = final.shape[2]
    partner = 2 * group + 1 - half

    def rows_of(index):
        return pl.ds(pl.multiple_of(index * capacity, capacity), capacity)

    def peer(step):
        return lax.rem(me + step, count)

    barrier = pltpu.get_barrier_semaphore()
    for step in range(1, count):
        pl.semaphore_signal(barrier, inc=1, device_id={"ep": peer(step)}, device_id_type=MESH)
    pl.semaphore_signal(barrier, inc=1, device_id={"tp": partner}, device_id_type=MESH)
    for step in range(1, pairs):
        there = 2 * lax.rem(group + step, pairs) + half
        pl.semaphore_signal(barrier, inc=1, device_id={"tp": there}, device_id_type=MESH)
    pl.semaphore_wait(barrier, count + pairs - 1)

    def cross(index):
        return pltpu.make_async_remote_copy(
            src_ref=crossing.at[index],
            dst_ref=halves.at[index],
            send_sem=half_send.at[index],
            recv_sem=half_recv.at[index],
            device_id={"tp": partner},
            device_id_type=MESH,
        )

    def pair(step):
        return pltpu.make_async_remote_copy(
            src_ref=paired.at[step],
            dst_ref=final.at[step],
            send_sem=pair_send.at[step],
            recv_sem=pair_recv.at[step],
            device_id={"tp": 2 * lax.rem(group + step, pairs) + half},
            device_id_type=MESH,
        )

    def home(turn, step):
        return pltpu.make_async_remote_copy(
            src_ref=final.at[turn, rows_of(peer(step))],
            dst_ref=back.at[turn, rows_of(me)],
            send_sem=back_send.at[turn, step],
            recv_sem=back_recv.at[turn, step],
            device_id={"ep": peer(step)},
            device_id_type=MESH,
        )

    rows = arrived[...]
    gate = jnp.dot(rows, gate_ref[0], preferred_element_type=jnp.float32)
    upward = jnp.dot(rows, up_ref[0], preferred_element_type=jnp.float32)
    hidden = (jax.nn.silu(gate) * upward).astype(jnp.bfloat16)

    def part(index):
        span = pl.ds(pl.multiple_of(index * columns, columns), columns)
        return jnp.dot(hidden, down_ref[0, :, span], preferred_element_type=jnp.float32).astype(
            jnp.bfloat16
        )

    order = list(range(1, pairs)) + [0]
    for step in order:
        crossing[step] = part(2 * lax.rem(group + step, pairs) + 1 - half)
        cross(step).start()
    own = {step: part(2 * lax.rem(group + step, pairs) + half) for step in order}
    for step in order:
        cross(step).wait_recv()
        total = (
            own[step].astype(jnp.float32) + halves[step].astype(jnp.float32)
        ).astype(jnp.bfloat16)
        if step:
            paired[step] = total
            pair(step).start()
        else:
            final[0] = total
    for turn in range(pairs):
        if turn:
            pair(turn).wait_recv()
        for step in range(1, count):
            home(turn, step).start()
        back[turn, rows_of(me), :] = final[turn, rows_of(me), :]
    for turn in range(pairs):
        for step in range(1, count):
            home(turn, step).wait_recv()
        result_ref[lax.rem(group + pairs - turn, pairs)] = back[turn]
    for step in order:
        cross(step).wait_send()
        if step:
            pair(step).wait_send()
    for turn in range(pairs):
        for step in range(1, count):
            home(turn, step).wait_send()


def routed_by_kernel(arrived, gate_weight, up_weight, down_weight, count, pairs):
    rows, model_width = arrived.shape
    columns = model_width // (2 * pairs)
    full = pl.BlockSpec(memory_space=pltpu.VMEM)
    dma = pltpu.SemaphoreType.DMA
    block = pltpu.VMEM((pairs, rows, columns), jnp.bfloat16)
    return pl.pallas_call(
        functools.partial(expert_kernel, count, pairs),
        out_shape=jax.ShapeDtypeStruct((pairs, rows, columns), jnp.bfloat16),
        in_specs=[full] * 4,
        out_specs=full,
        scratch_shapes=[block] * 5
        + [dma((pairs,))] * 4
        + [dma((pairs, count))] * 2,
        compiler_params=pltpu.CompilerParams(collective_id=1, has_side_effects=True),
        cost_estimate=pl.CostEstimate(
            flops=10 * rows * model_width * gate_weight.shape[2] * 6,
            bytes_accessed=model_width * gate_weight.shape[2] * 6,
            transcendentals=0,
        ),
    )(arrived, gate_weight, up_weight, down_weight)


def routed_by_exchange(flat_rows, gate_weight, up_weight, down_weight, count, pairs):
    rows, model_width = flat_rows.shape
    columns = model_width // (2 * pairs)
    gate = jnp.dot(flat_rows, gate_weight[0], preferred_element_type=jnp.float32)
    upward = jnp.dot(flat_rows, up_weight[0], preferred_element_type=jnp.float32)
    hidden = (jax.nn.silu(gate) * upward).astype(jnp.bfloat16)
    partial_value = jnp.dot(hidden, down_weight[0], preferred_element_type=jnp.float32).astype(
        jnp.bfloat16
    )
    pieces = lax.all_to_all(partial_value[None], "tp", split_axis=2, concat_axis=0, tiled=True)
    paired = pieces.reshape(pairs, 2, rows, columns).astype(jnp.float32)
    expert_value = (
        (paired[:, 0] + paired[:, 1])
        .astype(jnp.bfloat16)
        .reshape(pairs, count, rows // count, columns)
    )
    returned = lax.all_to_all(expert_value, "ep", split_axis=1, concat_axis=1, tiled=True)
    return returned.reshape(-1, columns)


def expert_half(
    expert_input_rows,
    expert_norm_gain,
    selected_expert_index,
    selected_expert_weight,
    routed_gate_weight,
    routed_up_weight,
    routed_down_weight,
    common_gate_weight,
    common_up_weight,
    common_down_weight,
):
    tok_rows, model_width = expert_input_rows.shape
    chosen_count = selected_expert_index.shape[1]
    ep_count = lax.axis_size("ep")
    tp_count = lax.axis_size("tp")
    group_count = tp_count // 2
    expert_total = group_count * ep_count
    capacity = 2 * tok_rows * chosen_count // expert_total
    column_count = model_width // tp_count
    tp_place = lax.axis_index("tp")
    group_index = tp_place // 2
    normed = rms_scale(expert_input_rows, expert_norm_gain).astype(jnp.bfloat16)
    assigned = selected_expert_index.reshape(-1)
    assign_count = assigned.shape[0]
    expert_ids = jnp.arange(expert_total, dtype=jnp.int32)
    onehot = (assigned[:, None] == expert_ids[None, :]).astype(jnp.int32)
    ranking = jnp.sum((jnp.cumsum(onehot, axis=0) - onehot) * onehot, axis=1)
    target = jnp.where(
        assigned % group_count == group_index, assigned // group_count * capacity + ranking, -1
    ).reshape(tok_rows, chosen_count)
    slots = jnp.arange(ep_count * capacity, dtype=jnp.int32)
    placing = jnp.any(target[:, :, None] == slots[None, None, :], axis=1).astype(jnp.bfloat16)
    outgoing = lax.dot_general(
        placing, normed, (((0,), (0,)), ((), ())), preferred_element_type=jnp.float32
    ).astype(jnp.bfloat16)
    arrived = lax.all_to_all(
        outgoing.reshape(ep_count, capacity, model_width),
        "ep",
        split_axis=0,
        concat_axis=0,
        tiled=True,
    ).reshape(-1, model_width)
    if capacity % 16 == 0 and column_count % 128 == 0:
        flat_back = routed_by_kernel(
            arrived, routed_gate_weight, routed_up_weight, routed_down_weight, ep_count, group_count
        ).reshape(-1, column_count)
    else:
        flat_back = routed_by_exchange(
            arrived, routed_gate_weight, routed_up_weight, routed_down_weight, ep_count, group_count
        )
    position = (
        assigned % group_count * (ep_count * capacity)
        + assigned // group_count * capacity
        + ranking
    )
    picked = (
        jnp.take(flat_back, position, axis=0)
        .astype(jnp.float32)
        .reshape(tok_rows, chosen_count, column_count)
    )
    routed = jnp.sum(picked * selected_expert_weight[:, :, None], axis=1)
    shared_hidden = (
        jax.nn.silu(jnp.dot(normed, common_gate_weight, preferred_element_type=jnp.float32))
        * jnp.dot(normed, common_up_weight, preferred_element_type=jnp.float32)
    ).astype(jnp.bfloat16)
    shared_sum = lax.psum_scatter(
        lax.dot_general(
            common_down_weight,
            shared_hidden,
            (((0,), (1,)), ((), ())),
            preferred_element_type=jnp.float32,
        ).astype(jnp.bfloat16),
        "tp",
        scatter_dimension=0,
        tiled=True,
    ).astype(jnp.float32)
    return (routed + shared_sum.T).astype(jnp.bfloat16)


def mm(x, y, dims=NN):
    return lax.dot_general(x, y, (dims, ((), ())), preferred_element_type=jnp.float32)


def pair_masks():
    lane = lax.broadcasted_iota(jnp.int32, (BLOCK, 2 * HEAD_CHANNELS), 1)
    first = jnp.where(lane < HEAD_CHANNELS, 1.0, 0.0)
    return first.astype(jnp.bfloat16), (1.0 - first).astype(jnp.bfloat16)


def stacked(y, masks):
    return jnp.concatenate([y * masks[0], y * masks[1]], axis=0)


def pair_dot(x, parts):
    xh, xl = split_parts(x)
    high, low = parts
    return mm(jnp.concatenate([xh, xl], axis=1), jnp.concatenate([high, high], axis=0)) + mm(
        xh, low
    )


def pair_parts(y, masks):
    yh, yl = split_parts(y)
    return stacked(yh, masks), stacked(yl, masks)


def side_by_side(one, two):
    return tuple(jnp.concatenate([p, q], axis=1) for p, q in zip(one, two))


def head_sum(x, block_ones):
    xh, xl = split_parts(x)
    return mm(jnp.concatenate([xh, xl], axis=1), block_ones)


def head_ones():
    wide = 2 * HEAD_CHANNELS
    row = lax.broadcasted_iota(jnp.int32, (2 * wide, wide), 0)
    col = lax.broadcasted_iota(jnp.int32, (2 * wide, wide), 1)
    same = (row // HEAD_CHANNELS) % 2 == col // HEAD_CHANNELS
    return jnp.where(same, 1.0, 0.0).astype(jnp.bfloat16)


def local_math(r_ref, k_ref, v_ref, dec_ref, lr_ref, off_ref, spike_ref):
    rows, width = r_ref.shape
    wide = 2 * HEAD_CHANNELS
    pairs = width // wide
    chunks = rows // BLOCK
    masks = pair_masks()
    ones_head = head_ones()
    row = lax.broadcasted_iota(jnp.int32, (BLOCK, wide), 0)
    col = lax.broadcasted_iota(jnp.int32, (BLOCK, wide), 1) % HEAD_CHANNELS
    strict = col < row
    inclusive = col <= row
    trow = lax.broadcasted_iota(jnp.int32, (BLOCK, 4 * BLOCK), 0)
    tcol = lax.broadcasted_iota(jnp.int32, (BLOCK, 4 * BLOCK), 1)
    running = jnp.where((tcol % BLOCK <= trow) & (tcol < 3 * BLOCK), 1.0, 0.0).astype(jnp.bfloat16)
    blank = jnp.zeros((BLOCK, wide), jnp.bfloat16)
    items = [(i, p) for i in range(chunks) for p in range(pairs)]
    lows, low_vs, out_bs, out_vs, ins_ends, b_ends, r_outs, a_ins, vs, ends = (
        [] for _ in range(10)
    )
    for i, p in items:
        span = slice(i * BLOCK, (i + 1) * BLOCK)
        lanes = slice(p * wide, (p + 1) * wide)
        r = r_ref[span, lanes].astype(jnp.float32)
        k = k_ref[span, lanes].astype(jnp.float32)
        v = v_ref[span, lanes]
        learn = jax.nn.sigmoid(lr_ref[span, lanes].astype(jnp.float32))
        pre = off_ref[:, lanes] + jnp.tanh(dec_ref[span, lanes].astype(jnp.float32))
        log = spike_ref[span, lanes] - jax.nn.sigmoid(pre) * jnp.exp(jnp.float32(-0.5))
        p0 = log.astype(jnp.bfloat16)
        rest = log - p0.astype(jnp.float32)
        p1 = rest.astype(jnp.bfloat16)
        p2 = (rest - p1.astype(jnp.float32)).astype(jnp.bfloat16)
        cum = mm(running, jnp.concatenate([p0, p1, p2, blank], axis=0))
        before = cum - log
        last = cum[BLOCK - 1 :]
        a = k * lax.rsqrt(head_sum(k * k, ones_head) + NORM_EPSILON)
        back = jnp.exp(-cum)
        end = jnp.exp(last)
        a_in = a * jnp.exp(before)
        r_out = r * jnp.exp(cum)
        b_back = a * learn * back
        ins_back = k * learn * back
        lh, ll = split_parts(jnp.concatenate([a_in, r_out], axis=0))
        bh, bl = split_parts(b_back)
        ih, il = split_parts(ins_back)
        right_high = jnp.concatenate([stacked(bh, masks), stacked(ih, masks)], axis=0)
        right_low = jnp.concatenate([stacked(bl, masks), stacked(il, masks)], axis=0)
        gram = mm(
            jnp.concatenate([lh, ll], axis=1),
            jnp.concatenate([right_high, right_high], axis=1),
            NT,
        ) + mm(lh, right_low, NT)
        lows.append(jnp.where(strict, gram[:BLOCK, :wide], 0.0))
        low_k = jnp.where(strict, gram[:BLOCK, wide:], 0.0)
        out_bs.append(jnp.where(inclusive, gram[BLOCK:, :wide], 0.0))
        out_k = jnp.where(inclusive, gram[BLOCK:, wide:], 0.0)
        kh, kl = split_parts(jnp.concatenate([low_k, out_k], axis=0))
        values = stacked(v, masks)
        weighted = mm(
            jnp.concatenate([kh, kl], axis=1), jnp.concatenate([values, values], axis=0)
        )
        low_vs.append(weighted[:BLOCK])
        out_vs.append(weighted[BLOCK:])
        ins_ends.append(ins_back * end)
        b_ends.append(b_back * end)
        r_outs.append(r_out)
        a_ins.append(a_in)
        vs.append(v)
        ends.append(end)
    count = range(len(items))
    eye = jnp.where(row == col, 1.0, 0.0)
    inverses = None
    size = 1
    while size < BLOCK:
        inside = (row // (2 * size) == col // (2 * size)) & (row // size != col // size)
        corners = [jnp.where(inside, low, 0.0) for low in lows]
        if size == 1:
            inverses = [eye - corner for corner in corners]
        else:
            firsts = [
                pair_dot(inverses[n], pair_parts(corners[n], masks)) for n in count
            ]
            inverses = [
                inverses[n] - pair_dot(firsts[n], pair_parts(inverses[n], masks)) for n in count
            ]
        size *= 2
    solved = [
        side_by_side(pair_parts(a_ins[n], masks), pair_parts(low_vs[n], masks)) for n in count
    ]
    solved = [pair_dot(inverses[n], solved[n]) for n in count]
    brow = lax.broadcasted_iota(jnp.int32, (wide, 2 * wide), 0)
    bcol = lax.broadcasted_iota(jnp.int32, (wide, 2 * wide), 1)
    same_head = brow // HEAD_CHANNELS == (bcol % wide) // HEAD_CHANNELS
    diagonal = brow == bcol
    maps = []
    for n in count:
        left = jnp.concatenate([-b_ends[n], ins_ends[n]], axis=0)
        lh, ll = split_parts(left)
        uh, ul = split_parts(solved[n])
        high = jnp.concatenate([uh, jnp.concatenate([blank, vs[n]], axis=1)], axis=0)
        low = jnp.concatenate([ul, jnp.concatenate([blank, blank], axis=1)], axis=0)
        made = mm(
            jnp.concatenate([lh, ll], axis=0), jnp.concatenate([high, high], axis=0), TN
        ) + mm(lh, low, TN)
        end = jnp.concatenate([ends[n], ends[n]], axis=1)
        maps.append(jnp.where(same_head, made + jnp.where(diagonal, end, 0.0), 0.0))
    whole = [None] * pairs
    heads_at = []
    for n in count:
        p = items[n][1]
        heads_at.append(whole[p])
        if whole[p] is None:
            whole[p] = maps[n]
        else:
            joined = pair_dot(maps[n][:, :wide], split_parts(whole[p]))
            whole[p] = jnp.concatenate(
                [joined[:, :wide], joined[:, wide:] + maps[n][:, wide:]], axis=1
            )
    compact = [m[:HEAD_CHANNELS] + m[HEAD_CHANNELS:] for m in whole]

    def finish():
        results = {}
        for n in count:
            uh, ul = split_parts(solved[n])
            parts = [
                jnp.concatenate([stacked(u[:, :wide], masks), stacked(u[:, wide:], masks)], axis=1)
                for u in (uh, ul)
            ]
            removed = pair_dot(out_bs[n], parts)
            carry = r_outs[n] - removed[:, :wide]
            value = out_vs[n] - removed[:, wide:]
            if heads_at[n] is not None:
                moved = pair_dot(carry, split_parts(heads_at[n]))
                carry = moved[:, :wide]
                value = value + moved[:, wide:]
            results[items[n]] = (carry, value)
        return results

    return compact, finish


def mega_kernel(ep_count, *refs):
    (
        r_in, k_in, v_in, dec_in, lr_in, gate_in, off_in, spike_in, hgain_in, wout_in, pgain_in,
        x_in, egain_in, idx_in, wsel_in, wg_in, wu_in, wd_in, cg_in, cu_in, cd_in,
    ) = refs[:21]
    attn_out, expert_out = refs[21:23]
    (
        r_ref, k_ref, v_ref, dec_ref, lr_ref, gate_ref, off_ref, spike_ref, hgain_ref, wout_ref,
        pgain_ref, x_ref, egain_ref, idx_ref, wsel_ref, wg_ref, wu_ref, wd_ref, cg_ref, cu_ref,
        cd_ref,
    ) = refs[23:44]
    (
        normed, outgoing, arrived, carry_ref, value_ref, own_map, part_map, own_join, held, state,
        shared, shared_half, shared_sum, shared_last, crossing, halves, own_ref, final, back,
        heads_ref, mix, mix_half, mix_sum, mix_last,
        load_sem, disp_send, disp_recv, fwd_send, fwd_recv, map_send, map_recv, join_send,
        join_recv, sh_send, sh_recv, cross_send, cross_recv, home_send, home_recv, mx_send,
        mx_recv, tail_send, tail_recv,
    ) = refs[44:]
    me = lax.axis_index("ep")
    place = lax.axis_index("tp")
    group = place // 2
    half = place % 2
    other = 1 - half
    partner = 2 * group + other
    across = 2 * (1 - group) + half
    seat = me // 2
    side = me % 2
    seats = ep_count // 2
    tok_rows, model_width = x_ref.shape
    slots = outgoing.shape[0]
    capacity = slots // ep_count
    fold = model_width // 2
    columns = model_width // 4
    rows, width = r_ref.shape
    wide = 2 * HEAD_CHANNELS
    pairs = width // wide
    block_rows = rows // 4

    barrier = pltpu.get_barrier_semaphore()

    def peer(step):
        return lax.rem(me + step, ep_count)

    for step in range(ep_count):
        for turn in range(2):
            if step or turn:
                pl.semaphore_signal(
                    barrier,
                    inc=1,
                    device_id={
                        "ep": peer(step),
                        "tp": 2 * lax.rem(group + turn, 2) + half,
                    },
                    device_id_type=MESH,
                )
    pl.semaphore_signal(barrier, inc=1, device_id={"tp": partner}, device_id_type=MESH)

    sources = (
        r_in, k_in, v_in, dec_in, lr_in, gate_in, off_in, spike_in, hgain_in, wout_in, pgain_in,
        x_in, egain_in, idx_in, wsel_in, wg_in, wu_in, wd_in, cg_in, cu_in, cd_in,
    )
    targets = (
        r_ref, k_ref, v_ref, dec_ref, lr_ref, gate_ref, off_ref, spike_ref, hgain_ref, wout_ref,
        pgain_ref, x_ref, egain_ref, idx_ref, wsel_ref, wg_ref, wu_ref, wd_ref, cg_ref, cu_ref,
        cd_ref,
    )
    loads = [
        pltpu.make_async_copy(source, target, load_sem.at[n])
        for n, (source, target) in enumerate(zip(sources, targets))
    ]
    for n in (11, 12, 13, 14, 0, 1, 2, 3, 4, 6, 7, 18, 19, 20, 15, 16, 17, 5, 8, 9, 10):
        loads[n].start()

    def rows_of(index):
        return pl.ds(pl.multiple_of(index * capacity, capacity), capacity)

    def remote(source, target, send, recv, where):
        return pltpu.make_async_remote_copy(
            src_ref=source,
            dst_ref=target,
            send_sem=send,
            recv_sem=recv,
            device_id=where,
            device_id_type=MESH,
        )

    def dispatch(step):
        return remote(
            outgoing.at[rows_of(peer(step))],
            arrived.at[half, rows_of(me)],
            disp_send.at[step],
            disp_recv.at[step],
            {"ep": peer(step)},
        )

    def forward(step):
        came = lax.rem(me + ep_count - step, ep_count)
        return remote(
            arrived.at[half, rows_of(came)],
            arrived.at[half, rows_of(came)],
            fwd_send.at[step],
            fwd_recv.at[step],
            {"tp": partner},
        )

    for n in (11, 12, 13, 14):
        loads[n].wait()
    normed[...] = rms_scale(x_ref[...], egain_ref[...]).astype(jnp.bfloat16)
    chosen_count = idx_ref.shape[0]
    experts = 2 * ep_count
    expert_row = lax.broadcasted_iota(jnp.int32, (experts, tok_rows), 0)
    named = [expert_row == idx_ref[k : k + 1, :] for k in range(chosen_count)]
    member = functools.reduce(jnp.logical_or, named)
    weight_of = functools.reduce(
        jnp.add, [jnp.where(n, wsel_ref[k : k + 1, :], 0.0) for k, n in enumerate(named)]
    )
    early = lax.broadcasted_iota(jnp.int32, (tok_rows, tok_rows), 0) < lax.broadcasted_iota(
        jnp.int32, (tok_rows, tok_rows), 1
    )
    rank = mm(
        jnp.where(member, 1.0, 0.0).astype(jnp.bfloat16),
        jnp.where(early, 1.0, 0.0).astype(jnp.bfloat16),
    )
    rank = jnp.where(member, rank, -1.0).astype(jnp.bfloat16)
    slot = lax.broadcasted_iota(jnp.int32, (slots, experts), 0)
    which = lax.broadcasted_iota(jnp.int32, (slots, experts), 1)
    mine = jnp.where(which == 2 * (slot // capacity) + group, 1.0, 0.0).astype(jnp.bfloat16)
    slot_rank = (
        lax.broadcasted_iota(jnp.int32, (slots, tok_rows), 0) % capacity
    ).astype(jnp.float32)
    placing = jnp.where(mm(mine, rank) == slot_rank, 1.0, 0.0).astype(jnp.bfloat16)
    fold_span = pl.ds(pl.multiple_of(half * fold, fold), fold)
    outgoing[...] = mm(placing, normed[:, fold_span]).astype(jnp.bfloat16)
    arrived[half, rows_of(me), :] = outgoing[rows_of(me), :]
    pl.semaphore_wait(barrier, 2 * ep_count)
    order = list(range(1, ep_count))
    for step in order:
        dispatch(step).start()
    forward(0).start()

    for n in (0, 1, 2, 3, 4, 6, 7):
        loads[n].wait()
    compact, finish = local_math(r_ref, k_ref, v_ref, dec_ref, lr_ref, off_ref, spike_ref)
    for p in range(pairs):
        own_map[p] = compact[p].astype(jnp.bfloat16)
    swap = remote(
        own_map, part_map, map_send.at[0], map_recv.at[0], {"ep": 2 * seat + 1 - side}
    )
    swap.start()
    for (i, p), (carry, value) in finish().items():
        span = slice(i * BLOCK, (i + 1) * BLOCK)
        lanes = slice(p * wide, (p + 1) * wide)
        carry_ref[span, lanes] = carry
        value_ref[span, lanes] = value

    masks = pair_masks()
    swap.wait_recv()
    for p in range(pairs):
        mine_map = own_map[p]
        their_map = part_map[p]
        first = jnp.where(side == 0, mine_map, their_map)
        second = jnp.where(side == 0, their_map, mine_map)
        blocks = jnp.concatenate(
            [stacked(first[:, :wide], masks), stacked(first[:, wide:], masks)], axis=1
        )
        joined = mm(second[:, :wide], blocks)
        own_join[p] = jnp.concatenate(
            [joined[:, :wide], joined[:, wide:] + second[:, wide:].astype(jnp.float32)], axis=1
        ).astype(jnp.bfloat16)

    def upward(step):
        return remote(
            own_join,
            held.at[seat],
            join_send.at[step],
            join_recv.at[seat],
            {"ep": lax.rem(me + 2 * step, ep_count)},
        )

    def arrival(turn):
        return remote(
            own_join, held.at[turn], join_send.at[1], join_recv.at[turn],
            {"ep": lax.rem(me + 2, ep_count)},
        )

    for step in range(1, seats):

        @pl.when(seat + step < seats)
        def _():
            upward(step).start()

    for n in (18, 19, 20):
        loads[n].wait()
    rows_in = normed[...]
    hidden = (jax.nn.silu(mm(rows_in, cg_ref[...])) * mm(rows_in, cu_ref[...])).astype(
        jnp.bfloat16
    )
    for j in range(4):
        shared[j] = mm(hidden, cd_ref[:, j * columns : (j + 1) * columns]).astype(jnp.bfloat16)

    def shared_cross(g):
        return remote(
            shared.at[2 * g + other],
            shared_half.at[g],
            sh_send.at[g],
            sh_recv.at[g],
            {"tp": partner},
        )

    for g in range(2):
        shared_cross(g).start()

    for n in (15, 16, 17):
        loads[n].wait()
    for step in order:
        dispatch(step).wait_recv()
        forward(step).start()
    other_span = pl.ds(pl.multiple_of(other * fold, fold), fold)
    own_rows = arrived[half]
    gate = mm(own_rows, wg_ref[fold_span, :])
    upper = mm(own_rows, wu_ref[fold_span, :])

    for g in range(2):
        shared_cross(g).wait_recv()
        shared_sum[g] = shared[2 * g + half].astype(jnp.float32) + shared_half[g].astype(
            jnp.float32
        )
    shared_last[0] = shared_sum[1 - group].astype(jnp.bfloat16)
    shared_tail = remote(
        shared_last.at[0], shared_last.at[1], tail_send.at[0], tail_recv.at[0], {"tp": across}
    )
    shared_tail.start()

    for step in range(ep_count):
        forward(step).wait_recv()
    other_rows = arrived[other]
    gate = gate + mm(other_rows, wg_ref[other_span, :])
    upper = upper + mm(other_rows, wu_ref[other_span, :])
    routed_hidden = (jax.nn.silu(gate) * upper).astype(jnp.bfloat16)

    def part(index):
        span = pl.ds(pl.multiple_of(index * columns, columns), columns)
        return mm(routed_hidden, wd_ref[:, span])

    def cross(turn):
        return remote(
            crossing.at[turn],
            halves.at[turn],
            cross_send.at[turn],
            cross_recv.at[turn],
            {"tp": partner},
        )

    turn_order = (1, 0)
    for turn in turn_order:
        crossing[turn] = part(2 * lax.rem(group + turn, 2) + other).astype(jnp.bfloat16)
        cross(turn).start()
    for turn in turn_order:
        own_ref[turn] = part(2 * lax.rem(group + turn, 2) + half)

    def home(turn, step):
        return remote(
            final.at[turn, rows_of(peer(step))],
            back.at[group, rows_of(me)],
            home_send.at[turn, step],
            home_recv.at[turn, step],
            {"ep": peer(step), "tp": 2 * lax.rem(group + turn, 2) + half},
        )

    for turn in turn_order:
        cross(turn).wait_recv()
        final[turn] = (own_ref[turn] + halves[turn].astype(jnp.float32)).astype(jnp.bfloat16)
        for step in list(range(1, ep_count)) + ([0] if turn else []):
            home(turn, step).start()
    back[group, rows_of(me), :] = final[0, rows_of(me), :]

    for n in (5, 8, 9, 10):
        loads[n].wait()
    state[...] = jnp.zeros_like(state)

    def one(turn, _):
        arrival(turn).wait_recv()
        for p in range(pairs):
            block = held[turn, p]
            high, low = pair_parts(state[p], masks)
            through = block[:, :wide]
            state[p] = mm(
                jnp.concatenate([through, through], axis=1), jnp.concatenate([high, low], axis=0)
            ) + block[:, wide:].astype(jnp.float32)
        return 0

    lax.fori_loop(0, seat, one, 0)
    ones_head = head_ones()
    for p in range(pairs):
        lanes = slice(p * wide, (p + 1) * wide)
        block = part_map[p]
        high, low = pair_parts(state[p], masks)
        through = block[:, :wide]
        moved = mm(
            jnp.concatenate([through, through], axis=1), jnp.concatenate([high, low], axis=0)
        ) + block[:, wide:].astype(jnp.float32)
        current = jnp.where(side == 1, moved, state[p])
        value = value_ref[:, lanes] + pair_dot(carry_ref[:, lanes], pair_parts(current, masks))
        centred = value - head_sum(value, ones_head) * (1.0 / HEAD_CHANNELS)
        spread = head_sum(centred * centred, ones_head) * (1.0 / HEAD_CHANNELS)
        heads_ref[:, lanes] = (
            centred
            * lax.rsqrt(spread + GROUP_EPSILON)
            * hgain_ref[:, lanes]
            * jax.nn.sigmoid(gate_ref[:, lanes].astype(jnp.float32))
        ).astype(jnp.bfloat16)
    for j in range(4):
        span = slice(j * columns, (j + 1) * columns)
        made = mm(heads_ref[...], wout_ref[:, span]).astype(jnp.bfloat16)
        for b in range(4):
            mix[b, :, span] = made[b * block_rows : (b + 1) * block_rows]

    def mix_cross(g):
        return remote(
            mix.at[2 * g + other],
            mix_half.at[g],
            mx_send.at[g],
            mx_recv.at[g],
            {"tp": partner},
        )

    for g in range(2):
        mix_cross(g).start()
    for g in range(2):
        mix_cross(g).wait_recv()
        mix_sum[g] = mix[2 * g + half].astype(jnp.float32) + mix_half[g].astype(jnp.float32)
    mix_last[0] = mix_sum[1 - group].astype(jnp.bfloat16)
    mix_tail = remote(
        mix_last.at[0], mix_last.at[1], tail_send.at[1], tail_recv.at[1], {"tp": across}
    )
    mix_tail.start()

    all_slots = 2 * slots
    slot = lax.broadcasted_iota(jnp.int32, (experts, all_slots), 1)
    which = lax.broadcasted_iota(jnp.int32, (experts, all_slots), 0)
    holder = jnp.where(
        which == 2 * ((slot % slots) // capacity) + slot // slots, 1.0, 0.0
    ).astype(jnp.bfloat16)
    slot_rank = (
        lax.broadcasted_iota(jnp.int32, (tok_rows, all_slots), 1) % capacity
    ).astype(jnp.float32)
    hit = mm(rank, holder, TN) == slot_rank
    weight_high, weight_low = split_parts(weight_of)
    picks = [
        jnp.where(hit, mm(w, holder, TN), 0.0).astype(jnp.bfloat16)
        for w in (weight_high, weight_low)
    ]
    shared_tail.wait_recv()
    base = shared_sum[group] + shared_last[1].astype(jnp.float32)
    for turn in range(2):
        for step in range(ep_count):
            if step or turn:
                home(turn, step).wait_recv()
    returned = back[...].reshape(all_slots, columns)
    routed = mm(
        jnp.concatenate(picks, axis=1), jnp.concatenate([returned, returned], axis=0)
    )
    expert_out[...] = (routed + base).astype(jnp.bfloat16)

    mix_tail.wait_recv()
    total = mix_sum[group] + mix_last[1].astype(jnp.float32)
    attn_out[...] = rms_scale(total, pgain_ref[...]).astype(jnp.bfloat16)

    for step in order:
        dispatch(step).wait_send()
    for step in range(ep_count):
        forward(step).wait_send()
    swap.wait_send()
    for step in range(1, seats):

        @pl.when(seat + step < seats)
        def _():
            upward(step).wait_send()

    for g in range(2):
        shared_cross(g).wait_send()
        cross(g).wait_send()
        mix_cross(g).wait_send()
    shared_tail.wait_send()
    mix_tail.wait_send()
    for turn in range(2):
        for step in range(ep_count):
            if step or turn:
                home(turn, step).wait_send()


def mega(
    receptance, head_key_input, head_value_input, decay_input_part, learning_rate_input,
    output_gate_input, decay_channel_offset, spike_log_decay, head_norm_gain, head_output_weight,
    projection_norm_gain, expert_input_rows, expert_norm_gain, selected_expert_index,
    selected_expert_weight, routed_gate_weight, routed_up_weight, routed_down_weight,
    common_gate_weight, common_up_weight, common_down_weight,
):
    ep_count = lax.axis_size("ep")
    rows, width = receptance.shape
    tok_rows, model_width = expert_input_rows.shape
    chosen = selected_expert_index.shape[1]
    capacity = tok_rows * chosen // ep_count
    slots = ep_count * capacity
    columns = model_width // 4
    wide = 2 * HEAD_CHANNELS
    pairs = width // wide
    operands = (
        receptance, head_key_input, head_value_input, decay_input_part, learning_rate_input,
        output_gate_input, decay_channel_offset[None, :], spike_log_decay, head_norm_gain[None, :],
        head_output_weight, projection_norm_gain[None, :], expert_input_rows,
        expert_norm_gain[None, :], selected_expert_index.T, selected_expert_weight.T,
        routed_gate_weight[0], routed_up_weight[0], routed_down_weight[0], common_gate_weight,
        common_up_weight, common_down_weight,
    )
    bf16, f32 = jnp.bfloat16, jnp.float32
    dma = pltpu.SemaphoreType.DMA
    scratch = [pltpu.VMEM(o.shape, o.dtype) for o in operands] + [
        pltpu.VMEM((tok_rows, model_width), bf16),
        pltpu.VMEM((slots, model_width // 2), bf16),
        pltpu.VMEM((2, slots, model_width // 2), bf16),
        pltpu.VMEM((rows, width), f32),
        pltpu.VMEM((rows, width), f32),
        pltpu.VMEM((pairs, HEAD_CHANNELS, 2 * wide), bf16),
        pltpu.VMEM((pairs, HEAD_CHANNELS, 2 * wide), bf16),
        pltpu.VMEM((pairs, HEAD_CHANNELS, 2 * wide), bf16),
        pltpu.VMEM((ep_count // 2, pairs, HEAD_CHANNELS, 2 * wide), bf16),
        pltpu.VMEM((pairs, HEAD_CHANNELS, wide), f32),
        pltpu.VMEM((4, tok_rows, columns), bf16),
        pltpu.VMEM((2, tok_rows, columns), bf16),
        pltpu.VMEM((2, tok_rows, columns), f32),
        pltpu.VMEM((2, tok_rows, columns), bf16),
        pltpu.VMEM((2, slots, columns), bf16),
        pltpu.VMEM((2, slots, columns), bf16),
        pltpu.VMEM((2, slots, columns), f32),
        pltpu.VMEM((2, slots, columns), bf16),
        pltpu.VMEM((2, slots, columns), bf16),
        pltpu.VMEM((rows, width), bf16),
        pltpu.VMEM((4, rows // 4, model_width), bf16),
        pltpu.VMEM((2, rows // 4, model_width), bf16),
        pltpu.VMEM((2, rows // 4, model_width), f32),
        pltpu.VMEM((2, rows // 4, model_width), bf16),
        dma((len(operands),)),
    ]
    scratch += [dma((ep_count,))] * 4
    scratch += [dma((1,))] * 2
    scratch += [dma((ep_count // 2,))] * 2
    scratch += [dma((2,))] * 4
    scratch += [dma((2, ep_count))] * 2
    scratch += [dma((2,))] * 4
    full = pl.BlockSpec(memory_space=pltpu.VMEM)
    return pl.pallas_call(
        functools.partial(mega_kernel, ep_count),
        out_shape=(
            jax.ShapeDtypeStruct((rows // 4, model_width), bf16),
            jax.ShapeDtypeStruct((tok_rows, columns), bf16),
        ),
        in_specs=[pl.BlockSpec(memory_space=pl.ANY)] * len(operands),
        out_specs=(full, full),
        scratch_shapes=scratch,
        compiler_params=pltpu.CompilerParams(collective_id=0, has_side_effects=True),
    )(*operands)


def fits_mega(receptance, expert_input_rows, selected_expert_index):
    ep_count = lax.axis_size("ep")
    rows, width = receptance.shape
    tok_rows, model_width = expert_input_rows.shape
    assigned = tok_rows * selected_expert_index.shape[1]
    return (
        lax.axis_size("tp") == 4
        and ep_count % 2 == 0
        and width % (2 * HEAD_CHANNELS) == 0
        and rows % (4 * BLOCK) == 0
        and assigned % (16 * ep_count) == 0
        and tok_rows % 128 == 0
        and tok_rows <= 256
        and model_width % 512 == 0
    )


def body(
    receptance,
    head_key_input,
    head_value_input,
    decay_input_part,
    learning_rate_input,
    output_gate_input,
    decay_channel_offset,
    spike_log_decay,
    head_norm_gain,
    head_output_weight,
    projection_norm_gain,
    expert_input_rows,
    expert_norm_gain,
    selected_expert_index,
    selected_expert_weight,
    routed_gate_weight,
    routed_up_weight,
    routed_down_weight,
    common_gate_weight,
    common_up_weight,
    common_down_weight,
):
    if fits_mega(receptance, expert_input_rows, selected_expert_index):
        return mega(
            receptance, head_key_input, head_value_input, decay_input_part, learning_rate_input,
            output_gate_input, decay_channel_offset, spike_log_decay, head_norm_gain,
            head_output_weight, projection_norm_gain, expert_input_rows, expert_norm_gain,
            selected_expert_index, selected_expert_weight, routed_gate_weight, routed_up_weight,
            routed_down_weight, common_gate_weight, common_up_weight, common_down_weight,
        )
    attention_output = attention_mixer(
        receptance,
        head_key_input,
        head_value_input,
        decay_input_part,
        learning_rate_input,
        output_gate_input,
        decay_channel_offset,
        spike_log_decay,
        head_norm_gain,
        head_output_weight,
        projection_norm_gain,
    )
    expert_output = expert_half(
        expert_input_rows,
        expert_norm_gain,
        selected_expert_index,
        selected_expert_weight,
        routed_gate_weight,
        routed_up_weight,
        routed_down_weight,
        common_gate_weight,
        common_up_weight,
        common_down_weight,
    )
    return (attention_output, expert_output)


def solution(mesh):
    placed = (
        P("ep", "tp"),
        P("ep", "tp"),
        P("ep", "tp"),
        P("ep", "tp"),
        P("ep", "tp"),
        P("ep", "tp"),
        P("tp"),
        P("ep", "tp"),
        P("tp"),
        P("tp", None),
        P(),
        P("ep", None),
        P(),
        P("ep", None),
        P("ep", None),
        P(("ep", "tp"), None, None),
        P(("ep", "tp"), None, None),
        P(("ep", "tp"), None, None),
        P(None, "tp"),
        P(None, "tp"),
        P("tp", None),
    )
    return jax.shard_map(
        body,
        mesh=mesh,
        in_specs=placed,
        out_specs=(P(("ep", "tp"), None), P("ep", "tp")),
        check_vma=False,
    )
```

```python
import functools

import jax
import jax.numpy as jnp
from jax import lax
from jax.experimental import pallas as pl
from jax.experimental.pallas import tpu as pltpu
from jax.sharding import PartitionSpec as P

HEAD_CHANNELS = 64
BLOCK = 64


MESH = pl.DeviceIdType.MESH
NORM_EPSILON = 1e-06
GROUP_EPSILON = 0.00064


def rms_scale(values, gain):
    values = values.astype(jnp.float32)
    return (
        values * lax.rsqrt(jnp.mean(values * values, axis=-1, keepdims=True) + NORM_EPSILON) * gain
    )


def split_parts(x):
    high = x.astype(jnp.bfloat16)
    return high, (x - high.astype(jnp.float32)).astype(jnp.bfloat16)


def dot3(x, y, dims):
    xh, xl = split_parts(x)
    yh, yl = split_parts(y)

    def one(p, q):
        return lax.dot_general(p, q, (dims, ((), ())), preferred_element_type=jnp.float32)

    return one(xh, yh) + (one(xh, yl) + one(xl, yh))


NN = ((1,), (0,))
NT = ((1,), (1,))
TN = ((0,), (0,))


def local_kernel(
    r_ref, k_ref, v_ref, dec_ref, lr_ref, off_ref, spike_ref, out_ref, carry_ref, map_ref
):
    rows, width = r_ref.shape
    heads = width // HEAD_CHANNELS
    blocks = rows // BLOCK
    row = lax.broadcasted_iota(jnp.int32, (rows, rows), 0)
    col = lax.broadcasted_iota(jnp.int32, (rows, rows), 1)
    strict = col < row
    inclusive = col <= row
    learn_all = jax.nn.sigmoid(lr_ref[...].astype(jnp.float32))
    pre = off_ref[...] + jnp.tanh(dec_ref[...].astype(jnp.float32))
    log_all = spike_ref[...] - jax.nn.sigmoid(pre) * jnp.exp(jnp.float32(-0.5))
    ones = jnp.where(inclusive, 1.0, 0.0).astype(jnp.bfloat16)
    p0 = log_all.astype(jnp.bfloat16)
    rest = log_all - p0.astype(jnp.float32)
    p1 = rest.astype(jnp.bfloat16)
    p2 = (rest - p1.astype(jnp.float32)).astype(jnp.bfloat16)
    cum_all = sum(jnp.dot(ones, p, preferred_element_type=jnp.float32) for p in (p0, p1, p2))
    before_all = cum_all - log_all
    for h in range(heads):
        lanes = slice(h * HEAD_CHANNELS, (h + 1) * HEAD_CHANNELS)
        r = r_ref[:, lanes].astype(jnp.float32)
        k = k_ref[:, lanes].astype(jnp.float32)
        v = v_ref[:, lanes].astype(jnp.float32)
        learn = learn_all[:, lanes]
        cum = cum_all[:, lanes]
        before = before_all[:, lanes]
        a = k * lax.rsqrt(jnp.sum(k * k, axis=-1, keepdims=True) + NORM_EPSILON)
        b = a * learn
        ins = k * learn
        parts = []
        for i in range(blocks):
            span = slice(i * BLOCK, (i + 1) * BLOCK)
            base = before[i * BLOCK : i * BLOCK + 1]
            left = jnp.concatenate(
                [a[span] * jnp.exp(before[span] - base), r[span] * jnp.exp(cum[span] - base)],
                axis=0,
            )
            back = jnp.exp(jnp.minimum(base - cum, 60.0))
            right = jnp.concatenate([b * back, ins * back], axis=0)
            parts.append(dot3(left, right, NT))
        low_b = jnp.where(strict, jnp.concatenate([p[:BLOCK, :rows] for p in parts], axis=0), 0.0)
        low_k = jnp.where(strict, jnp.concatenate([p[:BLOCK, rows:] for p in parts], axis=0), 0.0)
        out_b = jnp.where(
            inclusive, jnp.concatenate([p[BLOCK:, :rows] for p in parts], axis=0), 0.0
        )
        out_k = jnp.where(
            inclusive, jnp.concatenate([p[BLOCK:, rows:] for p in parts], axis=0), 0.0
        )
        inverse = jnp.where(row == col, 1.0, 0.0)
        size = 1
        while size < BLOCK:
            corner = (row // (2 * size) == col // (2 * size)) & (row // size != col // size)
            corner = jnp.where(corner, low_b, 0.0)
            if size == 1:
                inverse = inverse - corner
            else:
                inverse = inverse - dot3(dot3(inverse, corner, NN), inverse, NN)
            size *= 2
        right_side = jnp.concatenate([a * jnp.exp(before), dot3(low_k, v, NN)], axis=1)
        solved = []
        for i in range(blocks):
            span = slice(i * BLOCK, (i + 1) * BLOCK)
            piece = right_side[span]
            if i:
                piece = piece - dot3(
                    low_b[span, : i * BLOCK], jnp.concatenate(solved, axis=0), NN
                )
            solved.append(dot3(inverse[span, span], piece, NN))
        solved = jnp.concatenate(solved, axis=0)
        removed = dot3(out_b, solved, NN)
        out_ref[:, lanes] = dot3(out_k, v, NN) - removed[:, HEAD_CHANNELS:]
        carry_ref[:, lanes] = r * jnp.exp(cum) - removed[:, :HEAD_CHANNELS]
        last = cum[rows - 1 :]
        to_end = jnp.exp(last - cum)
        taken = dot3(solved, b * to_end, TN)
        added = dot3(v, ins * to_end, TN)
        small = (HEAD_CHANNELS, HEAD_CHANNELS)
        eye = lax.broadcasted_iota(jnp.int32, small, 0) == lax.broadcasted_iota(jnp.int32, small, 1)
        through = jnp.where(eye, jnp.exp(last), 0.0) - taken[:HEAD_CHANNELS]
        fresh = added - taken[HEAD_CHANNELS:]
        map_ref[lanes, :] = jnp.concatenate([through, fresh], axis=1).astype(jnp.bfloat16)


def join_kernel(
    count, out_ref, carry_ref, map_ref, gain_ref, gate_ref, weight_ref, mix_ref, held, state,
    send_sem, recv_sem
):
    me = lax.axis_index("ep")
    rows, width = out_ref.shape
    heads = width // HEAD_CHANNELS
    barrier = pltpu.get_barrier_semaphore()
    for step in range(1, count):
        pl.semaphore_signal(
            barrier, inc=1, device_id={"ep": lax.rem(me + step, count)}, device_id_type=MESH
        )
    pl.semaphore_wait(barrier, count - 1)

    def copy(slot, step):
        return pltpu.make_async_remote_copy(
            src_ref=map_ref,
            dst_ref=held.at[slot],
            send_sem=send_sem.at[step],
            recv_sem=recv_sem.at[slot],
            device_id={"ep": lax.rem(me + step, count)},
            device_id_type=MESH,
        )

    for step in range(1, count):

        @pl.when(me + step < count)
        def _():
            copy(me, step).start()

    state[...] = jnp.zeros_like(state)

    def one(turn, _):
        copy(turn, 1).wait_recv()
        for h in range(heads):
            lanes = slice(h * HEAD_CHANNELS, (h + 1) * HEAD_CHANNELS)
            block = held[turn, lanes, :]
            high, low = split_parts(state[lanes, :])
            through = block[:, :HEAD_CHANNELS]
            state[lanes, :] = (
                jnp.dot(high, through, preferred_element_type=jnp.float32)
                + jnp.dot(low, through, preferred_element_type=jnp.float32)
                + block[:, HEAD_CHANNELS:].astype(jnp.float32)
            )
        return 0

    lax.fori_loop(0, me, one, 0)
    normed = []
    for h in range(heads):
        lanes = slice(h * HEAD_CHANNELS, (h + 1) * HEAD_CHANNELS)
        value = out_ref[:, lanes] + dot3(carry_ref[:, lanes], state[lanes, :], NT)
        centred = value - jnp.mean(value, axis=-1, keepdims=True)
        normed.append(
            centred
            * lax.rsqrt(jnp.mean(centred * centred, axis=-1, keepdims=True) + GROUP_EPSILON)
        )
    flat = normed[0] if heads == 1 else jnp.concatenate(normed, axis=1)
    heads_out = flat * gain_ref[...] * jax.nn.sigmoid(gate_ref[...].astype(jnp.float32))
    mix_ref[...] = jnp.dot(
        heads_out.astype(jnp.bfloat16), weight_ref[...], preferred_element_type=jnp.float32
    ).astype(jnp.bfloat16)
    for step in range(1, count):

        @pl.when(me + step < count)
        def _():
            copy(me, step).wait_send()


def attention_mixer(
    receptance,
    head_key_input,
    head_value_input,
    decay_input_part,
    learning_rate_input,
    output_gate_input,
    decay_channel_offset,
    spike_log_decay,
    head_norm_gain,
    head_output_weight,
    projection_norm_gain,
):
    rows, width = receptance.shape
    count = lax.axis_size("ep")
    full = pl.BlockSpec(memory_space=pltpu.VMEM)
    out, carry, maps = pl.pallas_call(
        local_kernel,
        out_shape=(
            jax.ShapeDtypeStruct((rows, width), jnp.float32),
            jax.ShapeDtypeStruct((rows, width), jnp.float32),
            jax.ShapeDtypeStruct((width, 2 * HEAD_CHANNELS), jnp.bfloat16),
        ),
        in_specs=[full] * 7,
        out_specs=(full, full, full),
        cost_estimate=pl.CostEstimate(
            flops=rows * rows * width * 200, bytes_accessed=rows * width * 22, transcendentals=0
        ),
    )(
        receptance,
        head_key_input,
        head_value_input,
        decay_input_part,
        learning_rate_input,
        decay_channel_offset[None, :],
        spike_log_decay,
    )
    model_width = head_output_weight.shape[1]
    mix = pl.pallas_call(
        functools.partial(join_kernel, count),
        out_shape=jax.ShapeDtypeStruct((rows, model_width), jnp.bfloat16),
        in_specs=[full] * 6,
        out_specs=full,
        scratch_shapes=[
            pltpu.VMEM((count, width, 2 * HEAD_CHANNELS), jnp.bfloat16),
            pltpu.VMEM((width, HEAD_CHANNELS), jnp.float32),
            pltpu.SemaphoreType.DMA((count,)),
            pltpu.SemaphoreType.DMA((count,)),
        ],
        compiler_params=pltpu.CompilerParams(collective_id=0, has_side_effects=True),
        cost_estimate=pl.CostEstimate(
            flops=rows * width * model_width * 20,
            bytes_accessed=width * model_width * 2,
            transcendentals=0,
        ),
    )(out, carry, maps, head_norm_gain[None, :], output_gate_input, head_output_weight)
    mix_sum = lax.psum_scatter(mix, "tp", scatter_dimension=0, tiled=True).astype(jnp.float32)
    return rms_scale(mix_sum, projection_norm_gain).astype(jnp.bfloat16)


def expert_kernel(
    count, pairs, arrived, gate_ref, up_ref, down_ref, result_ref, crossing, halves, paired,
    final, back, half_send, half_recv, pair_send, pair_recv, back_send, back_recv
):
    me = lax.axis_index("ep")
    place = lax.axis_index("tp")
    group = place // 2
    half = place % 2
    capacity = arrived.shape[0] // count
    columns = final.shape[2]
    partner = 2 * group + 1 - half

    def rows_of(index):
        return pl.ds(pl.multiple_of(index * capacity, capacity), capacity)

    def peer(step):
        return lax.rem(me + step, count)

    barrier = pltpu.get_barrier_semaphore()
    for step in range(1, count):
        pl.semaphore_signal(barrier, inc=1, device_id={"ep": peer(step)}, device_id_type=MESH)
    pl.semaphore_signal(barrier, inc=1, device_id={"tp": partner}, device_id_type=MESH)
    for step in range(1, pairs):
        there = 2 * lax.rem(group + step, pairs) + half
        pl.semaphore_signal(barrier, inc=1, device_id={"tp": there}, device_id_type=MESH)
    pl.semaphore_wait(barrier, count + pairs - 1)

    def cross(index):
        return pltpu.make_async_remote_copy(
            src_ref=crossing.at[index],
            dst_ref=halves.at[index],
            send_sem=half_send.at[index],
            recv_sem=half_recv.at[index],
            device_id={"tp": partner},
            device_id_type=MESH,
        )

    def pair(step):
        return pltpu.make_async_remote_copy(
            src_ref=paired.at[step],
            dst_ref=final.at[step],
            send_sem=pair_send.at[step],
            recv_sem=pair_recv.at[step],
            device_id={"tp": 2 * lax.rem(group + step, pairs) + half},
            device_id_type=MESH,
        )

    def home(turn, step):
        return pltpu.make_async_remote_copy(
            src_ref=final.at[turn, rows_of(peer(step))],
            dst_ref=back.at[turn, rows_of(me)],
            send_sem=back_send.at[turn, step],
            recv_sem=back_recv.at[turn, step],
            device_id={"ep": peer(step)},
            device_id_type=MESH,
        )

    rows = arrived[...]
    gate = jnp.dot(rows, gate_ref[0], preferred_element_type=jnp.float32)
    upward = jnp.dot(rows, up_ref[0], preferred_element_type=jnp.float32)
    hidden = (jax.nn.silu(gate) * upward).astype(jnp.bfloat16)

    def part(index):
        span = pl.ds(pl.multiple_of(index * columns, columns), columns)
        return jnp.dot(hidden, down_ref[0, :, span], preferred_element_type=jnp.float32).astype(
            jnp.bfloat16
        )

    order = list(range(1, pairs)) + [0]
    for step in order:
        crossing[step] = part(2 * lax.rem(group + step, pairs) + 1 - half)
        cross(step).start()
    own = {step: part(2 * lax.rem(group + step, pairs) + half) for step in order}
    for step in order:
        cross(step).wait_recv()
        total = (
            own[step].astype(jnp.float32) + halves[step].astype(jnp.float32)
        ).astype(jnp.bfloat16)
        if step:
            paired[step] = total
            pair(step).start()
        else:
            final[0] = total
    for turn in range(pairs):
        if turn:
            pair(turn).wait_recv()
        for step in range(1, count):
            home(turn, step).start()
        back[turn, rows_of(me), :] = final[turn, rows_of(me), :]
    for turn in range(pairs):
        for step in range(1, count):
            home(turn, step).wait_recv()
        result_ref[lax.rem(group + pairs - turn, pairs)] = back[turn]
    for step in order:
        cross(step).wait_send()
        if step:
            pair(step).wait_send()
    for turn in range(pairs):
        for step in range(1, count):
            home(turn, step).wait_send()


def routed_by_kernel(arrived, gate_weight, up_weight, down_weight, count, pairs):
    rows, model_width = arrived.shape
    columns = model_width // (2 * pairs)
    full = pl.BlockSpec(memory_space=pltpu.VMEM)
    dma = pltpu.SemaphoreType.DMA
    block = pltpu.VMEM((pairs, rows, columns), jnp.bfloat16)
    return pl.pallas_call(
        functools.partial(expert_kernel, count, pairs),
        out_shape=jax.ShapeDtypeStruct((pairs, rows, columns), jnp.bfloat16),
        in_specs=[full] * 4,
        out_specs=full,
        scratch_shapes=[block] * 5
        + [dma((pairs,))] * 4
        + [dma((pairs, count))] * 2,
        compiler_params=pltpu.CompilerParams(collective_id=1, has_side_effects=True),
        cost_estimate=pl.CostEstimate(
            flops=10 * rows * model_width * gate_weight.shape[2] * 6,
            bytes_accessed=model_width * gate_weight.shape[2] * 6,
            transcendentals=0,
        ),
    )(arrived, gate_weight, up_weight, down_weight)


def routed_by_exchange(flat_rows, gate_weight, up_weight, down_weight, count, pairs):
    rows, model_width = flat_rows.shape
    columns = model_width // (2 * pairs)
    gate = jnp.dot(flat_rows, gate_weight[0], preferred_element_type=jnp.float32)
    upward = jnp.dot(flat_rows, up_weight[0], preferred_element_type=jnp.float32)
    hidden = (jax.nn.silu(gate) * upward).astype(jnp.bfloat16)
    partial_value = jnp.dot(hidden, down_weight[0], preferred_element_type=jnp.float32).astype(
        jnp.bfloat16
    )
    pieces = lax.all_to_all(partial_value[None], "tp", split_axis=2, concat_axis=0, tiled=True)
    paired = pieces.reshape(pairs, 2, rows, columns).astype(jnp.float32)
    expert_value = (
        (paired[:, 0] + paired[:, 1])
        .astype(jnp.bfloat16)
        .reshape(pairs, count, rows // count, columns)
    )
    returned = lax.all_to_all(expert_value, "ep", split_axis=1, concat_axis=1, tiled=True)
    return returned.reshape(-1, columns)


def expert_half(
    expert_input_rows,
    expert_norm_gain,
    selected_expert_index,
    selected_expert_weight,
    routed_gate_weight,
    routed_up_weight,
    routed_down_weight,
    common_gate_weight,
    common_up_weight,
    common_down_weight,
):
    tok_rows, model_width = expert_input_rows.shape
    chosen_count = selected_expert_index.shape[1]
    ep_count = lax.axis_size("ep")
    tp_count = lax.axis_size("tp")
    group_count = tp_count // 2
    expert_total = group_count * ep_count
    capacity = 2 * tok_rows * chosen_count // expert_total
    column_count = model_width // tp_count
    tp_place = lax.axis_index("tp")
    group_index = tp_place // 2
    normed = rms_scale(expert_input_rows, expert_norm_gain).astype(jnp.bfloat16)
    assigned = selected_expert_index.reshape(-1)
    assign_count = assigned.shape[0]
    expert_ids = jnp.arange(expert_total, dtype=jnp.int32)
    onehot = (assigned[:, None] == expert_ids[None, :]).astype(jnp.int32)
    ranking = jnp.sum((jnp.cumsum(onehot, axis=0) - onehot) * onehot, axis=1)
    target = jnp.where(
        assigned % group_count == group_index, assigned // group_count * capacity + ranking, -1
    ).reshape(tok_rows, chosen_count)
    slots = jnp.arange(ep_count * capacity, dtype=jnp.int32)
    placing = jnp.any(target[:, :, None] == slots[None, None, :], axis=1).astype(jnp.bfloat16)
    outgoing = lax.dot_general(
        placing, normed, (((0,), (0,)), ((), ())), preferred_element_type=jnp.float32
    ).astype(jnp.bfloat16)
    arrived = lax.all_to_all(
        outgoing.reshape(ep_count, capacity, model_width),
        "ep",
        split_axis=0,
        concat_axis=0,
        tiled=True,
    ).reshape(-1, model_width)
    if capacity % 16 == 0 and column_count % 128 == 0:
        flat_back = routed_by_kernel(
            arrived, routed_gate_weight, routed_up_weight, routed_down_weight, ep_count, group_count
        ).reshape(-1, column_count)
    else:
        flat_back = routed_by_exchange(
            arrived, routed_gate_weight, routed_up_weight, routed_down_weight, ep_count, group_count
        )
    position = (
        assigned % group_count * (ep_count * capacity)
        + assigned // group_count * capacity
        + ranking
    )
    picked = (
        jnp.take(flat_back, position, axis=0)
        .astype(jnp.float32)
        .reshape(tok_rows, chosen_count, column_count)
    )
    routed = jnp.sum(picked * selected_expert_weight[:, :, None], axis=1)
    shared_hidden = (
        jax.nn.silu(jnp.dot(normed, common_gate_weight, preferred_element_type=jnp.float32))
        * jnp.dot(normed, common_up_weight, preferred_element_type=jnp.float32)
    ).astype(jnp.bfloat16)
    shared_sum = lax.psum_scatter(
        lax.dot_general(
            common_down_weight,
            shared_hidden,
            (((0,), (1,)), ((), ())),
            preferred_element_type=jnp.float32,
        ).astype(jnp.bfloat16),
        "tp",
        scatter_dimension=0,
        tiled=True,
    ).astype(jnp.float32)
    return (routed + shared_sum.T).astype(jnp.bfloat16)


def mm(x, y, dims=NN):
    return lax.dot_general(x, y, (dims, ((), ())), preferred_element_type=jnp.float32)


def pair_masks():
    lane = lax.broadcasted_iota(jnp.int32, (BLOCK, 2 * HEAD_CHANNELS), 1)
    first = jnp.where(lane < HEAD_CHANNELS, 1.0, 0.0)
    return first.astype(jnp.bfloat16), (1.0 - first).astype(jnp.bfloat16)


def stacked(y, masks):
    return jnp.concatenate([y * masks[0], y * masks[1]], axis=0)


def pair_dot(x, parts):
    xh, xl = split_parts(x)
    high, low = parts
    return mm(jnp.concatenate([xh, xl], axis=1), jnp.concatenate([high, high], axis=0)) + mm(
        xh, low
    )


def pair_parts(y, masks):
    yh, yl = split_parts(y)
    return stacked(yh, masks), stacked(yl, masks)


def side_by_side(one, two):
    return tuple(jnp.concatenate([p, q], axis=1) for p, q in zip(one, two))


def head_sum(x, block_ones):
    xh, xl = split_parts(x)
    return mm(jnp.concatenate([xh, xl], axis=1), block_ones)


def head_ones():
    wide = 2 * HEAD_CHANNELS
    row = lax.broadcasted_iota(jnp.int32, (2 * wide, wide), 0)
    col = lax.broadcasted_iota(jnp.int32, (2 * wide, wide), 1)
    same = (row // HEAD_CHANNELS) % 2 == col // HEAD_CHANNELS
    return jnp.where(same, 1.0, 0.0).astype(jnp.bfloat16)


def local_math(r_ref, k_ref, v_ref, dec_ref, lr_ref, off_ref, spike_ref):
    rows, width = r_ref.shape
    wide = 2 * HEAD_CHANNELS
    pairs = width // wide
    chunks = rows // BLOCK
    masks = pair_masks()
    ones_head = head_ones()
    row = lax.broadcasted_iota(jnp.int32, (BLOCK, wide), 0)
    col = lax.broadcasted_iota(jnp.int32, (BLOCK, wide), 1) % HEAD_CHANNELS
    strict = col < row
    inclusive = col <= row
    trow = lax.broadcasted_iota(jnp.int32, (BLOCK, 4 * BLOCK), 0)
    tcol = lax.broadcasted_iota(jnp.int32, (BLOCK, 4 * BLOCK), 1)
    running = jnp.where((tcol % BLOCK <= trow) & (tcol < 3 * BLOCK), 1.0, 0.0).astype(jnp.bfloat16)
    blank = jnp.zeros((BLOCK, wide), jnp.bfloat16)
    items = [(i, p) for i in range(chunks) for p in range(pairs)]
    lows, low_vs, out_bs, out_vs, ins_ends, b_ends, r_outs, a_ins, vs, ends = (
        [] for _ in range(10)
    )
    for i, p in items:
        span = slice(i * BLOCK, (i + 1) * BLOCK)
        lanes = slice(p * wide, (p + 1) * wide)
        r = r_ref[span, lanes].astype(jnp.float32)
        k = k_ref[span, lanes].astype(jnp.float32)
        v = v_ref[span, lanes]
        learn = jax.nn.sigmoid(lr_ref[span, lanes].astype(jnp.float32))
        pre = off_ref[:, lanes] + jnp.tanh(dec_ref[span, lanes].astype(jnp.float32))
        log = spike_ref[span, lanes] - jax.nn.sigmoid(pre) * jnp.exp(jnp.float32(-0.5))
        p0 = log.astype(jnp.bfloat16)
        rest = log - p0.astype(jnp.float32)
        p1 = rest.astype(jnp.bfloat16)
        p2 = (rest - p1.astype(jnp.float32)).astype(jnp.bfloat16)
        cum = mm(running, jnp.concatenate([p0, p1, p2, blank], axis=0))
        before = cum - log
        last = cum[BLOCK - 1 :]
        a = k * lax.rsqrt(head_sum(k * k, ones_head) + NORM_EPSILON)
        back = jnp.exp(-cum)
        end = jnp.exp(last)
        a_in = a * jnp.exp(before)
        r_out = r * jnp.exp(cum)
        b_back = a * learn * back
        ins_back = k * learn * back
        lh, ll = split_parts(jnp.concatenate([a_in, r_out], axis=0))
        bh, bl = split_parts(b_back)
        ih, il = split_parts(ins_back)
        right_high = jnp.concatenate([stacked(bh, masks), stacked(ih, masks)], axis=0)
        right_low = jnp.concatenate([stacked(bl, masks), stacked(il, masks)], axis=0)
        gram = mm(
            jnp.concatenate([lh, ll], axis=1),
            jnp.concatenate([right_high, right_high], axis=1),
            NT,
        ) + mm(lh, right_low, NT)
        lows.append(jnp.where(strict, gram[:BLOCK, :wide], 0.0))
        low_k = jnp.where(strict, gram[:BLOCK, wide:], 0.0)
        out_bs.append(jnp.where(inclusive, gram[BLOCK:, :wide], 0.0))
        out_k = jnp.where(inclusive, gram[BLOCK:, wide:], 0.0)
        kh, kl = split_parts(jnp.concatenate([low_k, out_k], axis=0))
        values = stacked(v, masks)
        weighted = mm(
            jnp.concatenate([kh, kl], axis=1), jnp.concatenate([values, values], axis=0)
        )
        low_vs.append(weighted[:BLOCK])
        out_vs.append(weighted[BLOCK:])
        ins_ends.append(ins_back * end)
        b_ends.append(b_back * end)
        r_outs.append(r_out)
        a_ins.append(a_in)
        vs.append(v)
        ends.append(end)
    count = range(len(items))
    eye = jnp.where(row == col, 1.0, 0.0)
    inverses = None
    size = 1
    while size < BLOCK:
        inside = (row // (2 * size) == col // (2 * size)) & (row // size != col // size)
        corners = [jnp.where(inside, low, 0.0) for low in lows]
        if size == 1:
            inverses = [eye - corner for corner in corners]
        else:
            firsts = [
                pair_dot(inverses[n], pair_parts(corners[n], masks)) for n in count
            ]
            inverses = [
                inverses[n] - pair_dot(firsts[n], pair_parts(inverses[n], masks)) for n in count
            ]
        size *= 2
    solved = [
        side_by_side(pair_parts(a_ins[n], masks), pair_parts(low_vs[n], masks)) for n in count
    ]
    solved = [pair_dot(inverses[n], solved[n]) for n in count]
    brow = lax.broadcasted_iota(jnp.int32, (wide, 2 * wide), 0)
    bcol = lax.broadcasted_iota(jnp.int32, (wide, 2 * wide), 1)
    same_head = brow // HEAD_CHANNELS == (bcol % wide) // HEAD_CHANNELS
    diagonal = brow == bcol
    maps = []
    for n in count:
        left = jnp.concatenate([-b_ends[n], ins_ends[n]], axis=0)
        lh, ll = split_parts(left)
        uh, ul = split_parts(solved[n])
        high = jnp.concatenate([uh, jnp.concatenate([blank, vs[n]], axis=1)], axis=0)
        low = jnp.concatenate([ul, jnp.concatenate([blank, blank], axis=1)], axis=0)
        made = mm(
            jnp.concatenate([lh, ll], axis=0), jnp.concatenate([high, high], axis=0), TN
        ) + mm(lh, low, TN)
        end = jnp.concatenate([ends[n], ends[n]], axis=1)
        maps.append(jnp.where(same_head, made + jnp.where(diagonal, end, 0.0), 0.0))
    whole = [None] * pairs
    heads_at = []
    for n in count:
        p = items[n][1]
        heads_at.append(whole[p])
        if whole[p] is None:
            whole[p] = maps[n]
        else:
            joined = pair_dot(maps[n][:, :wide], split_parts(whole[p]))
            whole[p] = jnp.concatenate(
                [joined[:, :wide], joined[:, wide:] + maps[n][:, wide:]], axis=1
            )
    compact = [m[:HEAD_CHANNELS] + m[HEAD_CHANNELS:] for m in whole]

    def finish():
        results = {}
        for n in count:
            uh, ul = split_parts(solved[n])
            parts = [
                jnp.concatenate([stacked(u[:, :wide], masks), stacked(u[:, wide:], masks)], axis=1)
                for u in (uh, ul)
            ]
            removed = pair_dot(out_bs[n], parts)
            carry = r_outs[n] - removed[:, :wide]
            value = out_vs[n] - removed[:, wide:]
            if heads_at[n] is not None:
                moved = pair_dot(carry, split_parts(heads_at[n]))
                carry = moved[:, :wide]
                value = value + moved[:, wide:]
            results[items[n]] = (carry, value)
        return results

    return compact, finish


def flipped_rows(index, bits, count):
    result, unit = 0, 1
    while unit < count:
        digit = (index // unit) % 2
        result = result + unit * ((digit + bits // unit) % 2)
        unit *= 2
    return result


def mega_kernel(ep_count, *refs):
    inputs = refs[:21]
    attn_out, expert_out = refs[21:23]
    copies = refs[23:44]
    (
        r_ref, k_ref, v_ref, dec_ref, lr_ref, gate_ref, off_ref, spike_ref, hgain_ref, wout_ref,
        pgain_ref, x_ref, egain_ref, idx_ref, wsel_ref, wg_ref, wu_ref, wd_ref, cg_ref, cu_ref,
        cd_ref,
    ) = copies
    (
        normed, outgoing, arrived, carry_ref, value_ref, own_map, held, base_state, state,
        next_state, shared, shared_half, shared_sum, shared_last, crossing,
        halves, own_ref, final, back, heads_ref, mix, mix_half, mix_sum, mix_last,
        load_sem, disp_send, disp_recv, fwd_send, fwd_recv, map_send, map_recv, base_send,
        base_recv, sh_send, sh_recv, cross_send, cross_recv, home_send, home_recv, mx_send,
        mx_recv, tail_send, tail_recv,
    ) = refs[44:]
    me = lax.axis_index("ep")
    place = lax.axis_index("tp")
    group = place // 2
    half = place % 2
    other = 1 - half
    partner = 2 * group + other
    across = 2 * (1 - group) + half
    level = me // 4
    member = me % 4
    levels = ep_count // 4
    tok_rows, model_width = x_ref.shape
    slots = outgoing.shape[0]
    capacity = slots // ep_count
    fold = model_width // 2
    columns = model_width // 4
    rows, width = r_ref.shape
    wide = 2 * HEAD_CHANNELS
    pairs = width // wide
    block_rows = rows // 4
    quarter = ep_count // 4
    outer = (level + member // 2 + 1) % 2
    first_start = quarter * (2 + outer)
    second_start = quarter * (3 - outer)
    first_batch = [first_start + n for n in range(quarter)]
    second_batch = [second_start + n for n in range(quarter)]
    near_batch = list(range(2 * quarter))

    barrier = pltpu.get_barrier_semaphore()

    def peer(bits):
        return flipped_rows(me, bits, ep_count)

    def tp_of(turn):
        return 2 * lax.rem(group + turn, 2) + half

    for bits in range(ep_count):
        for turn in range(2):
            if bits or turn:
                pl.semaphore_signal(
                    barrier,
                    inc=1,
                    device_id={"ep": peer(bits), "tp": tp_of(turn)},
                    device_id_type=MESH,
                )
    pl.semaphore_signal(barrier, inc=1, device_id={"tp": partner}, device_id_type=MESH)

    loads = [
        pltpu.make_async_copy(source, target, load_sem.at[n])
        for n, (source, target) in enumerate(zip(inputs, copies))
    ]
    for n in (11, 12, 13, 14, 0, 1, 2, 3, 4, 6, 7, 18, 19, 20, 15, 16, 17, 5, 8, 9, 10):
        loads[n].start()

    def rows_of(bits):
        if isinstance(bits, int):
            return slice(bits * capacity, (bits + 1) * capacity)
        return pl.ds(pl.multiple_of(bits * capacity, capacity), capacity)

    def remote(source, target, send, recv, where):
        return pltpu.make_async_remote_copy(
            src_ref=source,
            dst_ref=target,
            send_sem=send,
            recv_sem=recv,
            device_id=where,
            device_id_type=MESH,
        )

    def dispatch(bits):
        return remote(
            outgoing.at[rows_of(bits)],
            arrived.at[half, rows_of(bits)],
            disp_send.at[bits],
            disp_recv.at[bits],
            {"ep": peer(bits)},
        )

    def forward(bits):
        return remote(
            arrived.at[half, rows_of(bits)],
            arrived.at[half, rows_of(bits)],
            fwd_send.at[bits],
            fwd_recv.at[bits],
            {"tp": partner},
        )

    for n in (11, 12, 13, 14):
        loads[n].wait()
    normed[...] = rms_scale(x_ref[...], egain_ref[...]).astype(jnp.bfloat16)
    chosen_count = idx_ref.shape[0]
    experts = 2 * ep_count
    expert_row = lax.broadcasted_iota(jnp.int32, (experts, tok_rows), 0)
    named = [expert_row == idx_ref[k : k + 1, :] for k in range(chosen_count)]
    chosen = functools.reduce(jnp.logical_or, named)
    weight_of = functools.reduce(
        jnp.add, [jnp.where(n, wsel_ref[k : k + 1, :], 0.0) for k, n in enumerate(named)]
    )
    early = lax.broadcasted_iota(jnp.int32, (tok_rows, tok_rows), 0) < lax.broadcasted_iota(
        jnp.int32, (tok_rows, tok_rows), 1
    )
    rank = mm(
        jnp.where(chosen, 1.0, 0.0).astype(jnp.bfloat16),
        jnp.where(early, 1.0, 0.0).astype(jnp.bfloat16),
    )
    rank = jnp.where(chosen, rank, -1.0).astype(jnp.bfloat16)
    slot = lax.broadcasted_iota(jnp.int32, (slots, experts), 0)
    which = lax.broadcasted_iota(jnp.int32, (slots, experts), 1)
    there = flipped_rows(me, slot // capacity, ep_count)
    mine = jnp.where(which == 2 * there + group, 1.0, 0.0).astype(jnp.bfloat16)
    slot_rank = (
        lax.broadcasted_iota(jnp.int32, (slots, tok_rows), 0) % capacity
    ).astype(jnp.float32)
    placing = jnp.where(mm(mine, rank) == slot_rank, 1.0, 0.0).astype(jnp.bfloat16)
    fold_span = pl.ds(pl.multiple_of(half * fold, fold), fold)
    other_span = pl.ds(pl.multiple_of(other * fold, fold), fold)
    outgoing[...] = mm(placing, normed[:, fold_span]).astype(jnp.bfloat16)
    pl.semaphore_wait(barrier, 2 * ep_count)
    order = list(range(2 * quarter, ep_count)) + near_batch[1:]
    for bits in order[: 2 * quarter]:
        dispatch(bits).start()

    @pl.when(outer == 0)
    def _():
        for bits in order[2 * quarter :]:
            dispatch(bits).start()

    arrived[half, rows_of(0), :] = outgoing[rows_of(0), :]
    arrived[other, rows_of(0), :] = mm(placing[:capacity], normed[:, other_span]).astype(
        jnp.bfloat16
    )

    for n in (0, 1, 2, 3, 4, 6, 7):
        loads[n].wait()
    compact, finish = local_math(r_ref, k_ref, v_ref, dec_ref, lr_ref, off_ref, spike_ref)
    for p in range(pairs):
        own_map[p] = compact[p].astype(jnp.bfloat16)
    masks = pair_masks()

    def give(there):
        return remote(
            own_map,
            held.at[member],
            map_send.at[there],
            map_recv.at[member],
            {"ep": 4 * level + there},
        )

    def taken(source):
        return remote(
            own_map, held.at[source], map_send.at[0], map_recv.at[source], {"ep": peer(1)}
        )

    def gives(there):
        above_me = member < there
        return above_me | (member == 3) if there == 2 else above_me

    for there in (3, 2, 1):

        @pl.when(gives(there))
        def _():
            give(there).start()

    for (i, p), (carry, value) in finish().items():
        span = slice(i * BLOCK, (i + 1) * BLOCK)
        lanes = slice(p * wide, (p + 1) * wide)
        carry_ref[span, lanes] = carry
        value_ref[span, lanes] = value

    for n in (18, 19, 20):
        loads[n].wait()
    rows_in = normed[...]
    hidden = (jax.nn.silu(mm(rows_in, cg_ref[...])) * mm(rows_in, cu_ref[...])).astype(
        jnp.bfloat16
    )
    for j in range(4):
        shared[j] = mm(hidden, cd_ref[:, j * columns : (j + 1) * columns]).astype(jnp.bfloat16)

    def shared_cross(turn):
        there = 2 * lax.rem(group + turn, 2) + other
        return remote(
            shared.at[there],
            shared_half.at[turn],
            sh_send.at[turn],
            sh_recv.at[turn],
            {"tp": partner},
        )

    for turn in (1, 0):
        shared_cross(turn).start()

    def take_in(batch):
        for bits in batch:
            if not isinstance(bits, int) or bits:
                dispatch(bits).wait_recv()
                forward(bits).start()

    take_in(first_batch)

    @pl.when(outer == 1)
    def _():
        for bits in order[2 * quarter :]:
            dispatch(bits).start()

    def wait_far(batch):
        for bits in batch:
            if not isinstance(bits, int) or bits:
                forward(bits).wait_recv()

    def cross(batch_index, turn, span):
        return remote(
            crossing.at[turn, span],
            halves.at[turn, span],
            cross_send.at[batch_index, turn],
            cross_recv.at[batch_index, turn],
            {"tp": partner},
        )

    def home(turn, bits):
        return remote(
            final.at[turn, rows_of(bits)],
            back.at[group, rows_of(bits)],
            home_send.at[turn, bits],
            home_recv.at[turn, bits],
            {"ep": peer(bits), "tp": tp_of(turn)},
        )

    def span_of(batch):
        if isinstance(batch[0], int):
            return slice(0, len(batch) * capacity)
        size = quarter * capacity
        return pl.ds(pl.multiple_of(batch[0] * capacity, size), size)

    def feed(batch_index, batch):
        span = span_of(batch)
        near, away = arrived[0, span, :], arrived[1, span, :]
        gate = mm(near, wg_ref[:fold, :]) + mm(away, wg_ref[fold:, :])
        upper = mm(near, wu_ref[:fold, :]) + mm(away, wu_ref[fold:, :])
        routed_hidden = (jax.nn.silu(gate) * upper).astype(jnp.bfloat16)

        def part(index):
            lanes = pl.ds(pl.multiple_of(index * columns, columns), columns)
            return mm(routed_hidden, wd_ref[:, lanes])

        for turn in (1, 0):
            crossing[turn, span, :] = part(2 * lax.rem(group + turn, 2) + other).astype(
                jnp.bfloat16
            )
            cross(batch_index, turn, span).start()
        for turn in (1, 0):
            own_ref[turn, span, :] = part(2 * lax.rem(group + turn, 2) + half)

    def send_home(batch_index, batch):
        span = span_of(batch)
        for turn in (1, 0):
            cross(batch_index, turn, span).wait_recv()
            final[turn, span, :] = (
                own_ref[turn, span, :] + halves[turn, span, :].astype(jnp.float32)
            ).astype(jnp.bfloat16)
            for bits in batch:
                if not isinstance(bits, int) or bits or turn:
                    home(turn, bits).start()
                else:
                    back[group, rows_of(0), :] = final[0, rows_of(0), :]

    for n in (15, 16, 17):
        loads[n].wait()
    wait_far(first_batch)
    feed(0, first_batch)
    for turn in (1, 0):
        shared_cross(turn).wait_recv()
        shared_sum[turn] = shared[tp_of(turn)].astype(jnp.float32) + shared_half[turn].astype(
            jnp.float32
        )
    shared_last[0] = shared_sum[1].astype(jnp.bfloat16)
    shared_tail = remote(
        shared_last.at[0], shared_last.at[1], tail_send.at[0], tail_recv.at[0], {"tp": across}
    )
    shared_tail.start()
    def moved_by(block, p, current):
        through = block[p, :, :wide]
        high, low = pair_parts(current, masks)
        return mm(
            jnp.concatenate([through, through], axis=1), jnp.concatenate([high, low], axis=0)
        ) + block[p, :, wide:].astype(jnp.float32)

    def above(turn):
        return remote(
            next_state,
            base_state,
            base_send.at[turn],
            base_recv.at[0],
            {"ep": lax.rem(4 * (level + 1) + 2 * turn + member % 2, ep_count)},
        )

    hands_on = (member >= 2) & (level + 1 < levels)

    def settle():
        for p in range(pairs):
            state[p] = base_state[p].astype(jnp.float32)
        for source in range(3):

            @pl.when(source < member)
            def _():
                taken(source).wait_recv()
                for p in range(pairs):
                    state[p] = moved_by(held.at[source], p, state[p])

        @pl.when(member == 2)
        def _():
            taken(3).wait_recv()

        @pl.when(hands_on)
        def _():
            for p in range(pairs):
                once = moved_by(own_map, p, state[p])
                twice = moved_by(held.at[3], p, once)
                next_state[p] = jnp.where(member == 2, twice, once).astype(jnp.bfloat16)
            for turn in range(2):
                above(turn).start()

    @pl.when(level == 0)
    def _():
        base_state[...] = jnp.zeros_like(base_state)
        settle()

    send_home(0, first_batch)
    for n in (5, 8, 9, 10):
        loads[n].wait()

    def mix_cross(turn):
        there = 2 * lax.rem(group + turn, 2) + other
        return remote(
            mix.at[there],
            mix_half.at[turn],
            mx_send.at[turn],
            mx_recv.at[turn],
            {"tp": partner},
        )

    def project(turn):
        there = lax.rem(group + turn, 2)
        rows_there = pl.ds(pl.multiple_of(there * 2 * block_rows, 2 * block_rows), 2 * block_rows)
        rows_made = heads_ref[rows_there, :]
        for j in range(4):
            span = slice(j * columns, (j + 1) * columns)
            made = mm(rows_made, wout_ref[:, span]).astype(jnp.bfloat16)
            for b in range(2):
                mix[2 * there + b, :, span] = made[b * block_rows : (b + 1) * block_rows]

    def attend():
        ones_head = head_ones()
        for p in range(pairs):
            lanes = slice(p * wide, (p + 1) * wide)
            value = value_ref[:, lanes] + pair_dot(
                carry_ref[:, lanes], pair_parts(state[p], masks)
            )
            centred = value - head_sum(value, ones_head) * (1.0 / HEAD_CHANNELS)
            spread = head_sum(centred * centred, ones_head) * (1.0 / HEAD_CHANNELS)
            heads_ref[:, lanes] = (
                centred
                * lax.rsqrt(spread + GROUP_EPSILON)
                * hgain_ref[:, lanes]
                * jax.nn.sigmoid(gate_ref[:, lanes].astype(jnp.float32))
            ).astype(jnp.bfloat16)
        for turn in (1, 0):
            project(turn)
            mix_cross(turn).start()

    mix_tail = remote(
        mix_last.at[0], mix_last.at[1], tail_send.at[1], tail_recv.at[1], {"tp": across}
    )

    def pass_mix():
        mix_cross(1).wait_recv()
        mix_last[0] = (
            mix[across].astype(jnp.float32) + mix_half[1].astype(jnp.float32)
        ).astype(jnp.bfloat16)
        mix_tail.start()

    @pl.when(level == 0)
    def _():
        attend()

    take_in(near_batch)
    wait_far(near_batch)
    @pl.when(level == 0)
    def _():
        pass_mix()

    feed(1, near_batch)
    take_in(second_batch)
    send_home(1, near_batch)

    @pl.when(level > 0)
    def _():
        above(0).wait_recv()
        settle()

    @pl.when(level > 0)
    def _():
        attend()

    wait_far(second_batch)
    feed(2, second_batch)
    @pl.when(level > 0)
    def _():
        pass_mix()

    send_home(2, second_batch)
    mix_cross(0).wait_recv()
    mix_sum[...] = mix[place].astype(jnp.float32) + mix_half[0].astype(jnp.float32)

    all_slots = 2 * slots
    slot = lax.broadcasted_iota(jnp.int32, (experts, all_slots), 1)
    which = lax.broadcasted_iota(jnp.int32, (experts, all_slots), 0)
    there = flipped_rows(me, (slot % slots) // capacity, ep_count)
    holder = jnp.where(which == 2 * there + slot // slots, 1.0, 0.0).astype(jnp.bfloat16)
    slot_rank = (
        lax.broadcasted_iota(jnp.int32, (tok_rows, all_slots), 1) % capacity
    ).astype(jnp.float32)
    hit = mm(rank, holder, TN) == slot_rank
    weight_high, weight_low = split_parts(weight_of)
    picks = [
        jnp.where(hit, mm(w, holder, TN), 0.0).astype(jnp.bfloat16)
        for w in (weight_high, weight_low)
    ]
    shared_tail.wait_recv()
    base = shared_sum[0] + shared_last[1].astype(jnp.float32)
    for batch in (first_batch, near_batch, second_batch):
        for turn in range(2):
            for bits in batch:
                if not isinstance(bits, int) or bits or turn:
                    home(turn, bits).wait_recv()
    returned = back[...].reshape(all_slots, columns)
    routed = mm(
        jnp.concatenate(picks, axis=1), jnp.concatenate([returned, returned], axis=0)
    )
    expert_out[...] = (routed + base).astype(jnp.bfloat16)

    mix_tail.wait_recv()
    total = mix_sum[...] + mix_last[1].astype(jnp.float32)
    attn_out[...] = rms_scale(total, pgain_ref[...]).astype(jnp.bfloat16)

    for bits in order:
        dispatch(bits).wait_send()
        forward(bits).wait_send()
    for there in (3, 2, 1):

        @pl.when(gives(there))
        def _():
            give(there).wait_send()

    @pl.when(hands_on)
    def _():
        for turn in range(2):
            above(turn).wait_send()

    for turn in range(2):
        shared_cross(turn).wait_send()
        mix_cross(turn).wait_send()
        for n, batch in enumerate((first_batch, near_batch, second_batch)):
            cross(n, turn, span_of(batch)).wait_send()
        for bits in range(ep_count):
            if bits or turn:
                home(turn, bits).wait_send()
    shared_tail.wait_send()
    mix_tail.wait_send()


def mega(
    receptance, head_key_input, head_value_input, decay_input_part, learning_rate_input,
    output_gate_input, decay_channel_offset, spike_log_decay, head_norm_gain, head_output_weight,
    projection_norm_gain, expert_input_rows, expert_norm_gain, selected_expert_index,
    selected_expert_weight, routed_gate_weight, routed_up_weight, routed_down_weight,
    common_gate_weight, common_up_weight, common_down_weight,
):
    ep_count = lax.axis_size("ep")
    rows, width = receptance.shape
    tok_rows, model_width = expert_input_rows.shape
    chosen = selected_expert_index.shape[1]
    capacity = tok_rows * chosen // ep_count
    slots = ep_count * capacity
    columns = model_width // 4
    wide = 2 * HEAD_CHANNELS
    pairs = width // wide
    operands = (
        receptance, head_key_input, head_value_input, decay_input_part, learning_rate_input,
        output_gate_input, decay_channel_offset[None, :], spike_log_decay, head_norm_gain[None, :],
        head_output_weight, projection_norm_gain[None, :], expert_input_rows,
        expert_norm_gain[None, :], selected_expert_index.T, selected_expert_weight.T,
        routed_gate_weight[0], routed_up_weight[0], routed_down_weight[0], common_gate_weight,
        common_up_weight, common_down_weight,
    )
    bf16, f32 = jnp.bfloat16, jnp.float32
    dma = pltpu.SemaphoreType.DMA
    scratch = [pltpu.VMEM(o.shape, o.dtype) for o in operands] + [
        pltpu.VMEM((tok_rows, model_width), bf16),
        pltpu.VMEM((slots, model_width // 2), bf16),
        pltpu.VMEM((2, slots, model_width // 2), bf16),
        pltpu.VMEM((rows, width), f32),
        pltpu.VMEM((rows, width), f32),
        pltpu.VMEM((pairs, HEAD_CHANNELS, 2 * wide), bf16),
        pltpu.VMEM((4, pairs, HEAD_CHANNELS, 2 * wide), bf16),
        pltpu.VMEM((pairs, HEAD_CHANNELS, wide), bf16),
        pltpu.VMEM((pairs, HEAD_CHANNELS, wide), f32),
        pltpu.VMEM((pairs, HEAD_CHANNELS, wide), bf16),
        pltpu.VMEM((4, tok_rows, columns), bf16),
        pltpu.VMEM((2, tok_rows, columns), bf16),
        pltpu.VMEM((2, tok_rows, columns), f32),
        pltpu.VMEM((2, tok_rows, columns), bf16),
        pltpu.VMEM((2, slots, columns), bf16),
        pltpu.VMEM((2, slots, columns), bf16),
        pltpu.VMEM((2, slots, columns), f32),
        pltpu.VMEM((2, slots, columns), bf16),
        pltpu.VMEM((2, slots, columns), bf16),
        pltpu.VMEM((rows, width), bf16),
        pltpu.VMEM((4, rows // 4, model_width), bf16),
        pltpu.VMEM((2, rows // 4, model_width), bf16),
        pltpu.VMEM((rows // 4, model_width), f32),
        pltpu.VMEM((2, rows // 4, model_width), bf16),
        dma((len(operands),)),
    ]
    scratch += [dma((ep_count,))] * 4
    scratch += [dma((4,))] * 2
    scratch += [dma((2,))] * 4
    scratch += [dma((3, 2))] * 2
    scratch += [dma((2, ep_count))] * 2
    scratch += [dma((2,))] * 4
    full = pl.BlockSpec(memory_space=pltpu.VMEM)
    return pl.pallas_call(
        functools.partial(mega_kernel, ep_count),
        out_shape=(
            jax.ShapeDtypeStruct((rows // 4, model_width), bf16),
            jax.ShapeDtypeStruct((tok_rows, columns), bf16),
        ),
        in_specs=[pl.BlockSpec(memory_space=pl.ANY)] * len(operands),
        out_specs=(full, full),
        scratch_shapes=scratch,
        compiler_params=pltpu.CompilerParams(collective_id=0, has_side_effects=True),
    )(*operands)


def fits_mega(receptance, expert_input_rows, selected_expert_index):
    ep_count = lax.axis_size("ep")
    rows, width = receptance.shape
    tok_rows, model_width = expert_input_rows.shape
    assigned = tok_rows * selected_expert_index.shape[1]
    return (
        lax.axis_size("tp") == 4
        and ep_count >= 4
        and ep_count & (ep_count - 1) == 0
        and width % (2 * HEAD_CHANNELS) == 0
        and rows % (4 * BLOCK) == 0
        and assigned % (16 * ep_count) == 0
        and tok_rows % 128 == 0
        and tok_rows <= 256
        and model_width % 512 == 0
    )


def body(
    receptance,
    head_key_input,
    head_value_input,
    decay_input_part,
    learning_rate_input,
    output_gate_input,
    decay_channel_offset,
    spike_log_decay,
    head_norm_gain,
    head_output_weight,
    projection_norm_gain,
    expert_input_rows,
    expert_norm_gain,
    selected_expert_index,
    selected_expert_weight,
    routed_gate_weight,
    routed_up_weight,
    routed_down_weight,
    common_gate_weight,
    common_up_weight,
    common_down_weight,
):
    if fits_mega(receptance, expert_input_rows, selected_expert_index):
        return mega(
            receptance, head_key_input, head_value_input, decay_input_part, learning_rate_input,
            output_gate_input, decay_channel_offset, spike_log_decay, head_norm_gain,
            head_output_weight, projection_norm_gain, expert_input_rows, expert_norm_gain,
            selected_expert_index, selected_expert_weight, routed_gate_weight, routed_up_weight,
            routed_down_weight, common_gate_weight, common_up_weight, common_down_weight,
        )
    attention_output = attention_mixer(
        receptance,
        head_key_input,
        head_value_input,
        decay_input_part,
        learning_rate_input,
        output_gate_input,
        decay_channel_offset,
        spike_log_decay,
        head_norm_gain,
        head_output_weight,
        projection_norm_gain,
    )
    expert_output = expert_half(
        expert_input_rows,
        expert_norm_gain,
        selected_expert_index,
        selected_expert_weight,
        routed_gate_weight,
        routed_up_weight,
        routed_down_weight,
        common_gate_weight,
        common_up_weight,
        common_down_weight,
    )
    return (attention_output, expert_output)


def solution(mesh):
    placed = (
        P("ep", "tp"),
        P("ep", "tp"),
        P("ep", "tp"),
        P("ep", "tp"),
        P("ep", "tp"),
        P("ep", "tp"),
        P("tp"),
        P("ep", "tp"),
        P("tp"),
        P("tp", None),
        P(),
        P("ep", None),
        P(),
        P("ep", None),
        P("ep", None),
        P(("ep", "tp"), None, None),
        P(("ep", "tp"), None, None),
        P(("ep", "tp"), None, None),
        P(None, "tp"),
        P(None, "tp"),
        P("tp", None),
    )
    return jax.shard_map(
        body,
        mesh=mesh,
        in_specs=placed,
        out_specs=(P(("ep", "tp"), None), P("ep", "tp")),
        check_vma=False,
    )
```

```python
import functools

import jax
import jax.numpy as jnp
from jax import lax
from jax.experimental import pallas as pl
from jax.experimental.pallas import tpu as pltpu
from jax.sharding import PartitionSpec as P

HEAD_CHANNELS = 64
BLOCK = 64


MESH = pl.DeviceIdType.MESH
NORM_EPSILON = 1e-06
GROUP_EPSILON = 0.00064


def rms_scale(values, gain):
    values = values.astype(jnp.float32)
    return (
        values * lax.rsqrt(jnp.mean(values * values, axis=-1, keepdims=True) + NORM_EPSILON) * gain
    )


def split_parts(x):
    high = x.astype(jnp.bfloat16)
    return high, (x - high.astype(jnp.float32)).astype(jnp.bfloat16)


def dot3(x, y, dims):
    xh, xl = split_parts(x)
    yh, yl = split_parts(y)

    def one(p, q):
        return lax.dot_general(p, q, (dims, ((), ())), preferred_element_type=jnp.float32)

    return one(xh, yh) + (one(xh, yl) + one(xl, yh))


NN = ((1,), (0,))
NT = ((1,), (1,))
TN = ((0,), (0,))


def local_kernel(
    r_ref, k_ref, v_ref, dec_ref, lr_ref, off_ref, spike_ref, out_ref, carry_ref, map_ref
):
    rows, width = r_ref.shape
    heads = width // HEAD_CHANNELS
    blocks = rows // BLOCK
    row = lax.broadcasted_iota(jnp.int32, (rows, rows), 0)
    col = lax.broadcasted_iota(jnp.int32, (rows, rows), 1)
    strict = col < row
    inclusive = col <= row
    learn_all = jax.nn.sigmoid(lr_ref[...].astype(jnp.float32))
    pre = off_ref[...] + jnp.tanh(dec_ref[...].astype(jnp.float32))
    log_all = spike_ref[...] - jax.nn.sigmoid(pre) * jnp.exp(jnp.float32(-0.5))
    ones = jnp.where(inclusive, 1.0, 0.0).astype(jnp.bfloat16)
    p0 = log_all.astype(jnp.bfloat16)
    rest = log_all - p0.astype(jnp.float32)
    p1 = rest.astype(jnp.bfloat16)
    p2 = (rest - p1.astype(jnp.float32)).astype(jnp.bfloat16)
    cum_all = sum(jnp.dot(ones, p, preferred_element_type=jnp.float32) for p in (p0, p1, p2))
    before_all = cum_all - log_all
    for h in range(heads):
        lanes = slice(h * HEAD_CHANNELS, (h + 1) * HEAD_CHANNELS)
        r = r_ref[:, lanes].astype(jnp.float32)
        k = k_ref[:, lanes].astype(jnp.float32)
        v = v_ref[:, lanes].astype(jnp.float32)
        learn = learn_all[:, lanes]
        cum = cum_all[:, lanes]
        before = before_all[:, lanes]
        a = k * lax.rsqrt(jnp.sum(k * k, axis=-1, keepdims=True) + NORM_EPSILON)
        b = a * learn
        ins = k * learn
        parts = []
        for i in range(blocks):
            span = slice(i * BLOCK, (i + 1) * BLOCK)
            base = before[i * BLOCK : i * BLOCK + 1]
            left = jnp.concatenate(
                [a[span] * jnp.exp(before[span] - base), r[span] * jnp.exp(cum[span] - base)],
                axis=0,
            )
            back = jnp.exp(jnp.minimum(base - cum, 60.0))
            right = jnp.concatenate([b * back, ins * back], axis=0)
            parts.append(dot3(left, right, NT))
        low_b = jnp.where(strict, jnp.concatenate([p[:BLOCK, :rows] for p in parts], axis=0), 0.0)
        low_k = jnp.where(strict, jnp.concatenate([p[:BLOCK, rows:] for p in parts], axis=0), 0.0)
        out_b = jnp.where(
            inclusive, jnp.concatenate([p[BLOCK:, :rows] for p in parts], axis=0), 0.0
        )
        out_k = jnp.where(
            inclusive, jnp.concatenate([p[BLOCK:, rows:] for p in parts], axis=0), 0.0
        )
        inverse = jnp.where(row == col, 1.0, 0.0)
        size = 1
        while size < BLOCK:
            corner = (row // (2 * size) == col // (2 * size)) & (row // size != col // size)
            corner = jnp.where(corner, low_b, 0.0)
            if size == 1:
                inverse = inverse - corner
            else:
                inverse = inverse - dot3(dot3(inverse, corner, NN), inverse, NN)
            size *= 2
        right_side = jnp.concatenate([a * jnp.exp(before), dot3(low_k, v, NN)], axis=1)
        solved = []
        for i in range(blocks):
            span = slice(i * BLOCK, (i + 1) * BLOCK)
            piece = right_side[span]
            if i:
                piece = piece - dot3(
                    low_b[span, : i * BLOCK], jnp.concatenate(solved, axis=0), NN
                )
            solved.append(dot3(inverse[span, span], piece, NN))
        solved = jnp.concatenate(solved, axis=0)
        removed = dot3(out_b, solved, NN)
        out_ref[:, lanes] = dot3(out_k, v, NN) - removed[:, HEAD_CHANNELS:]
        carry_ref[:, lanes] = r * jnp.exp(cum) - removed[:, :HEAD_CHANNELS]
        last = cum[rows - 1 :]
        to_end = jnp.exp(last - cum)
        taken = dot3(solved, b * to_end, TN)
        added = dot3(v, ins * to_end, TN)
        small = (HEAD_CHANNELS, HEAD_CHANNELS)
        eye = lax.broadcasted_iota(jnp.int32, small, 0) == lax.broadcasted_iota(jnp.int32, small, 1)
        through = jnp.where(eye, jnp.exp(last), 0.0) - taken[:HEAD_CHANNELS]
        fresh = added - taken[HEAD_CHANNELS:]
        map_ref[lanes, :] = jnp.concatenate([through, fresh], axis=1).astype(jnp.bfloat16)


def join_kernel(
    count, out_ref, carry_ref, map_ref, gain_ref, gate_ref, weight_ref, mix_ref, held, state,
    send_sem, recv_sem
):
    me = lax.axis_index("ep")
    rows, width = out_ref.shape
    heads = width // HEAD_CHANNELS
    barrier = pltpu.get_barrier_semaphore()
    for step in range(1, count):
        pl.semaphore_signal(
            barrier, inc=1, device_id={"ep": lax.rem(me + step, count)}, device_id_type=MESH
        )
    pl.semaphore_wait(barrier, count - 1)

    def copy(slot, step):
        return pltpu.make_async_remote_copy(
            src_ref=map_ref,
            dst_ref=held.at[slot],
            send_sem=send_sem.at[step],
            recv_sem=recv_sem.at[slot],
            device_id={"ep": lax.rem(me + step, count)},
            device_id_type=MESH,
        )

    for step in range(1, count):

        @pl.when(me + step < count)
        def _():
            copy(me, step).start()

    state[...] = jnp.zeros_like(state)

    def one(turn, _):
        copy(turn, 1).wait_recv()
        for h in range(heads):
            lanes = slice(h * HEAD_CHANNELS, (h + 1) * HEAD_CHANNELS)
            block = held[turn, lanes, :]
            high, low = split_parts(state[lanes, :])
            through = block[:, :HEAD_CHANNELS]
            state[lanes, :] = (
                jnp.dot(high, through, preferred_element_type=jnp.float32)
                + jnp.dot(low, through, preferred_element_type=jnp.float32)
                + block[:, HEAD_CHANNELS:].astype(jnp.float32)
            )
        return 0

    lax.fori_loop(0, me, one, 0)
    normed = []
    for h in range(heads):
        lanes = slice(h * HEAD_CHANNELS, (h + 1) * HEAD_CHANNELS)
        value = out_ref[:, lanes] + dot3(carry_ref[:, lanes], state[lanes, :], NT)
        centred = value - jnp.mean(value, axis=-1, keepdims=True)
        normed.append(
            centred
            * lax.rsqrt(jnp.mean(centred * centred, axis=-1, keepdims=True) + GROUP_EPSILON)
        )
    flat = normed[0] if heads == 1 else jnp.concatenate(normed, axis=1)
    heads_out = flat * gain_ref[...] * jax.nn.sigmoid(gate_ref[...].astype(jnp.float32))
    mix_ref[...] = jnp.dot(
        heads_out.astype(jnp.bfloat16), weight_ref[...], preferred_element_type=jnp.float32
    ).astype(jnp.bfloat16)
    for step in range(1, count):

        @pl.when(me + step < count)
        def _():
            copy(me, step).wait_send()


def attention_mixer(
    receptance,
    head_key_input,
    head_value_input,
    decay_input_part,
    learning_rate_input,
    output_gate_input,
    decay_channel_offset,
    spike_log_decay,
    head_norm_gain,
    head_output_weight,
    projection_norm_gain,
):
    rows, width = receptance.shape
    count = lax.axis_size("ep")
    full = pl.BlockSpec(memory_space=pltpu.VMEM)
    out, carry, maps = pl.pallas_call(
        local_kernel,
        out_shape=(
            jax.ShapeDtypeStruct((rows, width), jnp.float32),
            jax.ShapeDtypeStruct((rows, width), jnp.float32),
            jax.ShapeDtypeStruct((width, 2 * HEAD_CHANNELS), jnp.bfloat16),
        ),
        in_specs=[full] * 7,
        out_specs=(full, full, full),
        cost_estimate=pl.CostEstimate(
            flops=rows * rows * width * 200, bytes_accessed=rows * width * 22, transcendentals=0
        ),
    )(
        receptance,
        head_key_input,
        head_value_input,
        decay_input_part,
        learning_rate_input,
        decay_channel_offset[None, :],
        spike_log_decay,
    )
    model_width = head_output_weight.shape[1]
    mix = pl.pallas_call(
        functools.partial(join_kernel, count),
        out_shape=jax.ShapeDtypeStruct((rows, model_width), jnp.bfloat16),
        in_specs=[full] * 6,
        out_specs=full,
        scratch_shapes=[
            pltpu.VMEM((count, width, 2 * HEAD_CHANNELS), jnp.bfloat16),
            pltpu.VMEM((width, HEAD_CHANNELS), jnp.float32),
            pltpu.SemaphoreType.DMA((count,)),
            pltpu.SemaphoreType.DMA((count,)),
        ],
        compiler_params=pltpu.CompilerParams(collective_id=0, has_side_effects=True),
        cost_estimate=pl.CostEstimate(
            flops=rows * width * model_width * 20,
            bytes_accessed=width * model_width * 2,
            transcendentals=0,
        ),
    )(out, carry, maps, head_norm_gain[None, :], output_gate_input, head_output_weight)
    mix_sum = lax.psum_scatter(mix, "tp", scatter_dimension=0, tiled=True).astype(jnp.float32)
    return rms_scale(mix_sum, projection_norm_gain).astype(jnp.bfloat16)


def expert_kernel(
    count, pairs, arrived, gate_ref, up_ref, down_ref, result_ref, crossing, halves, paired,
    final, back, half_send, half_recv, pair_send, pair_recv, back_send, back_recv
):
    me = lax.axis_index("ep")
    place = lax.axis_index("tp")
    group = place // 2
    half = place % 2
    capacity = arrived.shape[0] // count
    columns = final.shape[2]
    partner = 2 * group + 1 - half

    def rows_of(index):
        return pl.ds(pl.multiple_of(index * capacity, capacity), capacity)

    def peer(step):
        return lax.rem(me + step, count)

    barrier = pltpu.get_barrier_semaphore()
    for step in range(1, count):
        pl.semaphore_signal(barrier, inc=1, device_id={"ep": peer(step)}, device_id_type=MESH)
    pl.semaphore_signal(barrier, inc=1, device_id={"tp": partner}, device_id_type=MESH)
    for step in range(1, pairs):
        there = 2 * lax.rem(group + step, pairs) + half
        pl.semaphore_signal(barrier, inc=1, device_id={"tp": there}, device_id_type=MESH)
    pl.semaphore_wait(barrier, count + pairs - 1)

    def cross(index):
        return pltpu.make_async_remote_copy(
            src_ref=crossing.at[index],
            dst_ref=halves.at[index],
            send_sem=half_send.at[index],
            recv_sem=half_recv.at[index],
            device_id={"tp": partner},
            device_id_type=MESH,
        )

    def pair(step):
        return pltpu.make_async_remote_copy(
            src_ref=paired.at[step],
            dst_ref=final.at[step],
            send_sem=pair_send.at[step],
            recv_sem=pair_recv.at[step],
            device_id={"tp": 2 * lax.rem(group + step, pairs) + half},
            device_id_type=MESH,
        )

    def home(turn, step):
        return pltpu.make_async_remote_copy(
            src_ref=final.at[turn, rows_of(peer(step))],
            dst_ref=back.at[turn, rows_of(me)],
            send_sem=back_send.at[turn, step],
            recv_sem=back_recv.at[turn, step],
            device_id={"ep": peer(step)},
            device_id_type=MESH,
        )

    rows = arrived[...]
    gate = jnp.dot(rows, gate_ref[0], preferred_element_type=jnp.float32)
    upward = jnp.dot(rows, up_ref[0], preferred_element_type=jnp.float32)
    hidden = (jax.nn.silu(gate) * upward).astype(jnp.bfloat16)

    def part(index):
        span = pl.ds(pl.multiple_of(index * columns, columns), columns)
        return jnp.dot(hidden, down_ref[0, :, span], preferred_element_type=jnp.float32).astype(
            jnp.bfloat16
        )

    order = list(range(1, pairs)) + [0]
    for step in order:
        crossing[step] = part(2 * lax.rem(group + step, pairs) + 1 - half)
        cross(step).start()
    own = {step: part(2 * lax.rem(group + step, pairs) + half) for step in order}
    for step in order:
        cross(step).wait_recv()
        total = (
            own[step].astype(jnp.float32) + halves[step].astype(jnp.float32)
        ).astype(jnp.bfloat16)
        if step:
            paired[step] = total
            pair(step).start()
        else:
            final[0] = total
    for turn in range(pairs):
        if turn:
            pair(turn).wait_recv()
        for step in range(1, count):
            home(turn, step).start()
        back[turn, rows_of(me), :] = final[turn, rows_of(me), :]
    for turn in range(pairs):
        for step in range(1, count):
            home(turn, step).wait_recv()
        result_ref[lax.rem(group + pairs - turn, pairs)] = back[turn]
    for step in order:
        cross(step).wait_send()
        if step:
            pair(step).wait_send()
    for turn in range(pairs):
        for step in range(1, count):
            home(turn, step).wait_send()


def routed_by_kernel(arrived, gate_weight, up_weight, down_weight, count, pairs):
    rows, model_width = arrived.shape
    columns = model_width // (2 * pairs)
    full = pl.BlockSpec(memory_space=pltpu.VMEM)
    dma = pltpu.SemaphoreType.DMA
    block = pltpu.VMEM((pairs, rows, columns), jnp.bfloat16)
    return pl.pallas_call(
        functools.partial(expert_kernel, count, pairs),
        out_shape=jax.ShapeDtypeStruct((pairs, rows, columns), jnp.bfloat16),
        in_specs=[full] * 4,
        out_specs=full,
        scratch_shapes=[block] * 5
        + [dma((pairs,))] * 4
        + [dma((pairs, count))] * 2,
        compiler_params=pltpu.CompilerParams(collective_id=1, has_side_effects=True),
        cost_estimate=pl.CostEstimate(
            flops=10 * rows * model_width * gate_weight.shape[2] * 6,
            bytes_accessed=model_width * gate_weight.shape[2] * 6,
            transcendentals=0,
        ),
    )(arrived, gate_weight, up_weight, down_weight)


def routed_by_exchange(flat_rows, gate_weight, up_weight, down_weight, count, pairs):
    rows, model_width = flat_rows.shape
    columns = model_width // (2 * pairs)
    gate = jnp.dot(flat_rows, gate_weight[0], preferred_element_type=jnp.float32)
    upward = jnp.dot(flat_rows, up_weight[0], preferred_element_type=jnp.float32)
    hidden = (jax.nn.silu(gate) * upward).astype(jnp.bfloat16)
    partial_value = jnp.dot(hidden, down_weight[0], preferred_element_type=jnp.float32).astype(
        jnp.bfloat16
    )
    pieces = lax.all_to_all(partial_value[None], "tp", split_axis=2, concat_axis=0, tiled=True)
    paired = pieces.reshape(pairs, 2, rows, columns).astype(jnp.float32)
    expert_value = (
        (paired[:, 0] + paired[:, 1])
        .astype(jnp.bfloat16)
        .reshape(pairs, count, rows // count, columns)
    )
    returned = lax.all_to_all(expert_value, "ep", split_axis=1, concat_axis=1, tiled=True)
    return returned.reshape(-1, columns)


def expert_half(
    expert_input_rows,
    expert_norm_gain,
    selected_expert_index,
    selected_expert_weight,
    routed_gate_weight,
    routed_up_weight,
    routed_down_weight,
    common_gate_weight,
    common_up_weight,
    common_down_weight,
):
    tok_rows, model_width = expert_input_rows.shape
    chosen_count = selected_expert_index.shape[1]
    ep_count = lax.axis_size("ep")
    tp_count = lax.axis_size("tp")
    group_count = tp_count // 2
    expert_total = group_count * ep_count
    capacity = 2 * tok_rows * chosen_count // expert_total
    column_count = model_width // tp_count
    tp_place = lax.axis_index("tp")
    group_index = tp_place // 2
    normed = rms_scale(expert_input_rows, expert_norm_gain).astype(jnp.bfloat16)
    assigned = selected_expert_index.reshape(-1)
    assign_count = assigned.shape[0]
    expert_ids = jnp.arange(expert_total, dtype=jnp.int32)
    onehot = (assigned[:, None] == expert_ids[None, :]).astype(jnp.int32)
    ranking = jnp.sum((jnp.cumsum(onehot, axis=0) - onehot) * onehot, axis=1)
    target = jnp.where(
        assigned % group_count == group_index, assigned // group_count * capacity + ranking, -1
    ).reshape(tok_rows, chosen_count)
    slots = jnp.arange(ep_count * capacity, dtype=jnp.int32)
    placing = jnp.any(target[:, :, None] == slots[None, None, :], axis=1).astype(jnp.bfloat16)
    outgoing = lax.dot_general(
        placing, normed, (((0,), (0,)), ((), ())), preferred_element_type=jnp.float32
    ).astype(jnp.bfloat16)
    arrived = lax.all_to_all(
        outgoing.reshape(ep_count, capacity, model_width),
        "ep",
        split_axis=0,
        concat_axis=0,
        tiled=True,
    ).reshape(-1, model_width)
    if capacity % 16 == 0 and column_count % 128 == 0:
        flat_back = routed_by_kernel(
            arrived, routed_gate_weight, routed_up_weight, routed_down_weight, ep_count, group_count
        ).reshape(-1, column_count)
    else:
        flat_back = routed_by_exchange(
            arrived, routed_gate_weight, routed_up_weight, routed_down_weight, ep_count, group_count
        )
    position = (
        assigned % group_count * (ep_count * capacity)
        + assigned // group_count * capacity
        + ranking
    )
    picked = (
        jnp.take(flat_back, position, axis=0)
        .astype(jnp.float32)
        .reshape(tok_rows, chosen_count, column_count)
    )
    routed = jnp.sum(picked * selected_expert_weight[:, :, None], axis=1)
    shared_hidden = (
        jax.nn.silu(jnp.dot(normed, common_gate_weight, preferred_element_type=jnp.float32))
        * jnp.dot(normed, common_up_weight, preferred_element_type=jnp.float32)
    ).astype(jnp.bfloat16)
    shared_sum = lax.psum_scatter(
        lax.dot_general(
            common_down_weight,
            shared_hidden,
            (((0,), (1,)), ((), ())),
            preferred_element_type=jnp.float32,
        ).astype(jnp.bfloat16),
        "tp",
        scatter_dimension=0,
        tiled=True,
    ).astype(jnp.float32)
    return (routed + shared_sum.T).astype(jnp.bfloat16)


def mm(x, y, dims=NN):
    return lax.dot_general(x, y, (dims, ((), ())), preferred_element_type=jnp.float32)


def pair_masks():
    lane = lax.broadcasted_iota(jnp.int32, (BLOCK, 2 * HEAD_CHANNELS), 1)
    first = jnp.where(lane < HEAD_CHANNELS, 1.0, 0.0)
    return first.astype(jnp.bfloat16), (1.0 - first).astype(jnp.bfloat16)


def stacked(y, masks):
    return jnp.concatenate([y * masks[0], y * masks[1]], axis=0)


def pair_dot(x, parts):
    xh, xl = split_parts(x)
    high, low = parts
    return mm(jnp.concatenate([xh, xl], axis=1), jnp.concatenate([high, high], axis=0)) + mm(
        xh, low
    )


def short_dot(x, y, masks):
    return mm(x.astype(jnp.bfloat16), stacked(y.astype(jnp.bfloat16), masks))


def pair_parts(y, masks):
    yh, yl = split_parts(y)
    return stacked(yh, masks), stacked(yl, masks)


def side_by_side(one, two):
    return tuple(jnp.concatenate([p, q], axis=1) for p, q in zip(one, two))


def head_sum(x, block_ones):
    xh, xl = split_parts(x)
    return mm(jnp.concatenate([xh, xl], axis=1), block_ones)


def head_ones():
    wide = 2 * HEAD_CHANNELS
    row = lax.broadcasted_iota(jnp.int32, (2 * wide, wide), 0)
    col = lax.broadcasted_iota(jnp.int32, (2 * wide, wide), 1)
    same = (row // HEAD_CHANNELS) % 2 == col // HEAD_CHANNELS
    return jnp.where(same, 1.0, 0.0).astype(jnp.bfloat16)


def local_math(r_ref, k_ref, v_ref, dec_ref, lr_ref, off_ref, spike_ref):
    rows, width = r_ref.shape
    wide = 2 * HEAD_CHANNELS
    pairs = width // wide
    chunks = rows // BLOCK
    masks = pair_masks()
    ones_head = head_ones()
    row = lax.broadcasted_iota(jnp.int32, (BLOCK, wide), 0)
    col = lax.broadcasted_iota(jnp.int32, (BLOCK, wide), 1) % HEAD_CHANNELS
    strict = col < row
    inclusive = col <= row
    trow = lax.broadcasted_iota(jnp.int32, (BLOCK, 4 * BLOCK), 0)
    tcol = lax.broadcasted_iota(jnp.int32, (BLOCK, 4 * BLOCK), 1)
    running = jnp.where((tcol % BLOCK <= trow) & (tcol < 3 * BLOCK), 1.0, 0.0).astype(jnp.bfloat16)
    blank = jnp.zeros((BLOCK, wide), jnp.bfloat16)
    items = [(i, p) for i in range(chunks) for p in range(pairs)]
    spans = [slice(i * BLOCK, (i + 1) * BLOCK) for i in range(chunks)]
    strips = [slice(p * wide, (p + 1) * wide) for p in range(pairs)]
    pre = off_ref[...] + jnp.tanh(dec_ref[...].astype(jnp.float32))
    log = spike_ref[...] - jax.nn.sigmoid(pre) * jnp.exp(jnp.float32(-0.5))
    p0 = log.astype(jnp.bfloat16)
    rest = log - p0.astype(jnp.float32)
    p1 = rest.astype(jnp.bfloat16)
    p2 = (rest - p1.astype(jnp.float32)).astype(jnp.bfloat16)
    empty = jnp.zeros((BLOCK, width), jnp.bfloat16)
    cums = [
        mm(running, jnp.concatenate([p0[span], p1[span], p2[span], empty], axis=0))
        for span in spans
    ]
    k_all = k_ref[...].astype(jnp.float32)
    squares = k_all * k_all
    sums = [head_sum(squares[:, strip], ones_head) for strip in strips]
    learn = jax.nn.sigmoid(lr_ref[...].astype(jnp.float32))
    scale = jnp.concatenate([lax.rsqrt(q + NORM_EPSILON) for q in sums], axis=1)
    cum_all = jnp.concatenate(cums, axis=0)
    back = learn * k_all * jnp.exp(-cum_all)
    b_all = back * scale
    a_all = k_all * scale * jnp.exp(cum_all - log)
    r_all = r_ref[...].astype(jnp.float32) * jnp.exp(cum_all)
    bh_all, bl_all = split_parts(b_all)
    ih_all, il_all = split_parts(back)
    ah_all, al_all = split_parts(a_all)
    rh_all, rl_all = split_parts(r_all)
    chunk_ends = [jnp.exp(c[BLOCK - 1 :]) for c in cums]
    grams = []
    for i, p in items:
        at = (spans[i], strips[p])
        left_high = jnp.concatenate([ah_all[at], rh_all[at]], axis=0)
        left_low = jnp.concatenate([al_all[at], rl_all[at]], axis=0)
        right_high = jnp.concatenate(
            [stacked(bh_all[at], masks), stacked(ih_all[at], masks)], axis=0
        )
        right_low = jnp.concatenate(
            [stacked(bl_all[at], masks), stacked(il_all[at], masks)], axis=0
        )
        grams.append(
            mm(
                jnp.concatenate([left_high, left_low], axis=1),
                jnp.concatenate([right_high, right_high], axis=1),
                NT,
            )
            + mm(left_high, right_low, NT)
        )
    lows = [jnp.where(strict, gram[:BLOCK, :wide], 0.0) for gram in grams]
    out_bs = [jnp.where(inclusive, gram[BLOCK:, :wide], 0.0) for gram in grams]
    vs = [v_ref[spans[i], strips[p]] for i, p in items]
    weighted = []
    for n, gram in enumerate(grams):
        kh, kl = split_parts(
            jnp.concatenate(
                [
                    jnp.where(strict, gram[:BLOCK, wide:], 0.0),
                    jnp.where(inclusive, gram[BLOCK:, wide:], 0.0),
                ],
                axis=0,
            )
        )
        values = stacked(vs[n], masks)
        weighted.append(
            mm(jnp.concatenate([kh, kl], axis=1), jnp.concatenate([values, values], axis=0))
        )
    low_vs = [w[:BLOCK] for w in weighted]
    out_vs = [w[BLOCK:] for w in weighted]
    ends = [chunk_ends[i][:, strips[p]] for i, p in items]
    ins_ends = [back[spans[i], strips[p]] * ends[n] for n, (i, p) in enumerate(items)]
    b_ends = [b_all[spans[i], strips[p]] * ends[n] for n, (i, p) in enumerate(items)]
    r_outs = [r_all[spans[i], strips[p]] for i, p in items]
    a_ins = [a_all[spans[i], strips[p]] for i, p in items]
    count = range(len(items))
    eye = jnp.where(row == col, 1.0, 0.0)
    inverses = None
    size = 1
    while size < BLOCK:
        inside = (row // (2 * size) == col // (2 * size)) & (row // size != col // size)
        corners = [jnp.where(inside, low, 0.0) for low in lows]
        if size == 1:
            inverses = [eye - corner for corner in corners]
        else:
            exact = 2 * size >= BLOCK
            firsts = [
                pair_dot(inverses[n], pair_parts(corners[n], masks))
                if exact
                else short_dot(inverses[n], corners[n], masks)
                for n in count
            ]
            changes = [
                pair_dot(firsts[n], pair_parts(inverses[n], masks))
                if exact
                else short_dot(firsts[n], inverses[n], masks)
                for n in count
            ]
            inverses = [inverses[n] - changes[n] for n in count]
        size *= 2
    solved = [
        side_by_side(pair_parts(a_ins[n], masks), pair_parts(low_vs[n], masks)) for n in count
    ]
    solved = [pair_dot(inverses[n], solved[n]) for n in count]
    brow = lax.broadcasted_iota(jnp.int32, (wide, 2 * wide), 0)
    bcol = lax.broadcasted_iota(jnp.int32, (wide, 2 * wide), 1)
    same_head = brow // HEAD_CHANNELS == (bcol % wide) // HEAD_CHANNELS
    diagonal = brow == bcol
    maps = []
    for n in count:
        left = jnp.concatenate([-b_ends[n], ins_ends[n]], axis=0)
        lh, ll = split_parts(left)
        uh, ul = split_parts(solved[n])
        high = jnp.concatenate([uh, jnp.concatenate([blank, vs[n]], axis=1)], axis=0)
        low = jnp.concatenate([ul, jnp.concatenate([blank, blank], axis=1)], axis=0)
        made = mm(
            jnp.concatenate([lh, ll], axis=0), jnp.concatenate([high, high], axis=0), TN
        ) + mm(lh, low, TN)
        end = jnp.concatenate([ends[n], ends[n]], axis=1)
        maps.append(jnp.where(same_head, made + jnp.where(diagonal, end, 0.0), 0.0))
    def after(second, first):
        joined = pair_dot(second[:, :wide], split_parts(first))
        return jnp.concatenate([joined[:, :wide], joined[:, wide:] + second[:, wide:]], axis=1)

    by_pair = [maps[p::pairs] for p in range(pairs)]
    stage = [list(row) for row in by_pair]
    tree = [stage]
    while len(stage[0]) > 1:
        stage = [
            [
                after(row[i + 1], row[i]) if i + 1 < len(row) else row[i]
                for i in range(0, len(row), 2)
            ]
            for row in stage
        ]
        tree.append(stage)
    whole = [row[0] for row in stage]

    def reaching(p, i):
        result, done = None, 0
        for depth in range(len(tree) - 1, -1, -1):
            if i - done >= 1 << depth:
                piece = tree[depth][p][done >> depth]
                result = piece if result is None else after(piece, result)
                done += 1 << depth
        return result

    compact = [m[:HEAD_CHANNELS] + m[HEAD_CHANNELS:] for m in whole]

    def finish():
        results = {}
        for n in count:
            uh, ul = split_parts(solved[n])
            parts = [
                jnp.concatenate([stacked(u[:, :wide], masks), stacked(u[:, wide:], masks)], axis=1)
                for u in (uh, ul)
            ]
            removed = pair_dot(out_bs[n], parts)
            carry = r_outs[n] - removed[:, :wide]
            value = out_vs[n] - removed[:, wide:]
            entry = reaching(items[n][1], items[n][0])
            if entry is not None:
                moved = pair_dot(carry, split_parts(entry))
                carry = moved[:, :wide]
                value = value + moved[:, wide:]
            results[items[n]] = (carry, value)
        return results

    return compact, finish


def flipped_rows(index, bits, count):
    result, unit = 0, 1
    while unit < count:
        digit = (index // unit) % 2
        result = result + unit * ((digit + bits // unit) % 2)
        unit *= 2
    return result


def mega_kernel(ep_count, *refs):
    inputs = refs[:21]
    attn_out, expert_out = refs[21:23]
    copies = refs[23:44]
    (
        r_ref, k_ref, v_ref, dec_ref, lr_ref, gate_ref, off_ref, spike_ref, hgain_ref, wout_ref,
        pgain_ref, x_ref, egain_ref, idx_ref, wsel_ref, wg_ref, wu_ref, wd_ref, cg_ref, cu_ref,
        cd_ref,
    ) = copies
    (
        normed, outgoing, arrived, carry_ref, value_ref, own_map, held, base_state, state,
        next_state, shared, shared_half, shared_sum, shared_last, crossing,
        halves, own_ref, final, back, heads_ref, mix, mix_half, mix_sum, mix_last,
        load_sem, disp_send, disp_recv, fwd_send, fwd_recv, map_send, map_recv, base_send,
        base_recv, sh_send, sh_recv, cross_send, cross_recv, home_send, home_recv, mx_send,
        mx_recv, tail_send, tail_recv,
    ) = refs[44:]
    me = lax.axis_index("ep")
    place = lax.axis_index("tp")
    group = place // 2
    half = place % 2
    other = 1 - half
    partner = 2 * group + other
    across = 2 * (1 - group) + half
    level = me // 4
    member = me % 4
    levels = ep_count // 4
    tok_rows, model_width = x_ref.shape
    slots = outgoing.shape[0]
    capacity = slots // ep_count
    fold = model_width // 2
    columns = model_width // 4
    rows, width = r_ref.shape
    wide = 2 * HEAD_CHANNELS
    pairs = width // wide
    block_rows = rows // 4
    quarter = ep_count // 4
    outer = (level + member // 2 + 1) % 2
    first_start = quarter * (2 + outer)
    second_start = quarter * (3 - outer)
    first_batch = [first_start + n for n in range(quarter)]
    second_batch = [second_start + n for n in range(quarter)]
    near_batch = list(range(2 * quarter))

    barrier = pltpu.get_barrier_semaphore()

    def peer(bits):
        return flipped_rows(me, bits, ep_count)

    def tp_of(turn):
        return 2 * lax.rem(group + turn, 2) + half

    for bits in range(ep_count):
        for turn in range(2):
            if bits or turn:
                pl.semaphore_signal(
                    barrier,
                    inc=1,
                    device_id={"ep": peer(bits), "tp": tp_of(turn)},
                    device_id_type=MESH,
                )
    pl.semaphore_signal(barrier, inc=1, device_id={"tp": partner}, device_id_type=MESH)

    loads = [
        pltpu.make_async_copy(source, target, load_sem.at[n])
        for n, (source, target) in enumerate(zip(inputs, copies))
    ]
    for n in (13, 14, 11, 12, 0, 1, 2, 3, 4, 6, 7, 18, 19, 20, 15, 16, 17, 5, 8, 9, 10):
        loads[n].start()

    def rows_of(bits):
        if isinstance(bits, int):
            return slice(bits * capacity, (bits + 1) * capacity)
        return pl.ds(pl.multiple_of(bits * capacity, capacity), capacity)

    def remote(source, target, send, recv, where):
        return pltpu.make_async_remote_copy(
            src_ref=source,
            dst_ref=target,
            send_sem=send,
            recv_sem=recv,
            device_id=where,
            device_id_type=MESH,
        )

    def dispatch(bits):
        return remote(
            outgoing.at[rows_of(bits)],
            arrived.at[half, rows_of(bits)],
            disp_send.at[bits],
            disp_recv.at[bits],
            {"ep": peer(bits)},
        )

    def forward(bits):
        return remote(
            arrived.at[half, rows_of(bits)],
            arrived.at[half, rows_of(bits)],
            fwd_send.at[bits],
            fwd_recv.at[bits],
            {"tp": partner},
        )

    for n in (13, 14):
        loads[n].wait()
    chosen_count = idx_ref.shape[0]
    experts = 2 * ep_count
    expert_row = lax.broadcasted_iota(jnp.int32, (experts, tok_rows), 0)
    named = [expert_row == idx_ref[k : k + 1, :] for k in range(chosen_count)]
    chosen = functools.reduce(jnp.logical_or, named)
    weight_of = functools.reduce(
        jnp.add, [jnp.where(n, wsel_ref[k : k + 1, :], 0.0) for k, n in enumerate(named)]
    )
    early = lax.broadcasted_iota(jnp.int32, (tok_rows, tok_rows), 0) < lax.broadcasted_iota(
        jnp.int32, (tok_rows, tok_rows), 1
    )
    rank = mm(
        jnp.where(chosen, 1.0, 0.0).astype(jnp.bfloat16),
        jnp.where(early, 1.0, 0.0).astype(jnp.bfloat16),
    )
    rank = jnp.where(chosen, rank, -1.0).astype(jnp.bfloat16)
    slot = lax.broadcasted_iota(jnp.int32, (slots, experts), 0)
    which = lax.broadcasted_iota(jnp.int32, (slots, experts), 1)
    there = flipped_rows(me, slot // capacity, ep_count)
    mine = jnp.where(which == 2 * there + group, 1.0, 0.0).astype(jnp.bfloat16)
    slot_rank = (
        lax.broadcasted_iota(jnp.int32, (slots, tok_rows), 0) % capacity
    ).astype(jnp.float32)
    placing = jnp.where(mm(mine, rank) == slot_rank, 1.0, 0.0).astype(jnp.bfloat16)
    for n in (11, 12):
        loads[n].wait()
    normed[...] = rms_scale(x_ref[...], egain_ref[...]).astype(jnp.bfloat16)
    fold_span = pl.ds(pl.multiple_of(half * fold, fold), fold)
    other_span = pl.ds(pl.multiple_of(other * fold, fold), fold)
    outgoing[...] = mm(placing, normed[:, fold_span]).astype(jnp.bfloat16)
    pl.semaphore_wait(barrier, 2 * ep_count)
    order = list(range(2 * quarter, ep_count)) + near_batch[1:]
    for bits in order[: 2 * quarter]:
        dispatch(bits).start()

    @pl.when(outer == 0)
    def _():
        for bits in order[2 * quarter :]:
            dispatch(bits).start()

    arrived[half, rows_of(0), :] = outgoing[rows_of(0), :]
    arrived[other, rows_of(0), :] = mm(placing[:capacity], normed[:, other_span]).astype(
        jnp.bfloat16
    )

    for n in (0, 1, 2, 3, 4, 6, 7):
        loads[n].wait()
    compact, finish = local_math(r_ref, k_ref, v_ref, dec_ref, lr_ref, off_ref, spike_ref)
    for p in range(pairs):
        own_map[p] = compact[p].astype(jnp.bfloat16)
    masks = pair_masks()

    def give(there):
        return remote(
            own_map,
            held.at[member],
            map_send.at[there],
            map_recv.at[member],
            {"ep": 4 * level + there},
        )

    def taken(source):
        return remote(
            own_map, held.at[source], map_send.at[0], map_recv.at[source], {"ep": peer(1)}
        )

    def gives(there):
        above_me = member < there
        return above_me | (member == 3) if there == 2 else above_me

    for there in (3, 2, 1):

        @pl.when(gives(there))
        def _():
            give(there).start()

    for (i, p), (carry, value) in finish().items():
        span = slice(i * BLOCK, (i + 1) * BLOCK)
        lanes = slice(p * wide, (p + 1) * wide)
        carry_ref[span, lanes] = carry
        value_ref[span, lanes] = value

    for n in (18, 19, 20):
        loads[n].wait()
    rows_in = normed[...]
    hidden = (jax.nn.silu(mm(rows_in, cg_ref[...])) * mm(rows_in, cu_ref[...])).astype(
        jnp.bfloat16
    )
    for j in range(4):
        shared[j] = mm(hidden, cd_ref[:, j * columns : (j + 1) * columns]).astype(jnp.bfloat16)

    def shared_cross(turn):
        there = 2 * lax.rem(group + turn, 2) + other
        return remote(
            shared.at[there],
            shared_half.at[turn],
            sh_send.at[turn],
            sh_recv.at[turn],
            {"tp": partner},
        )

    for turn in (1, 0):
        shared_cross(turn).start()

    def take_in(batch):
        for bits in batch:
            if not isinstance(bits, int) or bits:
                dispatch(bits).wait_recv()
                forward(bits).start()

    for turn in (1, 0):
        shared_cross(turn).wait_recv()
        shared_sum[turn] = shared[tp_of(turn)].astype(jnp.float32) + shared_half[turn].astype(
            jnp.float32
        )
    shared_last[0] = shared_sum[1].astype(jnp.bfloat16)
    shared_tail = remote(
        shared_last.at[0], shared_last.at[1], tail_send.at[0], tail_recv.at[0], {"tp": across}
    )
    shared_tail.start()
    take_in(first_batch)

    @pl.when(outer == 1)
    def _():
        for bits in order[2 * quarter :]:
            dispatch(bits).start()

    def wait_far(batch):
        for bits in batch:
            if not isinstance(bits, int) or bits:
                forward(bits).wait_recv()

    def cross(batch_index, turn, span):
        return remote(
            crossing.at[turn, span],
            halves.at[turn, span],
            cross_send.at[batch_index, turn],
            cross_recv.at[batch_index, turn],
            {"tp": partner},
        )

    def home(turn, bits):
        return remote(
            final.at[turn, rows_of(bits)],
            back.at[group, rows_of(bits)],
            home_send.at[turn, bits],
            home_recv.at[turn, bits],
            {"ep": peer(bits), "tp": tp_of(turn)},
        )

    def span_of(batch):
        if isinstance(batch[0], int):
            return slice(0, len(batch) * capacity)
        size = quarter * capacity
        return pl.ds(pl.multiple_of(batch[0] * capacity, size), size)

    def feed(batch_index, batch):
        span = span_of(batch)
        near, away = arrived[0, span, :], arrived[1, span, :]
        gate = mm(near, wg_ref[:fold, :]) + mm(away, wg_ref[fold:, :])
        upper = mm(near, wu_ref[:fold, :]) + mm(away, wu_ref[fold:, :])
        routed_hidden = (jax.nn.silu(gate) * upper).astype(jnp.bfloat16)

        def part(index):
            lanes = pl.ds(pl.multiple_of(index * columns, columns), columns)
            return mm(routed_hidden, wd_ref[:, lanes])

        for turn in (1, 0):
            crossing[turn, span, :] = part(2 * lax.rem(group + turn, 2) + other).astype(
                jnp.bfloat16
            )
            cross(batch_index, turn, span).start()
        for turn in (1, 0):
            own_ref[turn, span, :] = part(2 * lax.rem(group + turn, 2) + half)

    def send_home(batch_index, batch):
        span = span_of(batch)
        for turn in (1, 0):
            cross(batch_index, turn, span).wait_recv()
            final[turn, span, :] = (
                own_ref[turn, span, :] + halves[turn, span, :].astype(jnp.float32)
            ).astype(jnp.bfloat16)
            for bits in batch:
                if not isinstance(bits, int) or bits or turn:
                    home(turn, bits).start()
                else:
                    back[group, rows_of(0), :] = final[0, rows_of(0), :]

    for n in (15, 16, 17):
        loads[n].wait()
    wait_far(first_batch)
    feed(0, first_batch)
    def moved_by(block, p, current):
        through = block[p, :, :wide]
        high, low = pair_parts(current, masks)
        return mm(
            jnp.concatenate([through, through], axis=1), jnp.concatenate([high, low], axis=0)
        ) + block[p, :, wide:].astype(jnp.float32)

    def above(turn):
        return remote(
            next_state,
            base_state,
            base_send.at[turn],
            base_recv.at[0],
            {"ep": lax.rem(4 * (level + 1) + 2 * turn + member % 2, ep_count)},
        )

    hands_on = (member >= 2) & (level + 1 < levels)

    def settle():
        for p in range(pairs):
            state[p] = base_state[p].astype(jnp.float32)
        for source in range(3):

            @pl.when(source < member)
            def _():
                taken(source).wait_recv()
                for p in range(pairs):
                    state[p] = moved_by(held.at[source], p, state[p])

        @pl.when(member == 2)
        def _():
            taken(3).wait_recv()

        @pl.when(hands_on)
        def _():
            for p in range(pairs):
                once = moved_by(own_map, p, state[p])
                twice = moved_by(held.at[3], p, once)
                next_state[p] = jnp.where(member == 2, twice, once).astype(jnp.bfloat16)
            for turn in range(2):
                above(turn).start()

    @pl.when(level == 0)
    def _():
        base_state[...] = jnp.zeros_like(base_state)
        settle()

    send_home(0, first_batch)
    for n in (5, 8, 9, 10):
        loads[n].wait()

    def mix_cross(turn):
        there = 2 * lax.rem(group + turn, 2) + other
        return remote(
            mix.at[there],
            mix_half.at[turn],
            mx_send.at[turn],
            mx_recv.at[turn],
            {"tp": partner},
        )

    def project(turn):
        there = lax.rem(group + turn, 2)
        rows_there = pl.ds(pl.multiple_of(there * 2 * block_rows, 2 * block_rows), 2 * block_rows)
        rows_made = heads_ref[rows_there, :]
        for j in range(4):
            span = slice(j * columns, (j + 1) * columns)
            made = mm(rows_made, wout_ref[:, span]).astype(jnp.bfloat16)
            for b in range(2):
                mix[2 * there + b, :, span] = made[b * block_rows : (b + 1) * block_rows]

    def attend():
        ones_head = head_ones()
        for p in range(pairs):
            lanes = slice(p * wide, (p + 1) * wide)
            value = value_ref[:, lanes] + pair_dot(
                carry_ref[:, lanes], pair_parts(state[p], masks)
            )
            centred = value - head_sum(value, ones_head) * (1.0 / HEAD_CHANNELS)
            spread = head_sum(centred * centred, ones_head) * (1.0 / HEAD_CHANNELS)
            heads_ref[:, lanes] = (
                centred
                * lax.rsqrt(spread + GROUP_EPSILON)
                * hgain_ref[:, lanes]
                * jax.nn.sigmoid(gate_ref[:, lanes].astype(jnp.float32))
            ).astype(jnp.bfloat16)
        for turn in (1, 0):
            project(turn)
            mix_cross(turn).start()

    mix_tail = remote(
        mix_last.at[0], mix_last.at[1], tail_send.at[1], tail_recv.at[1], {"tp": across}
    )

    def pass_mix():
        mix_cross(1).wait_recv()
        mix_last[0] = (
            mix[across].astype(jnp.float32) + mix_half[1].astype(jnp.float32)
        ).astype(jnp.bfloat16)
        mix_tail.start()

    @pl.when(level == 0)
    def _():
        attend()

    take_in(near_batch)
    @pl.when(level == 0)
    def _():
        pass_mix()

    wait_far(near_batch)
    feed(1, near_batch)
    take_in(second_batch)
    send_home(1, near_batch)

    @pl.when(level > 0)
    def _():
        above(0).wait_recv()
        settle()

    @pl.when(level > 0)
    def _():
        attend()

    wait_far(second_batch)
    feed(2, second_batch)
    @pl.when(level > 0)
    def _():
        pass_mix()

    send_home(2, second_batch)
    mix_cross(0).wait_recv()
    mix_sum[...] = mix[place].astype(jnp.float32) + mix_half[0].astype(jnp.float32)

    all_slots = 2 * slots
    slot = lax.broadcasted_iota(jnp.int32, (experts, all_slots), 1)
    which = lax.broadcasted_iota(jnp.int32, (experts, all_slots), 0)
    there = flipped_rows(me, (slot % slots) // capacity, ep_count)
    holder = jnp.where(which == 2 * there + slot // slots, 1.0, 0.0).astype(jnp.bfloat16)
    slot_rank = (
        lax.broadcasted_iota(jnp.int32, (tok_rows, all_slots), 1) % capacity
    ).astype(jnp.float32)
    hit = mm(rank, holder, TN) == slot_rank
    weight_high, weight_low = split_parts(weight_of)
    picks = [
        jnp.where(hit, mm(w, holder, TN), 0.0).astype(jnp.bfloat16)
        for w in (weight_high, weight_low)
    ]
    shared_tail.wait_recv()
    base = shared_sum[0] + shared_last[1].astype(jnp.float32)
    for batch in (first_batch, near_batch, second_batch):
        for turn in range(2):
            for bits in batch:
                if not isinstance(bits, int) or bits or turn:
                    home(turn, bits).wait_recv()
    returned = back[...].reshape(all_slots, columns)
    routed = mm(
        jnp.concatenate(picks, axis=1), jnp.concatenate([returned, returned], axis=0)
    )
    expert_out[...] = (routed + base).astype(jnp.bfloat16)

    mix_tail.wait_recv()
    total = mix_sum[...] + mix_last[1].astype(jnp.float32)
    attn_out[...] = rms_scale(total, pgain_ref[...]).astype(jnp.bfloat16)

    for bits in order:
        dispatch(bits).wait_send()
        forward(bits).wait_send()
    for there in (3, 2, 1):

        @pl.when(gives(there))
        def _():
            give(there).wait_send()

    @pl.when(hands_on)
    def _():
        for turn in range(2):
            above(turn).wait_send()

    for turn in range(2):
        shared_cross(turn).wait_send()
        mix_cross(turn).wait_send()
        for n, batch in enumerate((first_batch, near_batch, second_batch)):
            cross(n, turn, span_of(batch)).wait_send()
        for bits in range(ep_count):
            if bits or turn:
                home(turn, bits).wait_send()
    shared_tail.wait_send()
    mix_tail.wait_send()


def mega(
    receptance, head_key_input, head_value_input, decay_input_part, learning_rate_input,
    output_gate_input, decay_channel_offset, spike_log_decay, head_norm_gain, head_output_weight,
    projection_norm_gain, expert_input_rows, expert_norm_gain, selected_expert_index,
    selected_expert_weight, routed_gate_weight, routed_up_weight, routed_down_weight,
    common_gate_weight, common_up_weight, common_down_weight,
):
    ep_count = lax.axis_size("ep")
    rows, width = receptance.shape
    tok_rows, model_width = expert_input_rows.shape
    chosen = selected_expert_index.shape[1]
    capacity = tok_rows * chosen // ep_count
    slots = ep_count * capacity
    columns = model_width // 4
    wide = 2 * HEAD_CHANNELS
    pairs = width // wide
    operands = (
        receptance, head_key_input, head_value_input, decay_input_part, learning_rate_input,
        output_gate_input, decay_channel_offset[None, :], spike_log_decay, head_norm_gain[None, :],
        head_output_weight, projection_norm_gain[None, :], expert_input_rows,
        expert_norm_gain[None, :], selected_expert_index.T, selected_expert_weight.T,
        routed_gate_weight[0], routed_up_weight[0], routed_down_weight[0], common_gate_weight,
        common_up_weight, common_down_weight,
    )
    bf16, f32 = jnp.bfloat16, jnp.float32
    dma = pltpu.SemaphoreType.DMA
    scratch = [pltpu.VMEM(o.shape, o.dtype) for o in operands] + [
        pltpu.VMEM((tok_rows, model_width), bf16),
        pltpu.VMEM((slots, model_width // 2), bf16),
        pltpu.VMEM((2, slots, model_width // 2), bf16),
        pltpu.VMEM((rows, width), f32),
        pltpu.VMEM((rows, width), f32),
        pltpu.VMEM((pairs, HEAD_CHANNELS, 2 * wide), bf16),
        pltpu.VMEM((4, pairs, HEAD_CHANNELS, 2 * wide), bf16),
        pltpu.VMEM((pairs, HEAD_CHANNELS, wide), bf16),
        pltpu.VMEM((pairs, HEAD_CHANNELS, wide), f32),
        pltpu.VMEM((pairs, HEAD_CHANNELS, wide), bf16),
        pltpu.VMEM((4, tok_rows, columns), bf16),
        pltpu.VMEM((2, tok_rows, columns), bf16),
        pltpu.VMEM((2, tok_rows, columns), f32),
        pltpu.VMEM((2, tok_rows, columns), bf16),
        pltpu.VMEM((2, slots, columns), bf16),
        pltpu.VMEM((2, slots, columns), bf16),
        pltpu.VMEM((2, slots, columns), f32),
        pltpu.VMEM((2, slots, columns), bf16),
        pltpu.VMEM((2, slots, columns), bf16),
        pltpu.VMEM((rows, width), bf16),
        pltpu.VMEM((4, rows // 4, model_width), bf16),
        pltpu.VMEM((2, rows // 4, model_width), bf16),
        pltpu.VMEM((rows // 4, model_width), f32),
        pltpu.VMEM((2, rows // 4, model_width), bf16),
        dma((len(operands),)),
    ]
    scratch += [dma((ep_count,))] * 4
    scratch += [dma((4,))] * 2
    scratch += [dma((2,))] * 4
    scratch += [dma((3, 2))] * 2
    scratch += [dma((2, ep_count))] * 2
    scratch += [dma((2,))] * 4
    full = pl.BlockSpec(memory_space=pltpu.VMEM)
    return pl.pallas_call(
        functools.partial(mega_kernel, ep_count),
        out_shape=(
            pltpu.VMEM((rows // 4, model_width), bf16),
            pltpu.VMEM((tok_rows, columns), bf16),
        ),
        in_specs=[pl.BlockSpec(memory_space=pl.ANY)] * len(operands),
        out_specs=(full, full),
        scratch_shapes=scratch,
        compiler_params=pltpu.CompilerParams(collective_id=0, has_side_effects=True),
    )(*operands)


def fits_mega(receptance, expert_input_rows, selected_expert_index):
    ep_count = lax.axis_size("ep")
    rows, width = receptance.shape
    tok_rows, model_width = expert_input_rows.shape
    assigned = tok_rows * selected_expert_index.shape[1]
    return (
        lax.axis_size("tp") == 4
        and ep_count >= 4
        and ep_count & (ep_count - 1) == 0
        and width % (2 * HEAD_CHANNELS) == 0
        and rows % (4 * BLOCK) == 0
        and assigned % (16 * ep_count) == 0
        and tok_rows % 128 == 0
        and tok_rows <= 256
        and model_width % 512 == 0
    )


def body(
    receptance,
    head_key_input,
    head_value_input,
    decay_input_part,
    learning_rate_input,
    output_gate_input,
    decay_channel_offset,
    spike_log_decay,
    head_norm_gain,
    head_output_weight,
    projection_norm_gain,
    expert_input_rows,
    expert_norm_gain,
    selected_expert_index,
    selected_expert_weight,
    routed_gate_weight,
    routed_up_weight,
    routed_down_weight,
    common_gate_weight,
    common_up_weight,
    common_down_weight,
):
    if fits_mega(receptance, expert_input_rows, selected_expert_index):
        return mega(
            receptance, head_key_input, head_value_input, decay_input_part, learning_rate_input,
            output_gate_input, decay_channel_offset, spike_log_decay, head_norm_gain,
            head_output_weight, projection_norm_gain, expert_input_rows, expert_norm_gain,
            selected_expert_index, selected_expert_weight, routed_gate_weight, routed_up_weight,
            routed_down_weight, common_gate_weight, common_up_weight, common_down_weight,
        )
    attention_output = attention_mixer(
        receptance,
        head_key_input,
        head_value_input,
        decay_input_part,
        learning_rate_input,
        output_gate_input,
        decay_channel_offset,
        spike_log_decay,
        head_norm_gain,
        head_output_weight,
        projection_norm_gain,
    )
    expert_output = expert_half(
        expert_input_rows,
        expert_norm_gain,
        selected_expert_index,
        selected_expert_weight,
        routed_gate_weight,
        routed_up_weight,
        routed_down_weight,
        common_gate_weight,
        common_up_weight,
        common_down_weight,
    )
    return (attention_output, expert_output)


def solution(mesh):
    placed = (
        P("ep", "tp"),
        P("ep", "tp"),
        P("ep", "tp"),
        P("ep", "tp"),
        P("ep", "tp"),
        P("ep", "tp"),
        P("tp"),
        P("ep", "tp"),
        P("tp"),
        P("tp", None),
        P(),
        P("ep", None),
        P(),
        P("ep", None),
        P("ep", None),
        P(("ep", "tp"), None, None),
        P(("ep", "tp"), None, None),
        P(("ep", "tp"), None, None),
        P(None, "tp"),
        P(None, "tp"),
        P("tp", None),
    )
    return jax.shard_map(
        body,
        mesh=mesh,
        in_specs=placed,
        out_specs=(P(("ep", "tp"), None), P("ep", "tp")),
        check_vma=False,
    )
```

```python
import functools

import jax
import jax.numpy as jnp
from jax import lax
from jax.experimental import pallas as pl
from jax.experimental.pallas import tpu as pltpu
from jax.sharding import PartitionSpec as P

HEAD_CHANNELS = 64
BLOCK = 64


MESH = pl.DeviceIdType.MESH
NORM_EPSILON = 1e-06
GROUP_EPSILON = 0.00064


def rms_scale(values, gain):
    values = values.astype(jnp.float32)
    return (
        values * lax.rsqrt(jnp.mean(values * values, axis=-1, keepdims=True) + NORM_EPSILON) * gain
    )


def split_parts(x):
    high = x.astype(jnp.bfloat16)
    return high, (x - high.astype(jnp.float32)).astype(jnp.bfloat16)


def dot3(x, y, dims):
    xh, xl = split_parts(x)
    yh, yl = split_parts(y)

    def one(p, q):
        return lax.dot_general(p, q, (dims, ((), ())), preferred_element_type=jnp.float32)

    return one(xh, yh) + (one(xh, yl) + one(xl, yh))


NN = ((1,), (0,))
NT = ((1,), (1,))
TN = ((0,), (0,))


def local_kernel(
    r_ref, k_ref, v_ref, dec_ref, lr_ref, off_ref, spike_ref, out_ref, carry_ref, map_ref
):
    rows, width = r_ref.shape
    heads = width // HEAD_CHANNELS
    blocks = rows // BLOCK
    row = lax.broadcasted_iota(jnp.int32, (rows, rows), 0)
    col = lax.broadcasted_iota(jnp.int32, (rows, rows), 1)
    strict = col < row
    inclusive = col <= row
    learn_all = jax.nn.sigmoid(lr_ref[...].astype(jnp.float32))
    pre = off_ref[...] + jnp.tanh(dec_ref[...].astype(jnp.float32))
    log_all = spike_ref[...] - jax.nn.sigmoid(pre) * jnp.exp(jnp.float32(-0.5))
    ones = jnp.where(inclusive, 1.0, 0.0).astype(jnp.bfloat16)
    p0 = log_all.astype(jnp.bfloat16)
    rest = log_all - p0.astype(jnp.float32)
    p1 = rest.astype(jnp.bfloat16)
    p2 = (rest - p1.astype(jnp.float32)).astype(jnp.bfloat16)
    cum_all = sum(jnp.dot(ones, p, preferred_element_type=jnp.float32) for p in (p0, p1, p2))
    before_all = cum_all - log_all
    for h in range(heads):
        lanes = slice(h * HEAD_CHANNELS, (h + 1) * HEAD_CHANNELS)
        r = r_ref[:, lanes].astype(jnp.float32)
        k = k_ref[:, lanes].astype(jnp.float32)
        v = v_ref[:, lanes].astype(jnp.float32)
        learn = learn_all[:, lanes]
        cum = cum_all[:, lanes]
        before = before_all[:, lanes]
        a = k * lax.rsqrt(jnp.sum(k * k, axis=-1, keepdims=True) + NORM_EPSILON)
        b = a * learn
        ins = k * learn
        parts = []
        for i in range(blocks):
            span = slice(i * BLOCK, (i + 1) * BLOCK)
            base = before[i * BLOCK : i * BLOCK + 1]
            left = jnp.concatenate(
                [a[span] * jnp.exp(before[span] - base), r[span] * jnp.exp(cum[span] - base)],
                axis=0,
            )
            back = jnp.exp(jnp.minimum(base - cum, 60.0))
            right = jnp.concatenate([b * back, ins * back], axis=0)
            parts.append(dot3(left, right, NT))
        low_b = jnp.where(strict, jnp.concatenate([p[:BLOCK, :rows] for p in parts], axis=0), 0.0)
        low_k = jnp.where(strict, jnp.concatenate([p[:BLOCK, rows:] for p in parts], axis=0), 0.0)
        out_b = jnp.where(
            inclusive, jnp.concatenate([p[BLOCK:, :rows] for p in parts], axis=0), 0.0
        )
        out_k = jnp.where(
            inclusive, jnp.concatenate([p[BLOCK:, rows:] for p in parts], axis=0), 0.0
        )
        inverse = jnp.where(row == col, 1.0, 0.0)
        size = 1
        while size < BLOCK:
            corner = (row // (2 * size) == col // (2 * size)) & (row // size != col // size)
            corner = jnp.where(corner, low_b, 0.0)
            if size == 1:
                inverse = inverse - corner
            else:
                inverse = inverse - dot3(dot3(inverse, corner, NN), inverse, NN)
            size *= 2
        right_side = jnp.concatenate([a * jnp.exp(before), dot3(low_k, v, NN)], axis=1)
        solved = []
        for i in range(blocks):
            span = slice(i * BLOCK, (i + 1) * BLOCK)
            piece = right_side[span]
            if i:
                piece = piece - dot3(
                    low_b[span, : i * BLOCK], jnp.concatenate(solved, axis=0), NN
                )
            solved.append(dot3(inverse[span, span], piece, NN))
        solved = jnp.concatenate(solved, axis=0)
        removed = dot3(out_b, solved, NN)
        out_ref[:, lanes] = dot3(out_k, v, NN) - removed[:, HEAD_CHANNELS:]
        carry_ref[:, lanes] = r * jnp.exp(cum) - removed[:, :HEAD_CHANNELS]
        last = cum[rows - 1 :]
        to_end = jnp.exp(last - cum)
        taken = dot3(solved, b * to_end, TN)
        added = dot3(v, ins * to_end, TN)
        small = (HEAD_CHANNELS, HEAD_CHANNELS)
        eye = lax.broadcasted_iota(jnp.int32, small, 0) == lax.broadcasted_iota(jnp.int32, small, 1)
        through = jnp.where(eye, jnp.exp(last), 0.0) - taken[:HEAD_CHANNELS]
        fresh = added - taken[HEAD_CHANNELS:]
        map_ref[lanes, :] = jnp.concatenate([through, fresh], axis=1).astype(jnp.bfloat16)


def join_kernel(
    count, out_ref, carry_ref, map_ref, gain_ref, gate_ref, weight_ref, mix_ref, held, state,
    send_sem, recv_sem
):
    me = lax.axis_index("ep")
    rows, width = out_ref.shape
    heads = width // HEAD_CHANNELS
    barrier = pltpu.get_barrier_semaphore()
    for step in range(1, count):
        pl.semaphore_signal(
            barrier, inc=1, device_id={"ep": lax.rem(me + step, count)}, device_id_type=MESH
        )
    pl.semaphore_wait(barrier, count - 1)

    def copy(slot, step):
        return pltpu.make_async_remote_copy(
            src_ref=map_ref,
            dst_ref=held.at[slot],
            send_sem=send_sem.at[step],
            recv_sem=recv_sem.at[slot],
            device_id={"ep": lax.rem(me + step, count)},
            device_id_type=MESH,
        )

    for step in range(1, count):

        @pl.when(me + step < count)
        def _():
            copy(me, step).start()

    state[...] = jnp.zeros_like(state)

    def one(turn, _):
        copy(turn, 1).wait_recv()
        for h in range(heads):
            lanes = slice(h * HEAD_CHANNELS, (h + 1) * HEAD_CHANNELS)
            block = held[turn, lanes, :]
            high, low = split_parts(state[lanes, :])
            through = block[:, :HEAD_CHANNELS]
            state[lanes, :] = (
                jnp.dot(high, through, preferred_element_type=jnp.float32)
                + jnp.dot(low, through, preferred_element_type=jnp.float32)
                + block[:, HEAD_CHANNELS:].astype(jnp.float32)
            )
        return 0

    lax.fori_loop(0, me, one, 0)
    normed = []
    for h in range(heads):
        lanes = slice(h * HEAD_CHANNELS, (h + 1) * HEAD_CHANNELS)
        value = out_ref[:, lanes] + dot3(carry_ref[:, lanes], state[lanes, :], NT)
        centred = value - jnp.mean(value, axis=-1, keepdims=True)
        normed.append(
            centred
            * lax.rsqrt(jnp.mean(centred * centred, axis=-1, keepdims=True) + GROUP_EPSILON)
        )
    flat = normed[0] if heads == 1 else jnp.concatenate(normed, axis=1)
    heads_out = flat * gain_ref[...] * jax.nn.sigmoid(gate_ref[...].astype(jnp.float32))
    mix_ref[...] = jnp.dot(
        heads_out.astype(jnp.bfloat16), weight_ref[...], preferred_element_type=jnp.float32
    ).astype(jnp.bfloat16)
    for step in range(1, count):

        @pl.when(me + step < count)
        def _():
            copy(me, step).wait_send()


def attention_mixer(
    receptance,
    head_key_input,
    head_value_input,
    decay_input_part,
    learning_rate_input,
    output_gate_input,
    decay_channel_offset,
    spike_log_decay,
    head_norm_gain,
    head_output_weight,
    projection_norm_gain,
):
    rows, width = receptance.shape
    count = lax.axis_size("ep")
    full = pl.BlockSpec(memory_space=pltpu.VMEM)
    out, carry, maps = pl.pallas_call(
        local_kernel,
        out_shape=(
            jax.ShapeDtypeStruct((rows, width), jnp.float32),
            jax.ShapeDtypeStruct((rows, width), jnp.float32),
            jax.ShapeDtypeStruct((width, 2 * HEAD_CHANNELS), jnp.bfloat16),
        ),
        in_specs=[full] * 7,
        out_specs=(full, full, full),
        cost_estimate=pl.CostEstimate(
            flops=rows * rows * width * 200, bytes_accessed=rows * width * 22, transcendentals=0
        ),
    )(
        receptance,
        head_key_input,
        head_value_input,
        decay_input_part,
        learning_rate_input,
        decay_channel_offset[None, :],
        spike_log_decay,
    )
    model_width = head_output_weight.shape[1]
    mix = pl.pallas_call(
        functools.partial(join_kernel, count),
        out_shape=jax.ShapeDtypeStruct((rows, model_width), jnp.bfloat16),
        in_specs=[full] * 6,
        out_specs=full,
        scratch_shapes=[
            pltpu.VMEM((count, width, 2 * HEAD_CHANNELS), jnp.bfloat16),
            pltpu.VMEM((width, HEAD_CHANNELS), jnp.float32),
            pltpu.SemaphoreType.DMA((count,)),
            pltpu.SemaphoreType.DMA((count,)),
        ],
        compiler_params=pltpu.CompilerParams(collective_id=0, has_side_effects=True),
        cost_estimate=pl.CostEstimate(
            flops=rows * width * model_width * 20,
            bytes_accessed=width * model_width * 2,
            transcendentals=0,
        ),
    )(out, carry, maps, head_norm_gain[None, :], output_gate_input, head_output_weight)
    mix_sum = lax.psum_scatter(mix, "tp", scatter_dimension=0, tiled=True).astype(jnp.float32)
    return rms_scale(mix_sum, projection_norm_gain).astype(jnp.bfloat16)


def expert_kernel(
    count, pairs, arrived, gate_ref, up_ref, down_ref, result_ref, crossing, halves, paired,
    final, back, half_send, half_recv, pair_send, pair_recv, back_send, back_recv
):
    me = lax.axis_index("ep")
    place = lax.axis_index("tp")
    group = place // 2
    half = place % 2
    capacity = arrived.shape[0] // count
    columns = final.shape[2]
    partner = 2 * group + 1 - half

    def rows_of(index):
        return pl.ds(pl.multiple_of(index * capacity, capacity), capacity)

    def peer(step):
        return lax.rem(me + step, count)

    barrier = pltpu.get_barrier_semaphore()
    for step in range(1, count):
        pl.semaphore_signal(barrier, inc=1, device_id={"ep": peer(step)}, device_id_type=MESH)
    pl.semaphore_signal(barrier, inc=1, device_id={"tp": partner}, device_id_type=MESH)
    for step in range(1, pairs):
        there = 2 * lax.rem(group + step, pairs) + half
        pl.semaphore_signal(barrier, inc=1, device_id={"tp": there}, device_id_type=MESH)
    pl.semaphore_wait(barrier, count + pairs - 1)

    def cross(index):
        return pltpu.make_async_remote_copy(
            src_ref=crossing.at[index],
            dst_ref=halves.at[index],
            send_sem=half_send.at[index],
            recv_sem=half_recv.at[index],
            device_id={"tp": partner},
            device_id_type=MESH,
        )

    def pair(step):
        return pltpu.make_async_remote_copy(
            src_ref=paired.at[step],
            dst_ref=final.at[step],
            send_sem=pair_send.at[step],
            recv_sem=pair_recv.at[step],
            device_id={"tp": 2 * lax.rem(group + step, pairs) + half},
            device_id_type=MESH,
        )

    def home(turn, step):
        return pltpu.make_async_remote_copy(
            src_ref=final.at[turn, rows_of(peer(step))],
            dst_ref=back.at[turn, rows_of(me)],
            send_sem=back_send.at[turn, step],
            recv_sem=back_recv.at[turn, step],
            device_id={"ep": peer(step)},
            device_id_type=MESH,
        )

    rows = arrived[...]
    gate = jnp.dot(rows, gate_ref[0], preferred_element_type=jnp.float32)
    upward = jnp.dot(rows, up_ref[0], preferred_element_type=jnp.float32)
    hidden = (jax.nn.silu(gate) * upward).astype(jnp.bfloat16)

    def part(index):
        span = pl.ds(pl.multiple_of(index * columns, columns), columns)
        return jnp.dot(hidden, down_ref[0, :, span], preferred_element_type=jnp.float32).astype(
            jnp.bfloat16
        )

    order = list(range(1, pairs)) + [0]
    for step in order:
        crossing[step] = part(2 * lax.rem(group + step, pairs) + 1 - half)
        cross(step).start()
    own = {step: part(2 * lax.rem(group + step, pairs) + half) for step in order}
    for step in order:
        cross(step).wait_recv()
        total = (
            own[step].astype(jnp.float32) + halves[step].astype(jnp.float32)
        ).astype(jnp.bfloat16)
        if step:
            paired[step] = total
            pair(step).start()
        else:
            final[0] = total
    for turn in range(pairs):
        if turn:
            pair(turn).wait_recv()
        for step in range(1, count):
            home(turn, step).start()
        back[turn, rows_of(me), :] = final[turn, rows_of(me), :]
    for turn in range(pairs):
        for step in range(1, count):
            home(turn, step).wait_recv()
        result_ref[lax.rem(group + pairs - turn, pairs)] = back[turn]
    for step in order:
        cross(step).wait_send()
        if step:
            pair(step).wait_send()
    for turn in range(pairs):
        for step in range(1, count):
            home(turn, step).wait_send()


def routed_by_kernel(arrived, gate_weight, up_weight, down_weight, count, pairs):
    rows, model_width = arrived.shape
    columns = model_width // (2 * pairs)
    full = pl.BlockSpec(memory_space=pltpu.VMEM)
    dma = pltpu.SemaphoreType.DMA
    block = pltpu.VMEM((pairs, rows, columns), jnp.bfloat16)
    return pl.pallas_call(
        functools.partial(expert_kernel, count, pairs),
        out_shape=jax.ShapeDtypeStruct((pairs, rows, columns), jnp.bfloat16),
        in_specs=[full] * 4,
        out_specs=full,
        scratch_shapes=[block] * 5
        + [dma((pairs,))] * 4
        + [dma((pairs, count))] * 2,
        compiler_params=pltpu.CompilerParams(collective_id=1, has_side_effects=True),
        cost_estimate=pl.CostEstimate(
            flops=10 * rows * model_width * gate_weight.shape[2] * 6,
            bytes_accessed=model_width * gate_weight.shape[2] * 6,
            transcendentals=0,
        ),
    )(arrived, gate_weight, up_weight, down_weight)


def routed_by_exchange(flat_rows, gate_weight, up_weight, down_weight, count, pairs):
    rows, model_width = flat_rows.shape
    columns = model_width // (2 * pairs)
    gate = jnp.dot(flat_rows, gate_weight[0], preferred_element_type=jnp.float32)
    upward = jnp.dot(flat_rows, up_weight[0], preferred_element_type=jnp.float32)
    hidden = (jax.nn.silu(gate) * upward).astype(jnp.bfloat16)
    partial_value = jnp.dot(hidden, down_weight[0], preferred_element_type=jnp.float32).astype(
        jnp.bfloat16
    )
    pieces = lax.all_to_all(partial_value[None], "tp", split_axis=2, concat_axis=0, tiled=True)
    paired = pieces.reshape(pairs, 2, rows, columns).astype(jnp.float32)
    expert_value = (
        (paired[:, 0] + paired[:, 1])
        .astype(jnp.bfloat16)
        .reshape(pairs, count, rows // count, columns)
    )
    returned = lax.all_to_all(expert_value, "ep", split_axis=1, concat_axis=1, tiled=True)
    return returned.reshape(-1, columns)


def expert_half(
    expert_input_rows,
    expert_norm_gain,
    selected_expert_index,
    selected_expert_weight,
    routed_gate_weight,
    routed_up_weight,
    routed_down_weight,
    common_gate_weight,
    common_up_weight,
    common_down_weight,
):
    tok_rows, model_width = expert_input_rows.shape
    chosen_count = selected_expert_index.shape[1]
    ep_count = lax.axis_size("ep")
    tp_count = lax.axis_size("tp")
    group_count = tp_count // 2
    expert_total = group_count * ep_count
    capacity = 2 * tok_rows * chosen_count // expert_total
    column_count = model_width // tp_count
    tp_place = lax.axis_index("tp")
    group_index = tp_place // 2
    normed = rms_scale(expert_input_rows, expert_norm_gain).astype(jnp.bfloat16)
    assigned = selected_expert_index.reshape(-1)
    assign_count = assigned.shape[0]
    expert_ids = jnp.arange(expert_total, dtype=jnp.int32)
    onehot = (assigned[:, None] == expert_ids[None, :]).astype(jnp.int32)
    ranking = jnp.sum((jnp.cumsum(onehot, axis=0) - onehot) * onehot, axis=1)
    target = jnp.where(
        assigned % group_count == group_index, assigned // group_count * capacity + ranking, -1
    ).reshape(tok_rows, chosen_count)
    slots = jnp.arange(ep_count * capacity, dtype=jnp.int32)
    placing = jnp.any(target[:, :, None] == slots[None, None, :], axis=1).astype(jnp.bfloat16)
    outgoing = lax.dot_general(
        placing, normed, (((0,), (0,)), ((), ())), preferred_element_type=jnp.float32
    ).astype(jnp.bfloat16)
    arrived = lax.all_to_all(
        outgoing.reshape(ep_count, capacity, model_width),
        "ep",
        split_axis=0,
        concat_axis=0,
        tiled=True,
    ).reshape(-1, model_width)
    if capacity % 16 == 0 and column_count % 128 == 0:
        flat_back = routed_by_kernel(
            arrived, routed_gate_weight, routed_up_weight, routed_down_weight, ep_count, group_count
        ).reshape(-1, column_count)
    else:
        flat_back = routed_by_exchange(
            arrived, routed_gate_weight, routed_up_weight, routed_down_weight, ep_count, group_count
        )
    position = (
        assigned % group_count * (ep_count * capacity)
        + assigned // group_count * capacity
        + ranking
    )
    picked = (
        jnp.take(flat_back, position, axis=0)
        .astype(jnp.float32)
        .reshape(tok_rows, chosen_count, column_count)
    )
    routed = jnp.sum(picked * selected_expert_weight[:, :, None], axis=1)
    shared_hidden = (
        jax.nn.silu(jnp.dot(normed, common_gate_weight, preferred_element_type=jnp.float32))
        * jnp.dot(normed, common_up_weight, preferred_element_type=jnp.float32)
    ).astype(jnp.bfloat16)
    shared_sum = lax.psum_scatter(
        lax.dot_general(
            common_down_weight,
            shared_hidden,
            (((0,), (1,)), ((), ())),
            preferred_element_type=jnp.float32,
        ).astype(jnp.bfloat16),
        "tp",
        scatter_dimension=0,
        tiled=True,
    ).astype(jnp.float32)
    return (routed + shared_sum.T).astype(jnp.bfloat16)


def mm(x, y, dims=NN):
    return lax.dot_general(x, y, (dims, ((), ())), preferred_element_type=jnp.float32)


def pair_masks():
    lane = lax.broadcasted_iota(jnp.int32, (BLOCK, 2 * HEAD_CHANNELS), 1)
    first = jnp.where(lane < HEAD_CHANNELS, 1.0, 0.0)
    return first.astype(jnp.bfloat16), (1.0 - first).astype(jnp.bfloat16)


def stacked(y, masks):
    return jnp.concatenate([y * masks[0], y * masks[1]], axis=0)


def pair_dot(x, parts):
    xh, xl = split_parts(x)
    high, low = parts
    return mm(jnp.concatenate([xh, xl], axis=1), jnp.concatenate([high, high], axis=0)) + mm(
        xh, low
    )


def short_dot(x, y, masks):
    return mm(x.astype(jnp.bfloat16), stacked(y.astype(jnp.bfloat16), masks))


def pair_parts(y, masks):
    yh, yl = split_parts(y)
    return stacked(yh, masks), stacked(yl, masks)


def side_by_side(one, two):
    return tuple(jnp.concatenate([p, q], axis=1) for p, q in zip(one, two))


def head_sum(x, block_ones):
    xh, xl = split_parts(x)
    return mm(jnp.concatenate([xh, xl], axis=1), block_ones)


def head_ones():
    wide = 2 * HEAD_CHANNELS
    row = lax.broadcasted_iota(jnp.int32, (2 * wide, wide), 0)
    col = lax.broadcasted_iota(jnp.int32, (2 * wide, wide), 1)
    same = (row // HEAD_CHANNELS) % 2 == col // HEAD_CHANNELS
    return jnp.where(same, 1.0, 0.0).astype(jnp.bfloat16)


def local_math(r_ref, k_ref, v_ref, dec_ref, lr_ref, off_ref, spike_ref):
    rows, width = r_ref.shape
    wide = 2 * HEAD_CHANNELS
    pairs = width // wide
    chunks = rows // BLOCK
    masks = pair_masks()
    ones_head = head_ones()
    row = lax.broadcasted_iota(jnp.int32, (BLOCK, wide), 0)
    col = lax.broadcasted_iota(jnp.int32, (BLOCK, wide), 1) % HEAD_CHANNELS
    strict = col < row
    inclusive = col <= row
    trow = lax.broadcasted_iota(jnp.int32, (BLOCK, 4 * BLOCK), 0)
    tcol = lax.broadcasted_iota(jnp.int32, (BLOCK, 4 * BLOCK), 1)
    running = jnp.where((tcol % BLOCK <= trow) & (tcol < 3 * BLOCK), 1.0, 0.0).astype(jnp.bfloat16)
    blank = jnp.zeros((BLOCK, wide), jnp.bfloat16)
    items = [(i, p) for i in range(chunks) for p in range(pairs)]
    spans = [slice(i * BLOCK, (i + 1) * BLOCK) for i in range(chunks)]
    strips = [slice(p * wide, (p + 1) * wide) for p in range(pairs)]
    pre = off_ref[...] + jnp.tanh(dec_ref[...].astype(jnp.float32))
    log = spike_ref[...] - jax.nn.sigmoid(pre) * jnp.exp(jnp.float32(-0.5))
    p0 = log.astype(jnp.bfloat16)
    rest = log - p0.astype(jnp.float32)
    p1 = rest.astype(jnp.bfloat16)
    p2 = (rest - p1.astype(jnp.float32)).astype(jnp.bfloat16)
    empty = jnp.zeros((BLOCK, width), jnp.bfloat16)
    cums = [
        mm(running, jnp.concatenate([p0[span], p1[span], p2[span], empty], axis=0))
        for span in spans
    ]
    k_all = k_ref[...].astype(jnp.float32)
    squares = k_all * k_all
    sums = [head_sum(squares[:, strip], ones_head) for strip in strips]
    learn = jax.nn.sigmoid(lr_ref[...].astype(jnp.float32))
    scale = jnp.concatenate([lax.rsqrt(q + NORM_EPSILON) for q in sums], axis=1)
    cum_all = jnp.concatenate(cums, axis=0)
    back = learn * k_all * jnp.exp(-cum_all)
    b_all = back * scale
    a_all = k_all * scale * jnp.exp(cum_all - log)
    r_all = r_ref[...].astype(jnp.float32) * jnp.exp(cum_all)
    bh_all, bl_all = split_parts(b_all)
    ih_all, il_all = split_parts(back)
    ah_all, al_all = split_parts(a_all)
    rh_all, rl_all = split_parts(r_all)
    chunk_ends = [jnp.exp(c[BLOCK - 1 :]) for c in cums]
    grams = []
    for i, p in items:
        at = (spans[i], strips[p])
        left_high = jnp.concatenate([ah_all[at], rh_all[at]], axis=0)
        left_low = jnp.concatenate([al_all[at], rl_all[at]], axis=0)
        right_high = jnp.concatenate(
            [stacked(bh_all[at], masks), stacked(ih_all[at], masks)], axis=0
        )
        right_low = jnp.concatenate(
            [stacked(bl_all[at], masks), stacked(il_all[at], masks)], axis=0
        )
        grams.append(
            mm(
                jnp.concatenate([left_high, left_low], axis=1),
                jnp.concatenate([right_high, right_high], axis=1),
                NT,
            )
            + mm(left_high, right_low, NT)
        )
    lows = [jnp.where(strict, gram[:BLOCK, :wide], 0.0) for gram in grams]
    out_bs = [jnp.where(inclusive, gram[BLOCK:, :wide], 0.0) for gram in grams]
    vs = [v_ref[spans[i], strips[p]] for i, p in items]
    weighted = []
    for n, gram in enumerate(grams):
        kh, kl = split_parts(
            jnp.concatenate(
                [
                    jnp.where(strict, gram[:BLOCK, wide:], 0.0),
                    jnp.where(inclusive, gram[BLOCK:, wide:], 0.0),
                ],
                axis=0,
            )
        )
        values = stacked(vs[n], masks)
        weighted.append(
            mm(jnp.concatenate([kh, kl], axis=1), jnp.concatenate([values, values], axis=0))
        )
    low_vs = [w[:BLOCK] for w in weighted]
    out_vs = [w[BLOCK:] for w in weighted]
    ends = [chunk_ends[i][:, strips[p]] for i, p in items]
    ins_ends = [back[spans[i], strips[p]] * ends[n] for n, (i, p) in enumerate(items)]
    b_ends = [b_all[spans[i], strips[p]] * ends[n] for n, (i, p) in enumerate(items)]
    r_outs = [r_all[spans[i], strips[p]] for i, p in items]
    a_ins = [a_all[spans[i], strips[p]] for i, p in items]
    count = range(len(items))
    eye = jnp.where(row == col, 1.0, 0.0)
    inverses = None
    size = 1
    while size < BLOCK:
        inside = (row // (2 * size) == col // (2 * size)) & (row // size != col // size)
        corners = [jnp.where(inside, low, 0.0) for low in lows]
        if size == 1:
            inverses = [eye - corner for corner in corners]
        else:
            exact = 2 * size >= BLOCK
            firsts = [
                pair_dot(inverses[n], pair_parts(corners[n], masks))
                if exact
                else short_dot(inverses[n], corners[n], masks)
                for n in count
            ]
            changes = [
                pair_dot(firsts[n], pair_parts(inverses[n], masks))
                if exact
                else short_dot(firsts[n], inverses[n], masks)
                for n in count
            ]
            inverses = [inverses[n] - changes[n] for n in count]
        size *= 2
    solved = [
        side_by_side(pair_parts(a_ins[n], masks), pair_parts(low_vs[n], masks)) for n in count
    ]
    solved = [pair_dot(inverses[n], solved[n]) for n in count]
    brow = lax.broadcasted_iota(jnp.int32, (wide, 2 * wide), 0)
    bcol = lax.broadcasted_iota(jnp.int32, (wide, 2 * wide), 1)
    same_head = brow // HEAD_CHANNELS == (bcol % wide) // HEAD_CHANNELS
    diagonal = brow == bcol
    maps = []
    for n in count:
        left = jnp.concatenate([-b_ends[n], ins_ends[n]], axis=0)
        lh, ll = split_parts(left)
        uh, ul = split_parts(solved[n])
        high = jnp.concatenate([uh, jnp.concatenate([blank, vs[n]], axis=1)], axis=0)
        low = jnp.concatenate([ul, jnp.concatenate([blank, blank], axis=1)], axis=0)
        made = mm(
            jnp.concatenate([lh, ll], axis=0), jnp.concatenate([high, high], axis=0), TN
        ) + mm(lh, low, TN)
        end = jnp.concatenate([ends[n], ends[n]], axis=1)
        maps.append(jnp.where(same_head, made + jnp.where(diagonal, end, 0.0), 0.0))
    def after(second, first):
        joined = pair_dot(second[:, :wide], split_parts(first))
        return jnp.concatenate([joined[:, :wide], joined[:, wide:] + second[:, wide:]], axis=1)

    by_pair = [maps[p::pairs] for p in range(pairs)]
    stage = [list(row) for row in by_pair]
    tree = [stage]
    while len(stage[0]) > 1:
        stage = [
            [
                after(row[i + 1], row[i]) if i + 1 < len(row) else row[i]
                for i in range(0, len(row), 2)
            ]
            for row in stage
        ]
        tree.append(stage)
    whole = [row[0] for row in stage]

    def reaching(p, i):
        result, done = None, 0
        for depth in range(len(tree) - 1, -1, -1):
            if i - done >= 1 << depth:
                piece = tree[depth][p][done >> depth]
                result = piece if result is None else after(piece, result)
                done += 1 << depth
        return result

    compact = [m[:HEAD_CHANNELS] + m[HEAD_CHANNELS:] for m in whole]

    def finish():
        results = {}
        for n in count:
            uh, ul = split_parts(solved[n])
            parts = [
                jnp.concatenate([stacked(u[:, :wide], masks), stacked(u[:, wide:], masks)], axis=1)
                for u in (uh, ul)
            ]
            removed = pair_dot(out_bs[n], parts)
            carry = r_outs[n] - removed[:, :wide]
            value = out_vs[n] - removed[:, wide:]
            entry = reaching(items[n][1], items[n][0])
            if entry is not None:
                moved = pair_dot(carry, split_parts(entry))
                carry = moved[:, :wide]
                value = value + moved[:, wide:]
            results[items[n]] = (carry, value)
        return results

    return compact, finish


def flipped_rows(index, bits, count):
    result, unit = 0, 1
    while unit < count:
        digit = (index // unit) % 2
        result = result + unit * ((digit + bits // unit) % 2)
        unit *= 2
    return result


def mega_kernel(ep_count, *refs):
    inputs = refs[:21]
    attn_out, expert_out = refs[21:23]
    copies = refs[23:44]
    (
        r_ref, k_ref, v_ref, dec_ref, lr_ref, gate_ref, off_ref, spike_ref, hgain_ref, wout_ref,
        pgain_ref, x_ref, egain_ref, idx_ref, wsel_ref, wg_ref, wu_ref, wd_ref, cg_ref, cu_ref,
        cd_ref,
    ) = copies
    (
        normed, outgoing, arrived, carry_ref, value_ref, own_map, held, base_state, state,
        next_state, shared, shared_half, shared_sum, shared_last, crossing,
        halves, own_ref, final, back, heads_ref, mix, mix_half, mix_sum, mix_last,
        load_sem, disp_send, disp_recv, fwd_send, fwd_recv, map_send, map_recv, base_send,
        base_recv, sh_send, sh_recv, cross_send, cross_recv, home_send, home_recv, mx_send,
        mx_recv, tail_send, tail_recv,
    ) = refs[44:]
    me = lax.axis_index("ep")
    place = lax.axis_index("tp")
    group = place // 2
    half = place % 2
    other = 1 - half
    partner = 2 * group + other
    across = 2 * (1 - group) + half
    level = me // 4
    member = me % 4
    levels = ep_count // 4
    tok_rows, model_width = x_ref.shape
    slots = outgoing.shape[0]
    capacity = slots // ep_count
    fold = model_width // 2
    columns = model_width // 4
    rows, width = r_ref.shape
    wide = 2 * HEAD_CHANNELS
    pairs = width // wide
    block_rows = rows // 4
    quarter = ep_count // 4
    outer = (level + member // 2 + 1) % 2
    first_start = quarter * (2 + outer)
    second_start = quarter * (3 - outer)
    first_batch = [first_start + n for n in range(quarter)]
    second_batch = [second_start + n for n in range(quarter)]
    near_batch = list(range(2 * quarter))

    barrier = pltpu.get_barrier_semaphore()

    def peer(bits):
        return flipped_rows(me, bits, ep_count)

    def tp_of(turn):
        return 2 * lax.rem(group + turn, 2) + half

    for bits in range(ep_count):
        for turn in range(2):
            if bits or turn:
                pl.semaphore_signal(
                    barrier,
                    inc=1,
                    device_id={"ep": peer(bits), "tp": tp_of(turn)},
                    device_id_type=MESH,
                )
    pl.semaphore_signal(barrier, inc=1, device_id={"tp": partner}, device_id_type=MESH)

    loads = [
        pltpu.make_async_copy(source, target, load_sem.at[n])
        for n, (source, target) in enumerate(zip(inputs, copies))
    ]
    for n in (13, 14, 11, 12, 0, 1, 2, 3, 4, 6, 7, 18, 19, 20, 15, 16, 17, 5, 8, 9, 10):
        loads[n].start()

    def rows_of(bits):
        if isinstance(bits, int):
            return slice(bits * capacity, (bits + 1) * capacity)
        return pl.ds(pl.multiple_of(bits * capacity, capacity), capacity)

    def remote(source, target, send, recv, where):
        return pltpu.make_async_remote_copy(
            src_ref=source,
            dst_ref=target,
            send_sem=send,
            recv_sem=recv,
            device_id=where,
            device_id_type=MESH,
        )

    def dispatch(bits):
        return remote(
            outgoing.at[rows_of(bits)],
            arrived.at[half, rows_of(bits)],
            disp_send.at[bits],
            disp_recv.at[bits],
            {"ep": peer(bits)},
        )

    def forward(bits):
        return remote(
            arrived.at[half, rows_of(bits)],
            arrived.at[half, rows_of(bits)],
            fwd_send.at[bits],
            fwd_recv.at[bits],
            {"tp": partner},
        )

    for n in (13, 14):
        loads[n].wait()
    chosen_count = idx_ref.shape[0]
    experts = 2 * ep_count
    expert_row = lax.broadcasted_iota(jnp.int32, (experts, tok_rows), 0)
    named = [expert_row == idx_ref[k : k + 1, :] for k in range(chosen_count)]
    chosen = functools.reduce(jnp.logical_or, named)
    weight_of = functools.reduce(
        jnp.add, [jnp.where(n, wsel_ref[k : k + 1, :], 0.0) for k, n in enumerate(named)]
    )
    early = lax.broadcasted_iota(jnp.int32, (tok_rows, tok_rows), 0) < lax.broadcasted_iota(
        jnp.int32, (tok_rows, tok_rows), 1
    )
    rank = mm(
        jnp.where(chosen, 1.0, 0.0).astype(jnp.bfloat16),
        jnp.where(early, 1.0, 0.0).astype(jnp.bfloat16),
    )
    rank = jnp.where(chosen, rank, -1.0).astype(jnp.bfloat16)
    slot = lax.broadcasted_iota(jnp.int32, (slots, experts), 0)
    which = lax.broadcasted_iota(jnp.int32, (slots, experts), 1)
    there = flipped_rows(me, slot // capacity, ep_count)
    mine = jnp.where(which == 2 * there + group, 1.0, 0.0).astype(jnp.bfloat16)
    slot_rank = (
        lax.broadcasted_iota(jnp.int32, (slots, tok_rows), 0) % capacity
    ).astype(jnp.float32)
    placing = jnp.where(mm(mine, rank) == slot_rank, 1.0, 0.0).astype(jnp.bfloat16)
    for n in (11, 12):
        loads[n].wait()
    normed[...] = rms_scale(x_ref[...], egain_ref[...]).astype(jnp.bfloat16)
    fold_span = pl.ds(pl.multiple_of(half * fold, fold), fold)
    other_span = pl.ds(pl.multiple_of(other * fold, fold), fold)
    outgoing[...] = mm(placing, normed[:, fold_span]).astype(jnp.bfloat16)
    pl.semaphore_wait(barrier, 2 * ep_count)
    order = list(range(2 * quarter, ep_count)) + near_batch[1:]
    for bits in order[: 2 * quarter]:
        dispatch(bits).start()

    @pl.when(outer == 0)
    def _():
        for bits in order[2 * quarter :]:
            dispatch(bits).start()

    arrived[half, rows_of(0), :] = outgoing[rows_of(0), :]
    arrived[other, rows_of(0), :] = mm(placing[:capacity], normed[:, other_span]).astype(
        jnp.bfloat16
    )

    for n in (0, 1, 2, 3, 4, 6, 7):
        loads[n].wait()
    compact, finish = local_math(r_ref, k_ref, v_ref, dec_ref, lr_ref, off_ref, spike_ref)
    for p in range(pairs):
        own_map[p] = compact[p].astype(jnp.bfloat16)
    masks = pair_masks()

    def give(there):
        return remote(
            own_map,
            held.at[member],
            map_send.at[there],
            map_recv.at[member],
            {"ep": 4 * level + there},
        )

    def taken(source):
        return remote(
            own_map, held.at[source], map_send.at[0], map_recv.at[source], {"ep": peer(1)}
        )

    def gives(there):
        above_me = member < there
        return above_me | (member == 3) if there == 2 else above_me

    for there in (3, 2, 1):

        @pl.when(gives(there))
        def _():
            give(there).start()

    for (i, p), (carry, value) in finish().items():
        span = slice(i * BLOCK, (i + 1) * BLOCK)
        lanes = slice(p * wide, (p + 1) * wide)
        carry_ref[span, lanes] = carry
        value_ref[span, lanes] = value

    for n in (18, 19, 20):
        loads[n].wait()
    rows_in = normed[...]
    hidden = (jax.nn.silu(mm(rows_in, cg_ref[...])) * mm(rows_in, cu_ref[...])).astype(
        jnp.bfloat16
    )
    for j in range(4):
        shared[j] = mm(hidden, cd_ref[:, j * columns : (j + 1) * columns]).astype(jnp.bfloat16)

    def shared_cross(turn):
        there = 2 * lax.rem(group + turn, 2) + other
        return remote(
            shared.at[there],
            shared_half.at[turn],
            sh_send.at[turn],
            sh_recv.at[turn],
            {"tp": partner},
        )

    for turn in (1, 0):
        shared_cross(turn).start()

    def take_in(batch):
        for bits in batch:
            if not isinstance(bits, int) or bits:
                dispatch(bits).wait_recv()
                forward(bits).start()

    for turn in (1, 0):
        shared_cross(turn).wait_recv()
        shared_sum[turn] = shared[tp_of(turn)].astype(jnp.float32) + shared_half[turn].astype(
            jnp.float32
        )
    shared_last[0] = shared_sum[1].astype(jnp.bfloat16)
    shared_tail = remote(
        shared_last.at[0], shared_last.at[1], tail_send.at[0], tail_recv.at[0], {"tp": across}
    )
    shared_tail.start()
    take_in(first_batch)

    @pl.when(outer == 1)
    def _():
        for bits in order[2 * quarter :]:
            dispatch(bits).start()

    def wait_far(batch):
        for bits in batch:
            if not isinstance(bits, int) or bits:
                forward(bits).wait_recv()

    def cross(batch_index, turn, span):
        return remote(
            crossing.at[turn, span],
            halves.at[turn, span],
            cross_send.at[batch_index, turn],
            cross_recv.at[batch_index, turn],
            {"tp": partner},
        )

    def home(turn, bits):
        return remote(
            final.at[turn, rows_of(bits)],
            back.at[group, rows_of(bits)],
            home_send.at[turn, bits],
            home_recv.at[turn, bits],
            {"ep": peer(bits), "tp": tp_of(turn)},
        )

    def span_of(batch):
        if isinstance(batch[0], int):
            return slice(0, len(batch) * capacity)
        size = quarter * capacity
        return pl.ds(pl.multiple_of(batch[0] * capacity, size), size)

    def feed(batch_index, batch):
        span = span_of(batch)
        near, away = arrived[0, span, :], arrived[1, span, :]
        gate = mm(near, wg_ref[:fold, :]) + mm(away, wg_ref[fold:, :])
        upper = mm(near, wu_ref[:fold, :]) + mm(away, wu_ref[fold:, :])
        routed_hidden = (jax.nn.silu(gate) * upper).astype(jnp.bfloat16)

        def part(index):
            lanes = pl.ds(pl.multiple_of(index * columns, columns), columns)
            return mm(routed_hidden, wd_ref[:, lanes])

        for turn in (1, 0):
            crossing[turn, span, :] = part(2 * lax.rem(group + turn, 2) + other).astype(
                jnp.bfloat16
            )
            cross(batch_index, turn, span).start()
        for turn in (1, 0):
            own_ref[turn, span, :] = part(2 * lax.rem(group + turn, 2) + half)

    def send_home(batch_index, batch):
        span = span_of(batch)
        for turn in (1, 0):
            cross(batch_index, turn, span).wait_recv()
            final[turn, span, :] = (
                own_ref[turn, span, :] + halves[turn, span, :].astype(jnp.float32)
            ).astype(jnp.bfloat16)
            for bits in batch:
                if not isinstance(bits, int) or bits or turn:
                    home(turn, bits).start()
                else:
                    back[group, rows_of(0), :] = final[0, rows_of(0), :]

    for n in (15, 16, 17):
        loads[n].wait()
    wait_far(first_batch)
    feed(0, first_batch)
    def moved_by(block, p, current):
        through = block[p, :, :wide]
        high, low = pair_parts(current, masks)
        return mm(
            jnp.concatenate([through, through], axis=1), jnp.concatenate([high, low], axis=0)
        ) + block[p, :, wide:].astype(jnp.float32)

    def above(turn):
        return remote(
            next_state,
            base_state,
            base_send.at[turn],
            base_recv.at[0],
            {"ep": lax.rem(4 * (level + 1) + 2 * turn + member % 2, ep_count)},
        )

    hands_on = (member >= 2) & (level + 1 < levels)

    def settle():
        for p in range(pairs):
            state[p] = base_state[p].astype(jnp.float32)
        for source in range(3):

            @pl.when(source < member)
            def _():
                taken(source).wait_recv()
                for p in range(pairs):
                    state[p] = moved_by(held.at[source], p, state[p])

        @pl.when(member == 2)
        def _():
            taken(3).wait_recv()

        @pl.when(hands_on)
        def _():
            for p in range(pairs):
                once = moved_by(own_map, p, state[p])
                twice = moved_by(held.at[3], p, once)
                next_state[p] = jnp.where(member == 2, twice, once).astype(jnp.bfloat16)
            for turn in range(2):
                above(turn).start()

    @pl.when(level == 0)
    def _():
        base_state[...] = jnp.zeros_like(base_state)
        settle()

    for n in (5, 8, 9, 10):
        loads[n].wait()

    def mix_cross(turn):
        there = 2 * lax.rem(group + turn, 2) + other
        return remote(
            mix.at[there],
            mix_half.at[turn],
            mx_send.at[turn],
            mx_recv.at[turn],
            {"tp": partner},
        )

    def project(turn):
        there = lax.rem(group + turn, 2)
        rows_there = pl.ds(pl.multiple_of(there * 2 * block_rows, 2 * block_rows), 2 * block_rows)
        rows_made = heads_ref[rows_there, :]
        for j in range(4):
            span = slice(j * columns, (j + 1) * columns)
            made = mm(rows_made, wout_ref[:, span]).astype(jnp.bfloat16)
            for b in range(2):
                mix[2 * there + b, :, span] = made[b * block_rows : (b + 1) * block_rows]

    def attend():
        ones_head = head_ones()
        for p in range(pairs):
            lanes = slice(p * wide, (p + 1) * wide)
            value = value_ref[:, lanes] + pair_dot(
                carry_ref[:, lanes], pair_parts(state[p], masks)
            )
            centred = value - head_sum(value, ones_head) * (1.0 / HEAD_CHANNELS)
            spread = head_sum(centred * centred, ones_head) * (1.0 / HEAD_CHANNELS)
            heads_ref[:, lanes] = (
                centred
                * lax.rsqrt(spread + GROUP_EPSILON)
                * hgain_ref[:, lanes]
                * jax.nn.sigmoid(gate_ref[:, lanes].astype(jnp.float32))
            ).astype(jnp.bfloat16)
        for turn in (1, 0):
            project(turn)
            mix_cross(turn).start()

    mix_tail = remote(
        mix_last.at[0], mix_last.at[1], tail_send.at[1], tail_recv.at[1], {"tp": across}
    )

    def pass_mix():
        mix_cross(1).wait_recv()
        mix_last[0] = (
            mix[across].astype(jnp.float32) + mix_half[1].astype(jnp.float32)
        ).astype(jnp.bfloat16)
        mix_tail.start()

    @pl.when(level == 0)
    def _():
        attend()

    send_home(0, first_batch)
    take_in(near_batch)
    @pl.when(level == 0)
    def _():
        pass_mix()

    wait_far(near_batch)
    feed(1, near_batch)
    take_in(second_batch)
    send_home(1, near_batch)

    last_first = (level > 0) & (outer == 1)

    def feed_last():
        wait_far(second_batch)
        feed(2, second_batch)
        send_home(2, second_batch)

    @pl.when(last_first)
    def _():
        feed_last()

    @pl.when(level > 0)
    def _():
        above(0).wait_recv()
        settle()

    @pl.when(level > 0)
    def _():
        attend()

    @pl.when(level > 0)
    def _():
        pass_mix()

    @pl.when(jnp.logical_not(last_first))
    def _():
        feed_last()

    mix_cross(0).wait_recv()
    mix_sum[...] = mix[place].astype(jnp.float32) + mix_half[0].astype(jnp.float32)

    all_slots = 2 * slots
    slot = lax.broadcasted_iota(jnp.int32, (experts, all_slots), 1)
    which = lax.broadcasted_iota(jnp.int32, (experts, all_slots), 0)
    there = flipped_rows(me, (slot % slots) // capacity, ep_count)
    holder = jnp.where(which == 2 * there + slot // slots, 1.0, 0.0).astype(jnp.bfloat16)
    slot_rank = (
        lax.broadcasted_iota(jnp.int32, (tok_rows, all_slots), 1) % capacity
    ).astype(jnp.float32)
    hit = mm(rank, holder, TN) == slot_rank
    weight_high, weight_low = split_parts(weight_of)
    picks = [
        jnp.where(hit, mm(w, holder, TN), 0.0).astype(jnp.bfloat16)
        for w in (weight_high, weight_low)
    ]
    shared_tail.wait_recv()
    base = shared_sum[0] + shared_last[1].astype(jnp.float32)
    for turn in range(2):
        for bits in first_batch:
            home(turn, bits).wait_recv()
    for turn in range(2):
        for bits in near_batch:
            if bits or turn:
                home(turn, bits).wait_recv()
    for turn in range(2):
        for bits in second_batch:
            home(turn, bits).wait_recv()
    returned = back[...].reshape(all_slots, columns)
    routed = mm(
        jnp.concatenate(picks, axis=1), jnp.concatenate([returned, returned], axis=0)
    )
    expert_out[...] = (routed + base).astype(jnp.bfloat16)

    mix_tail.wait_recv()
    total = mix_sum[...] + mix_last[1].astype(jnp.float32)
    attn_out[...] = rms_scale(total, pgain_ref[...]).astype(jnp.bfloat16)

    for bits in order:
        dispatch(bits).wait_send()
        forward(bits).wait_send()
    for there in (3, 2, 1):

        @pl.when(gives(there))
        def _():
            give(there).wait_send()

    @pl.when(hands_on)
    def _():
        for turn in range(2):
            above(turn).wait_send()

    for turn in range(2):
        shared_cross(turn).wait_send()
        mix_cross(turn).wait_send()
        for n, batch in enumerate((first_batch, near_batch, second_batch)):
            cross(n, turn, span_of(batch)).wait_send()
        for bits in range(ep_count):
            if bits or turn:
                home(turn, bits).wait_send()
    shared_tail.wait_send()
    mix_tail.wait_send()


def mega(
    receptance, head_key_input, head_value_input, decay_input_part, learning_rate_input,
    output_gate_input, decay_channel_offset, spike_log_decay, head_norm_gain, head_output_weight,
    projection_norm_gain, expert_input_rows, expert_norm_gain, selected_expert_index,
    selected_expert_weight, routed_gate_weight, routed_up_weight, routed_down_weight,
    common_gate_weight, common_up_weight, common_down_weight,
):
    ep_count = lax.axis_size("ep")
    rows, width = receptance.shape
    tok_rows, model_width = expert_input_rows.shape
    chosen = selected_expert_index.shape[1]
    capacity = tok_rows * chosen // ep_count
    slots = ep_count * capacity
    columns = model_width // 4
    wide = 2 * HEAD_CHANNELS
    pairs = width // wide
    operands = (
        receptance, head_key_input, head_value_input, decay_input_part, learning_rate_input,
        output_gate_input, decay_channel_offset[None, :], spike_log_decay, head_norm_gain[None, :],
        head_output_weight, projection_norm_gain[None, :], expert_input_rows,
        expert_norm_gain[None, :], selected_expert_index.T, selected_expert_weight.T,
        routed_gate_weight[0], routed_up_weight[0], routed_down_weight[0], common_gate_weight,
        common_up_weight, common_down_weight,
    )
    bf16, f32 = jnp.bfloat16, jnp.float32
    dma = pltpu.SemaphoreType.DMA
    scratch = [pltpu.VMEM(o.shape, o.dtype) for o in operands] + [
        pltpu.VMEM((tok_rows, model_width), bf16),
        pltpu.VMEM((slots, model_width // 2), bf16),
        pltpu.VMEM((2, slots, model_width // 2), bf16),
        pltpu.VMEM((rows, width), f32),
        pltpu.VMEM((rows, width), f32),
        pltpu.VMEM((pairs, HEAD_CHANNELS, 2 * wide), bf16),
        pltpu.VMEM((4, pairs, HEAD_CHANNELS, 2 * wide), bf16),
        pltpu.VMEM((pairs, HEAD_CHANNELS, wide), bf16),
        pltpu.VMEM((pairs, HEAD_CHANNELS, wide), f32),
        pltpu.VMEM((pairs, HEAD_CHANNELS, wide), bf16),
        pltpu.VMEM((4, tok_rows, columns), bf16),
        pltpu.VMEM((2, tok_rows, columns), bf16),
        pltpu.VMEM((2, tok_rows, columns), f32),
        pltpu.VMEM((2, tok_rows, columns), bf16),
        pltpu.VMEM((2, slots, columns), bf16),
        pltpu.VMEM((2, slots, columns), bf16),
        pltpu.VMEM((2, slots, columns), f32),
        pltpu.VMEM((2, slots, columns), bf16),
        pltpu.VMEM((2, slots, columns), bf16),
        pltpu.VMEM((rows, width), bf16),
        pltpu.VMEM((4, rows // 4, model_width), bf16),
        pltpu.VMEM((2, rows // 4, model_width), bf16),
        pltpu.VMEM((rows // 4, model_width), f32),
        pltpu.VMEM((2, rows // 4, model_width), bf16),
        dma((len(operands),)),
    ]
    scratch += [dma((ep_count,))] * 4
    scratch += [dma((4,))] * 2
    scratch += [dma((2,))] * 4
    scratch += [dma((3, 2))] * 2
    scratch += [dma((2, ep_count))] * 2
    scratch += [dma((2,))] * 4
    full = pl.BlockSpec(memory_space=pltpu.VMEM)
    return pl.pallas_call(
        functools.partial(mega_kernel, ep_count),
        out_shape=(
            pltpu.VMEM((rows // 4, model_width), bf16),
            pltpu.VMEM((tok_rows, columns), bf16),
        ),
        in_specs=[pl.BlockSpec(memory_space=pl.ANY)] * len(operands),
        out_specs=(full, full),
        scratch_shapes=scratch,
        compiler_params=pltpu.CompilerParams(collective_id=0, has_side_effects=True),
    )(*operands)


def fits_mega(receptance, expert_input_rows, selected_expert_index):
    ep_count = lax.axis_size("ep")
    rows, width = receptance.shape
    tok_rows, model_width = expert_input_rows.shape
    assigned = tok_rows * selected_expert_index.shape[1]
    return (
        lax.axis_size("tp") == 4
        and ep_count >= 4
        and ep_count & (ep_count - 1) == 0
        and width % (2 * HEAD_CHANNELS) == 0
        and rows % (4 * BLOCK) == 0
        and assigned % (16 * ep_count) == 0
        and tok_rows % 128 == 0
        and tok_rows <= 256
        and model_width % 512 == 0
    )


def body(
    receptance,
    head_key_input,
    head_value_input,
    decay_input_part,
    learning_rate_input,
    output_gate_input,
    decay_channel_offset,
    spike_log_decay,
    head_norm_gain,
    head_output_weight,
    projection_norm_gain,
    expert_input_rows,
    expert_norm_gain,
    selected_expert_index,
    selected_expert_weight,
    routed_gate_weight,
    routed_up_weight,
    routed_down_weight,
    common_gate_weight,
    common_up_weight,
    common_down_weight,
):
    if fits_mega(receptance, expert_input_rows, selected_expert_index):
        return mega(
            receptance, head_key_input, head_value_input, decay_input_part, learning_rate_input,
            output_gate_input, decay_channel_offset, spike_log_decay, head_norm_gain,
            head_output_weight, projection_norm_gain, expert_input_rows, expert_norm_gain,
            selected_expert_index, selected_expert_weight, routed_gate_weight, routed_up_weight,
            routed_down_weight, common_gate_weight, common_up_weight, common_down_weight,
        )
    attention_output = attention_mixer(
        receptance,
        head_key_input,
        head_value_input,
        decay_input_part,
        learning_rate_input,
        output_gate_input,
        decay_channel_offset,
        spike_log_decay,
        head_norm_gain,
        head_output_weight,
        projection_norm_gain,
    )
    expert_output = expert_half(
        expert_input_rows,
        expert_norm_gain,
        selected_expert_index,
        selected_expert_weight,
        routed_gate_weight,
        routed_up_weight,
        routed_down_weight,
        common_gate_weight,
        common_up_weight,
        common_down_weight,
    )
    return (attention_output, expert_output)


def solution(mesh):
    placed = (
        P("ep", "tp"),
        P("ep", "tp"),
        P("ep", "tp"),
        P("ep", "tp"),
        P("ep", "tp"),
        P("ep", "tp"),
        P("tp"),
        P("ep", "tp"),
        P("tp"),
        P("tp", None),
        P(),
        P("ep", None),
        P(),
        P("ep", None),
        P("ep", None),
        P(("ep", "tp"), None, None),
        P(("ep", "tp"), None, None),
        P(("ep", "tp"), None, None),
        P(None, "tp"),
        P(None, "tp"),
        P("tp", None),
    )
    return jax.shard_map(
        body,
        mesh=mesh,
        in_specs=placed,
        out_specs=(P(("ep", "tp"), None), P("ep", "tp")),
        check_vma=False,
    )
```

```python
import functools

import jax
import jax.numpy as jnp
from jax import lax
from jax.experimental import pallas as pl
from jax.experimental.pallas import tpu as pltpu
from jax.sharding import PartitionSpec as P

HEAD_CHANNELS = 64
BLOCK = 64


MESH = pl.DeviceIdType.MESH
NORM_EPSILON = 1e-06
GROUP_EPSILON = 0.00064


def rms_scale(values, gain):
    values = values.astype(jnp.float32)
    return (
        values * lax.rsqrt(jnp.mean(values * values, axis=-1, keepdims=True) + NORM_EPSILON) * gain
    )


def split_parts(x):
    high = x.astype(jnp.bfloat16)
    return high, (x - high.astype(jnp.float32)).astype(jnp.bfloat16)


def dot3(x, y, dims):
    xh, xl = split_parts(x)
    yh, yl = split_parts(y)

    def one(p, q):
        return lax.dot_general(p, q, (dims, ((), ())), preferred_element_type=jnp.float32)

    return one(xh, yh) + (one(xh, yl) + one(xl, yh))


NN = ((1,), (0,))
NT = ((1,), (1,))
TN = ((0,), (0,))


def local_kernel(
    r_ref, k_ref, v_ref, dec_ref, lr_ref, off_ref, spike_ref, out_ref, carry_ref, map_ref
):
    rows, width = r_ref.shape
    heads = width // HEAD_CHANNELS
    blocks = rows // BLOCK
    row = lax.broadcasted_iota(jnp.int32, (rows, rows), 0)
    col = lax.broadcasted_iota(jnp.int32, (rows, rows), 1)
    strict = col < row
    inclusive = col <= row
    learn_all = jax.nn.sigmoid(lr_ref[...].astype(jnp.float32))
    pre = off_ref[...] + jnp.tanh(dec_ref[...].astype(jnp.float32))
    log_all = spike_ref[...] - jax.nn.sigmoid(pre) * jnp.exp(jnp.float32(-0.5))
    ones = jnp.where(inclusive, 1.0, 0.0).astype(jnp.bfloat16)
    p0 = log_all.astype(jnp.bfloat16)
    rest = log_all - p0.astype(jnp.float32)
    p1 = rest.astype(jnp.bfloat16)
    p2 = (rest - p1.astype(jnp.float32)).astype(jnp.bfloat16)
    cum_all = sum(jnp.dot(ones, p, preferred_element_type=jnp.float32) for p in (p0, p1, p2))
    before_all = cum_all - log_all
    for h in range(heads):
        lanes = slice(h * HEAD_CHANNELS, (h + 1) * HEAD_CHANNELS)
        r = r_ref[:, lanes].astype(jnp.float32)
        k = k_ref[:, lanes].astype(jnp.float32)
        v = v_ref[:, lanes].astype(jnp.float32)
        learn = learn_all[:, lanes]
        cum = cum_all[:, lanes]
        before = before_all[:, lanes]
        a = k * lax.rsqrt(jnp.sum(k * k, axis=-1, keepdims=True) + NORM_EPSILON)
        b = a * learn
        ins = k * learn
        parts = []
        for i in range(blocks):
            span = slice(i * BLOCK, (i + 1) * BLOCK)
            base = before[i * BLOCK : i * BLOCK + 1]
            left = jnp.concatenate(
                [a[span] * jnp.exp(before[span] - base), r[span] * jnp.exp(cum[span] - base)],
                axis=0,
            )
            back = jnp.exp(jnp.minimum(base - cum, 60.0))
            right = jnp.concatenate([b * back, ins * back], axis=0)
            parts.append(dot3(left, right, NT))
        low_b = jnp.where(strict, jnp.concatenate([p[:BLOCK, :rows] for p in parts], axis=0), 0.0)
        low_k = jnp.where(strict, jnp.concatenate([p[:BLOCK, rows:] for p in parts], axis=0), 0.0)
        out_b = jnp.where(
            inclusive, jnp.concatenate([p[BLOCK:, :rows] for p in parts], axis=0), 0.0
        )
        out_k = jnp.where(
            inclusive, jnp.concatenate([p[BLOCK:, rows:] for p in parts], axis=0), 0.0
        )
        inverse = jnp.where(row == col, 1.0, 0.0)
        size = 1
        while size < BLOCK:
            corner = (row // (2 * size) == col // (2 * size)) & (row // size != col // size)
            corner = jnp.where(corner, low_b, 0.0)
            if size == 1:
                inverse = inverse - corner
            else:
                inverse = inverse - dot3(dot3(inverse, corner, NN), inverse, NN)
            size *= 2
        right_side = jnp.concatenate([a * jnp.exp(before), dot3(low_k, v, NN)], axis=1)
        solved = []
        for i in range(blocks):
            span = slice(i * BLOCK, (i + 1) * BLOCK)
            piece = right_side[span]
            if i:
                piece = piece - dot3(
                    low_b[span, : i * BLOCK], jnp.concatenate(solved, axis=0), NN
                )
            solved.append(dot3(inverse[span, span], piece, NN))
        solved = jnp.concatenate(solved, axis=0)
        removed = dot3(out_b, solved, NN)
        out_ref[:, lanes] = dot3(out_k, v, NN) - removed[:, HEAD_CHANNELS:]
        carry_ref[:, lanes] = r * jnp.exp(cum) - removed[:, :HEAD_CHANNELS]
        last = cum[rows - 1 :]
        to_end = jnp.exp(last - cum)
        taken = dot3(solved, b * to_end, TN)
        added = dot3(v, ins * to_end, TN)
        small = (HEAD_CHANNELS, HEAD_CHANNELS)
        eye = lax.broadcasted_iota(jnp.int32, small, 0) == lax.broadcasted_iota(jnp.int32, small, 1)
        through = jnp.where(eye, jnp.exp(last), 0.0) - taken[:HEAD_CHANNELS]
        fresh = added - taken[HEAD_CHANNELS:]
        map_ref[lanes, :] = jnp.concatenate([through, fresh], axis=1).astype(jnp.bfloat16)


def join_kernel(
    count, out_ref, carry_ref, map_ref, gain_ref, gate_ref, weight_ref, mix_ref, held, state,
    send_sem, recv_sem
):
    me = lax.axis_index("ep")
    rows, width = out_ref.shape
    heads = width // HEAD_CHANNELS
    barrier = pltpu.get_barrier_semaphore()
    for step in range(1, count):
        pl.semaphore_signal(
            barrier, inc=1, device_id={"ep": lax.rem(me + step, count)}, device_id_type=MESH
        )
    pl.semaphore_wait(barrier, count - 1)

    def copy(slot, step):
        return pltpu.make_async_remote_copy(
            src_ref=map_ref,
            dst_ref=held.at[slot],
            send_sem=send_sem.at[step],
            recv_sem=recv_sem.at[slot],
            device_id={"ep": lax.rem(me + step, count)},
            device_id_type=MESH,
        )

    for step in range(1, count):

        @pl.when(me + step < count)
        def _():
            copy(me, step).start()

    state[...] = jnp.zeros_like(state)

    def one(turn, _):
        copy(turn, 1).wait_recv()
        for h in range(heads):
            lanes = slice(h * HEAD_CHANNELS, (h + 1) * HEAD_CHANNELS)
            block = held[turn, lanes, :]
            high, low = split_parts(state[lanes, :])
            through = block[:, :HEAD_CHANNELS]
            state[lanes, :] = (
                jnp.dot(high, through, preferred_element_type=jnp.float32)
                + jnp.dot(low, through, preferred_element_type=jnp.float32)
                + block[:, HEAD_CHANNELS:].astype(jnp.float32)
            )
        return 0

    lax.fori_loop(0, me, one, 0)
    normed = []
    for h in range(heads):
        lanes = slice(h * HEAD_CHANNELS, (h + 1) * HEAD_CHANNELS)
        value = out_ref[:, lanes] + dot3(carry_ref[:, lanes], state[lanes, :], NT)
        centred = value - jnp.mean(value, axis=-1, keepdims=True)
        normed.append(
            centred
            * lax.rsqrt(jnp.mean(centred * centred, axis=-1, keepdims=True) + GROUP_EPSILON)
        )
    flat = normed[0] if heads == 1 else jnp.concatenate(normed, axis=1)
    heads_out = flat * gain_ref[...] * jax.nn.sigmoid(gate_ref[...].astype(jnp.float32))
    mix_ref[...] = jnp.dot(
        heads_out.astype(jnp.bfloat16), weight_ref[...], preferred_element_type=jnp.float32
    ).astype(jnp.bfloat16)
    for step in range(1, count):

        @pl.when(me + step < count)
        def _():
            copy(me, step).wait_send()


def attention_mixer(
    receptance,
    head_key_input,
    head_value_input,
    decay_input_part,
    learning_rate_input,
    output_gate_input,
    decay_channel_offset,
    spike_log_decay,
    head_norm_gain,
    head_output_weight,
    projection_norm_gain,
):
    rows, width = receptance.shape
    count = lax.axis_size("ep")
    full = pl.BlockSpec(memory_space=pltpu.VMEM)
    out, carry, maps = pl.pallas_call(
        local_kernel,
        out_shape=(
            jax.ShapeDtypeStruct((rows, width), jnp.float32),
            jax.ShapeDtypeStruct((rows, width), jnp.float32),
            jax.ShapeDtypeStruct((width, 2 * HEAD_CHANNELS), jnp.bfloat16),
        ),
        in_specs=[full] * 7,
        out_specs=(full, full, full),
        cost_estimate=pl.CostEstimate(
            flops=rows * rows * width * 200, bytes_accessed=rows * width * 22, transcendentals=0
        ),
    )(
        receptance,
        head_key_input,
        head_value_input,
        decay_input_part,
        learning_rate_input,
        decay_channel_offset[None, :],
        spike_log_decay,
    )
    model_width = head_output_weight.shape[1]
    mix = pl.pallas_call(
        functools.partial(join_kernel, count),
        out_shape=jax.ShapeDtypeStruct((rows, model_width), jnp.bfloat16),
        in_specs=[full] * 6,
        out_specs=full,
        scratch_shapes=[
            pltpu.VMEM((count, width, 2 * HEAD_CHANNELS), jnp.bfloat16),
            pltpu.VMEM((width, HEAD_CHANNELS), jnp.float32),
            pltpu.SemaphoreType.DMA((count,)),
            pltpu.SemaphoreType.DMA((count,)),
        ],
        compiler_params=pltpu.CompilerParams(collective_id=0, has_side_effects=True),
        cost_estimate=pl.CostEstimate(
            flops=rows * width * model_width * 20,
            bytes_accessed=width * model_width * 2,
            transcendentals=0,
        ),
    )(out, carry, maps, head_norm_gain[None, :], output_gate_input, head_output_weight)
    mix_sum = lax.psum_scatter(mix, "tp", scatter_dimension=0, tiled=True).astype(jnp.float32)
    return rms_scale(mix_sum, projection_norm_gain).astype(jnp.bfloat16)


def expert_kernel(
    count, pairs, arrived, gate_ref, up_ref, down_ref, result_ref, crossing, halves, paired,
    final, back, half_send, half_recv, pair_send, pair_recv, back_send, back_recv
):
    me = lax.axis_index("ep")
    place = lax.axis_index("tp")
    group = place // 2
    half = place % 2
    capacity = arrived.shape[0] // count
    columns = final.shape[2]
    partner = 2 * group + 1 - half

    def rows_of(index):
        return pl.ds(pl.multiple_of(index * capacity, capacity), capacity)

    def peer(step):
        return lax.rem(me + step, count)

    barrier = pltpu.get_barrier_semaphore()
    for step in range(1, count):
        pl.semaphore_signal(barrier, inc=1, device_id={"ep": peer(step)}, device_id_type=MESH)
    pl.semaphore_signal(barrier, inc=1, device_id={"tp": partner}, device_id_type=MESH)
    for step in range(1, pairs):
        there = 2 * lax.rem(group + step, pairs) + half
        pl.semaphore_signal(barrier, inc=1, device_id={"tp": there}, device_id_type=MESH)
    pl.semaphore_wait(barrier, count + pairs - 1)

    def cross(index):
        return pltpu.make_async_remote_copy(
            src_ref=crossing.at[index],
            dst_ref=halves.at[index],
            send_sem=half_send.at[index],
            recv_sem=half_recv.at[index],
            device_id={"tp": partner},
            device_id_type=MESH,
        )

    def pair(step):
        return pltpu.make_async_remote_copy(
            src_ref=paired.at[step],
            dst_ref=final.at[step],
            send_sem=pair_send.at[step],
            recv_sem=pair_recv.at[step],
            device_id={"tp": 2 * lax.rem(group + step, pairs) + half},
            device_id_type=MESH,
        )

    def home(turn, step):
        return pltpu.make_async_remote_copy(
            src_ref=final.at[turn, rows_of(peer(step))],
            dst_ref=back.at[turn, rows_of(me)],
            send_sem=back_send.at[turn, step],
            recv_sem=back_recv.at[turn, step],
            device_id={"ep": peer(step)},
            device_id_type=MESH,
        )

    rows = arrived[...]
    gate = jnp.dot(rows, gate_ref[0], preferred_element_type=jnp.float32)
    upward = jnp.dot(rows, up_ref[0], preferred_element_type=jnp.float32)
    hidden = (jax.nn.silu(gate) * upward).astype(jnp.bfloat16)

    def part(index):
        span = pl.ds(pl.multiple_of(index * columns, columns), columns)
        return jnp.dot(hidden, down_ref[0, :, span], preferred_element_type=jnp.float32).astype(
            jnp.bfloat16
        )

    order = list(range(1, pairs)) + [0]
    for step in order:
        crossing[step] = part(2 * lax.rem(group + step, pairs) + 1 - half)
        cross(step).start()
    own = {step: part(2 * lax.rem(group + step, pairs) + half) for step in order}
    for step in order:
        cross(step).wait_recv()
        total = (
            own[step].astype(jnp.float32) + halves[step].astype(jnp.float32)
        ).astype(jnp.bfloat16)
        if step:
            paired[step] = total
            pair(step).start()
        else:
            final[0] = total
    for turn in range(pairs):
        if turn:
            pair(turn).wait_recv()
        for step in range(1, count):
            home(turn, step).start()
        back[turn, rows_of(me), :] = final[turn, rows_of(me), :]
    for turn in range(pairs):
        for step in range(1, count):
            home(turn, step).wait_recv()
        result_ref[lax.rem(group + pairs - turn, pairs)] = back[turn]
    for step in order:
        cross(step).wait_send()
        if step:
            pair(step).wait_send()
    for turn in range(pairs):
        for step in range(1, count):
            home(turn, step).wait_send()


def routed_by_kernel(arrived, gate_weight, up_weight, down_weight, count, pairs):
    rows, model_width = arrived.shape
    columns = model_width // (2 * pairs)
    full = pl.BlockSpec(memory_space=pltpu.VMEM)
    dma = pltpu.SemaphoreType.DMA
    block = pltpu.VMEM((pairs, rows, columns), jnp.bfloat16)
    return pl.pallas_call(
        functools.partial(expert_kernel, count, pairs),
        out_shape=jax.ShapeDtypeStruct((pairs, rows, columns), jnp.bfloat16),
        in_specs=[full] * 4,
        out_specs=full,
        scratch_shapes=[block] * 5
        + [dma((pairs,))] * 4
        + [dma((pairs, count))] * 2,
        compiler_params=pltpu.CompilerParams(collective_id=1, has_side_effects=True),
        cost_estimate=pl.CostEstimate(
            flops=10 * rows * model_width * gate_weight.shape[2] * 6,
            bytes_accessed=model_width * gate_weight.shape[2] * 6,
            transcendentals=0,
        ),
    )(arrived, gate_weight, up_weight, down_weight)


def routed_by_exchange(flat_rows, gate_weight, up_weight, down_weight, count, pairs):
    rows, model_width = flat_rows.shape
    columns = model_width // (2 * pairs)
    gate = jnp.dot(flat_rows, gate_weight[0], preferred_element_type=jnp.float32)
    upward = jnp.dot(flat_rows, up_weight[0], preferred_element_type=jnp.float32)
    hidden = (jax.nn.silu(gate) * upward).astype(jnp.bfloat16)
    partial_value = jnp.dot(hidden, down_weight[0], preferred_element_type=jnp.float32).astype(
        jnp.bfloat16
    )
    pieces = lax.all_to_all(partial_value[None], "tp", split_axis=2, concat_axis=0, tiled=True)
    paired = pieces.reshape(pairs, 2, rows, columns).astype(jnp.float32)
    expert_value = (
        (paired[:, 0] + paired[:, 1])
        .astype(jnp.bfloat16)
        .reshape(pairs, count, rows // count, columns)
    )
    returned = lax.all_to_all(expert_value, "ep", split_axis=1, concat_axis=1, tiled=True)
    return returned.reshape(-1, columns)


def expert_half(
    expert_input_rows,
    expert_norm_gain,
    selected_expert_index,
    selected_expert_weight,
    routed_gate_weight,
    routed_up_weight,
    routed_down_weight,
    common_gate_weight,
    common_up_weight,
    common_down_weight,
):
    tok_rows, model_width = expert_input_rows.shape
    chosen_count = selected_expert_index.shape[1]
    ep_count = lax.axis_size("ep")
    tp_count = lax.axis_size("tp")
    group_count = tp_count // 2
    expert_total = group_count * ep_count
    capacity = 2 * tok_rows * chosen_count // expert_total
    column_count = model_width // tp_count
    tp_place = lax.axis_index("tp")
    group_index = tp_place // 2
    normed = rms_scale(expert_input_rows, expert_norm_gain).astype(jnp.bfloat16)
    assigned = selected_expert_index.reshape(-1)
    assign_count = assigned.shape[0]
    expert_ids = jnp.arange(expert_total, dtype=jnp.int32)
    onehot = (assigned[:, None] == expert_ids[None, :]).astype(jnp.int32)
    ranking = jnp.sum((jnp.cumsum(onehot, axis=0) - onehot) * onehot, axis=1)
    target = jnp.where(
        assigned % group_count == group_index, assigned // group_count * capacity + ranking, -1
    ).reshape(tok_rows, chosen_count)
    slots = jnp.arange(ep_count * capacity, dtype=jnp.int32)
    placing = jnp.any(target[:, :, None] == slots[None, None, :], axis=1).astype(jnp.bfloat16)
    outgoing = lax.dot_general(
        placing, normed, (((0,), (0,)), ((), ())), preferred_element_type=jnp.float32
    ).astype(jnp.bfloat16)
    arrived = lax.all_to_all(
        outgoing.reshape(ep_count, capacity, model_width),
        "ep",
        split_axis=0,
        concat_axis=0,
        tiled=True,
    ).reshape(-1, model_width)
    if capacity % 16 == 0 and column_count % 128 == 0:
        flat_back = routed_by_kernel(
            arrived, routed_gate_weight, routed_up_weight, routed_down_weight, ep_count, group_count
        ).reshape(-1, column_count)
    else:
        flat_back = routed_by_exchange(
            arrived, routed_gate_weight, routed_up_weight, routed_down_weight, ep_count, group_count
        )
    position = (
        assigned % group_count * (ep_count * capacity)
        + assigned // group_count * capacity
        + ranking
    )
    picked = (
        jnp.take(flat_back, position, axis=0)
        .astype(jnp.float32)
        .reshape(tok_rows, chosen_count, column_count)
    )
    routed = jnp.sum(picked * selected_expert_weight[:, :, None], axis=1)
    shared_hidden = (
        jax.nn.silu(jnp.dot(normed, common_gate_weight, preferred_element_type=jnp.float32))
        * jnp.dot(normed, common_up_weight, preferred_element_type=jnp.float32)
    ).astype(jnp.bfloat16)
    shared_sum = lax.psum_scatter(
        lax.dot_general(
            common_down_weight,
            shared_hidden,
            (((0,), (1,)), ((), ())),
            preferred_element_type=jnp.float32,
        ).astype(jnp.bfloat16),
        "tp",
        scatter_dimension=0,
        tiled=True,
    ).astype(jnp.float32)
    return (routed + shared_sum.T).astype(jnp.bfloat16)


def mm(x, y, dims=NN):
    return lax.dot_general(x, y, (dims, ((), ())), preferred_element_type=jnp.float32)


def pair_masks():
    lane = lax.broadcasted_iota(jnp.int32, (BLOCK, 2 * HEAD_CHANNELS), 1)
    first = jnp.where(lane < HEAD_CHANNELS, 1.0, 0.0)
    return first.astype(jnp.bfloat16), (1.0 - first).astype(jnp.bfloat16)


def stacked(y, masks):
    return jnp.concatenate([y * masks[0], y * masks[1]], axis=0)


def pair_dot(x, parts):
    xh, xl = split_parts(x)
    high, low = parts
    return mm(jnp.concatenate([xh, xl], axis=1), jnp.concatenate([high, high], axis=0)) + mm(
        xh, low
    )


def short_dot(x, y, masks):
    return mm(x.astype(jnp.bfloat16), stacked(y.astype(jnp.bfloat16), masks))


def pair_parts(y, masks):
    yh, yl = split_parts(y)
    return stacked(yh, masks), stacked(yl, masks)


def side_by_side(one, two):
    return tuple(jnp.concatenate([p, q], axis=1) for p, q in zip(one, two))


def head_sum(x, block_ones):
    xh, xl = split_parts(x)
    return mm(jnp.concatenate([xh, xl], axis=1), block_ones)


def head_ones():
    wide = 2 * HEAD_CHANNELS
    row = lax.broadcasted_iota(jnp.int32, (2 * wide, wide), 0)
    col = lax.broadcasted_iota(jnp.int32, (2 * wide, wide), 1)
    same = (row // HEAD_CHANNELS) % 2 == col // HEAD_CHANNELS
    return jnp.where(same, 1.0, 0.0).astype(jnp.bfloat16)


def local_math(r_ref, k_ref, v_ref, dec_ref, lr_ref, off_ref, spike_ref):
    rows, width = r_ref.shape
    wide = 2 * HEAD_CHANNELS
    pairs = width // wide
    chunks = rows // BLOCK
    masks = pair_masks()
    ones_head = head_ones()
    row = lax.broadcasted_iota(jnp.int32, (BLOCK, wide), 0)
    col = lax.broadcasted_iota(jnp.int32, (BLOCK, wide), 1) % HEAD_CHANNELS
    strict = col < row
    inclusive = col <= row
    trow = lax.broadcasted_iota(jnp.int32, (BLOCK, 4 * BLOCK), 0)
    tcol = lax.broadcasted_iota(jnp.int32, (BLOCK, 4 * BLOCK), 1)
    running = jnp.where((tcol % BLOCK <= trow) & (tcol < 3 * BLOCK), 1.0, 0.0).astype(jnp.bfloat16)
    blank = jnp.zeros((BLOCK, wide), jnp.bfloat16)
    items = [(i, p) for i in range(chunks) for p in range(pairs)]
    spans = [slice(i * BLOCK, (i + 1) * BLOCK) for i in range(chunks)]
    strips = [slice(p * wide, (p + 1) * wide) for p in range(pairs)]
    pre = off_ref[...] + jnp.tanh(dec_ref[...].astype(jnp.float32))
    log = spike_ref[...] - jax.nn.sigmoid(pre) * jnp.exp(jnp.float32(-0.5))
    p0 = log.astype(jnp.bfloat16)
    rest = log - p0.astype(jnp.float32)
    p1 = rest.astype(jnp.bfloat16)
    p2 = (rest - p1.astype(jnp.float32)).astype(jnp.bfloat16)
    empty = jnp.zeros((BLOCK, width), jnp.bfloat16)
    cums = [
        mm(running, jnp.concatenate([p0[span], p1[span], p2[span], empty], axis=0))
        for span in spans
    ]
    k_all = k_ref[...].astype(jnp.float32)
    squares = k_all * k_all
    sums = [head_sum(squares[:, strip], ones_head) for strip in strips]
    learn = jax.nn.sigmoid(lr_ref[...].astype(jnp.float32))
    scale = jnp.concatenate([lax.rsqrt(q + NORM_EPSILON) for q in sums], axis=1)
    cum_all = jnp.concatenate(cums, axis=0)
    back = learn * k_all * jnp.exp(-cum_all)
    b_all = back * scale
    a_all = k_all * scale * jnp.exp(cum_all - log)
    r_all = r_ref[...].astype(jnp.float32) * jnp.exp(cum_all)
    bh_all, bl_all = split_parts(b_all)
    ih_all, il_all = split_parts(back)
    ah_all, al_all = split_parts(a_all)
    rh_all, rl_all = split_parts(r_all)
    chunk_ends = [jnp.exp(c[BLOCK - 1 :]) for c in cums]
    grams = []
    for i, p in items:
        at = (spans[i], strips[p])
        left_high = jnp.concatenate([ah_all[at], rh_all[at]], axis=0)
        left_low = jnp.concatenate([al_all[at], rl_all[at]], axis=0)
        right_high = jnp.concatenate(
            [stacked(bh_all[at], masks), stacked(ih_all[at], masks)], axis=0
        )
        right_low = jnp.concatenate(
            [stacked(bl_all[at], masks), stacked(il_all[at], masks)], axis=0
        )
        grams.append(
            mm(
                jnp.concatenate([left_high, left_low], axis=1),
                jnp.concatenate([right_high, right_high], axis=1),
                NT,
            )
            + mm(left_high, right_low, NT)
        )
    lows = [jnp.where(strict, gram[:BLOCK, :wide], 0.0) for gram in grams]
    out_bs = [jnp.where(inclusive, gram[BLOCK:, :wide], 0.0) for gram in grams]
    vs = [v_ref[spans[i], strips[p]] for i, p in items]
    weighted = []
    for n, gram in enumerate(grams):
        kh, kl = split_parts(
            jnp.concatenate(
                [
                    jnp.where(strict, gram[:BLOCK, wide:], 0.0),
                    jnp.where(inclusive, gram[BLOCK:, wide:], 0.0),
                ],
                axis=0,
            )
        )
        values = stacked(vs[n], masks)
        weighted.append(
            mm(jnp.concatenate([kh, kl], axis=1), jnp.concatenate([values, values], axis=0))
        )
    low_vs = [w[:BLOCK] for w in weighted]
    out_vs = [w[BLOCK:] for w in weighted]
    ends = [chunk_ends[i][:, strips[p]] for i, p in items]
    ins_ends = [back[spans[i], strips[p]] * ends[n] for n, (i, p) in enumerate(items)]
    b_ends = [b_all[spans[i], strips[p]] * ends[n] for n, (i, p) in enumerate(items)]
    r_outs = [r_all[spans[i], strips[p]] for i, p in items]
    a_ins = [a_all[spans[i], strips[p]] for i, p in items]
    count = range(len(items))
    eye = jnp.where(row == col, 1.0, 0.0)
    inverses = None
    size = 1
    while size < BLOCK:
        inside = (row // (2 * size) == col // (2 * size)) & (row // size != col // size)
        corners = [jnp.where(inside, low, 0.0) for low in lows]
        if size == 1:
            inverses = [eye - corner for corner in corners]
        else:
            exact = 2 * size >= BLOCK
            firsts = [
                pair_dot(inverses[n], pair_parts(corners[n], masks))
                if exact
                else short_dot(inverses[n], corners[n], masks)
                for n in count
            ]
            changes = [
                pair_dot(firsts[n], pair_parts(inverses[n], masks))
                if exact
                else short_dot(firsts[n], inverses[n], masks)
                for n in count
            ]
            inverses = [inverses[n] - changes[n] for n in count]
        size *= 2
    solved = [
        side_by_side(pair_parts(a_ins[n], masks), pair_parts(low_vs[n], masks)) for n in count
    ]
    solved = [pair_dot(inverses[n], solved[n]) for n in count]
    brow = lax.broadcasted_iota(jnp.int32, (wide, 2 * wide), 0)
    bcol = lax.broadcasted_iota(jnp.int32, (wide, 2 * wide), 1)
    same_head = brow // HEAD_CHANNELS == (bcol % wide) // HEAD_CHANNELS
    diagonal = brow == bcol
    maps = []
    for n in count:
        left = jnp.concatenate([-b_ends[n], ins_ends[n]], axis=0)
        lh, ll = split_parts(left)
        uh, ul = split_parts(solved[n])
        high = jnp.concatenate([uh, jnp.concatenate([blank, vs[n]], axis=1)], axis=0)
        low = jnp.concatenate([ul, jnp.concatenate([blank, blank], axis=1)], axis=0)
        made = mm(
            jnp.concatenate([lh, ll], axis=0), jnp.concatenate([high, high], axis=0), TN
        ) + mm(lh, low, TN)
        end = jnp.concatenate([ends[n], ends[n]], axis=1)
        maps.append(jnp.where(same_head, made + jnp.where(diagonal, end, 0.0), 0.0))
    def after(second, first):
        joined = pair_dot(second[:, :wide], split_parts(first))
        return jnp.concatenate([joined[:, :wide], joined[:, wide:] + second[:, wide:]], axis=1)

    by_pair = [maps[p::pairs] for p in range(pairs)]
    stage = [list(row) for row in by_pair]
    tree = [stage]
    while len(stage[0]) > 1:
        stage = [
            [
                after(row[i + 1], row[i]) if i + 1 < len(row) else row[i]
                for i in range(0, len(row), 2)
            ]
            for row in stage
        ]
        tree.append(stage)
    whole = [row[0] for row in stage]

    def reaching(p, i):
        result, done = None, 0
        for depth in range(len(tree) - 1, -1, -1):
            if i - done >= 1 << depth:
                piece = tree[depth][p][done >> depth]
                result = piece if result is None else after(piece, result)
                done += 1 << depth
        return result

    compact = [m[:HEAD_CHANNELS] + m[HEAD_CHANNELS:] for m in whole]

    def finish():
        results = {}
        for n in count:
            uh, ul = split_parts(solved[n])
            parts = [
                jnp.concatenate([stacked(u[:, :wide], masks), stacked(u[:, wide:], masks)], axis=1)
                for u in (uh, ul)
            ]
            removed = pair_dot(out_bs[n], parts)
            carry = r_outs[n] - removed[:, :wide]
            value = out_vs[n] - removed[:, wide:]
            entry = reaching(items[n][1], items[n][0])
            if entry is not None:
                moved = pair_dot(carry, split_parts(entry))
                carry = moved[:, :wide]
                value = value + moved[:, wide:]
            results[items[n]] = (carry, value)
        return results

    return compact, finish


def flipped_rows(index, bits, count):
    result, unit = 0, 1
    while unit < count:
        digit = (index // unit) % 2
        result = result + unit * ((digit + bits // unit) % 2)
        unit *= 2
    return result


def mega_kernel(ep_count, *refs):
    inputs = refs[:21]
    attn_out, expert_out = refs[21:23]
    copies = refs[23:44]
    (
        r_ref, k_ref, v_ref, dec_ref, lr_ref, gate_ref, off_ref, spike_ref, hgain_ref, wout_ref,
        pgain_ref, x_ref, egain_ref, idx_ref, wsel_ref, wg_ref, wu_ref, wd_ref, cg_ref, cu_ref,
        cd_ref,
    ) = copies
    (
        normed, outgoing, arrived, carry_ref, value_ref, own_map, held, base_state, state,
        next_state, shared, shared_half, shared_sum, shared_last, crossing,
        halves, own_ref, final, back, heads_ref, scale_ref, mix, mix_half, mix_sum, mix_last,
        load_sem, disp_send, disp_recv, fwd_send, fwd_recv, map_send, map_recv, base_send,
        base_recv, sh_send, sh_recv, cross_send, cross_recv, home_send, home_recv, mx_send,
        mx_recv, tail_send, tail_recv,
    ) = refs[44:]
    me = lax.axis_index("ep")
    place = lax.axis_index("tp")
    group = place // 2
    half = place % 2
    other = 1 - half
    partner = 2 * group + other
    across = 2 * (1 - group) + half
    level = me // 4
    member = me % 4
    levels = ep_count // 4
    tok_rows, model_width = x_ref.shape
    slots = outgoing.shape[0]
    capacity = slots // ep_count
    fold = model_width // 2
    columns = model_width // 4
    rows, width = r_ref.shape
    wide = 2 * HEAD_CHANNELS
    pairs = width // wide
    block_rows = rows // 4
    quarter = ep_count // 4
    outer = (level + member // 2 + 1) % 2
    first_start = quarter * (2 + outer)
    second_start = quarter * (3 - outer)
    first_batch = [first_start + n for n in range(quarter)]
    second_batch = [second_start + n for n in range(quarter)]
    near_batch = list(range(2 * quarter))

    barrier = pltpu.get_barrier_semaphore()

    def peer(bits):
        return flipped_rows(me, bits, ep_count)

    def tp_of(turn):
        return 2 * lax.rem(group + turn, 2) + half

    for bits in range(ep_count):
        for turn in range(2):
            if bits or turn:
                pl.semaphore_signal(
                    barrier,
                    inc=1,
                    device_id={"ep": peer(bits), "tp": tp_of(turn)},
                    device_id_type=MESH,
                )
    pl.semaphore_signal(barrier, inc=1, device_id={"tp": partner}, device_id_type=MESH)

    loads = [
        pltpu.make_async_copy(source, target, load_sem.at[n])
        for n, (source, target) in enumerate(zip(inputs, copies))
    ]
    for n in (13, 14, 11, 12, 0, 1, 2, 3, 4, 6, 7, 18, 19, 20, 15, 16, 17, 5, 8, 9, 10):
        loads[n].start()

    def rows_of(bits):
        if isinstance(bits, int):
            return slice(bits * capacity, (bits + 1) * capacity)
        return pl.ds(pl.multiple_of(bits * capacity, capacity), capacity)

    def remote(source, target, send, recv, where):
        return pltpu.make_async_remote_copy(
            src_ref=source,
            dst_ref=target,
            send_sem=send,
            recv_sem=recv,
            device_id=where,
            device_id_type=MESH,
        )

    def dispatch(bits):
        return remote(
            outgoing.at[rows_of(bits)],
            arrived.at[half, rows_of(bits)],
            disp_send.at[bits],
            disp_recv.at[bits],
            {"ep": peer(bits)},
        )

    def forward(bits):
        return remote(
            arrived.at[half, rows_of(bits)],
            arrived.at[half, rows_of(bits)],
            fwd_send.at[bits],
            fwd_recv.at[bits],
            {"tp": partner},
        )

    for n in (13, 14):
        loads[n].wait()
    chosen_count = idx_ref.shape[0]
    experts = 2 * ep_count
    expert_row = lax.broadcasted_iota(jnp.int32, (experts, tok_rows), 0)
    named = [expert_row == idx_ref[k : k + 1, :] for k in range(chosen_count)]
    chosen = functools.reduce(jnp.logical_or, named)
    weight_of = functools.reduce(
        jnp.add, [jnp.where(n, wsel_ref[k : k + 1, :], 0.0) for k, n in enumerate(named)]
    )
    early = lax.broadcasted_iota(jnp.int32, (tok_rows, tok_rows), 0) < lax.broadcasted_iota(
        jnp.int32, (tok_rows, tok_rows), 1
    )
    rank = mm(
        jnp.where(chosen, 1.0, 0.0).astype(jnp.bfloat16),
        jnp.where(early, 1.0, 0.0).astype(jnp.bfloat16),
    )
    rank = jnp.where(chosen, rank, -1.0).astype(jnp.bfloat16)
    slot = lax.broadcasted_iota(jnp.int32, (slots, experts), 0)
    which = lax.broadcasted_iota(jnp.int32, (slots, experts), 1)
    there = flipped_rows(me, slot // capacity, ep_count)
    mine = jnp.where(which == 2 * there + group, 1.0, 0.0).astype(jnp.bfloat16)
    slot_rank = (
        lax.broadcasted_iota(jnp.int32, (slots, tok_rows), 0) % capacity
    ).astype(jnp.float32)
    placing = jnp.where(mm(mine, rank) == slot_rank, 1.0, 0.0).astype(jnp.bfloat16)
    for n in (11, 12):
        loads[n].wait()
    normed[...] = rms_scale(x_ref[...], egain_ref[...]).astype(jnp.bfloat16)
    fold_span = pl.ds(pl.multiple_of(half * fold, fold), fold)
    other_span = pl.ds(pl.multiple_of(other * fold, fold), fold)
    outgoing[...] = mm(placing, normed[:, fold_span]).astype(jnp.bfloat16)
    pl.semaphore_wait(barrier, 2 * ep_count)
    order = list(range(2 * quarter, ep_count)) + near_batch[1:]
    for bits in order[: 2 * quarter]:
        dispatch(bits).start()

    @pl.when(outer == 0)
    def _():
        for bits in order[2 * quarter :]:
            dispatch(bits).start()

    arrived[half, rows_of(0), :] = outgoing[rows_of(0), :]
    arrived[other, rows_of(0), :] = mm(placing[:capacity], normed[:, other_span]).astype(
        jnp.bfloat16
    )

    for n in (0, 1, 2, 3, 4, 6, 7):
        loads[n].wait()
    compact, finish = local_math(r_ref, k_ref, v_ref, dec_ref, lr_ref, off_ref, spike_ref)
    for p in range(pairs):
        own_map[p] = compact[p].astype(jnp.bfloat16)
    masks = pair_masks()

    def give(there):
        return remote(
            own_map,
            held.at[member],
            map_send.at[there],
            map_recv.at[member],
            {"ep": 4 * level + there},
        )

    def taken(source):
        return remote(
            own_map, held.at[source], map_send.at[0], map_recv.at[source], {"ep": peer(1)}
        )

    def gives(there):
        above_me = member < there
        return above_me | (member == 3) if there == 2 else above_me

    for there in (3, 2, 1):

        @pl.when(gives(there))
        def _():
            give(there).start()

    for (i, p), (carry, value) in finish().items():
        span = slice(i * BLOCK, (i + 1) * BLOCK)
        lanes = slice(p * wide, (p + 1) * wide)
        carry_ref[span, lanes] = carry
        value_ref[span, lanes] = value

    for n in (18, 19, 20):
        loads[n].wait()
    rows_in = normed[...]
    hidden = (jax.nn.silu(mm(rows_in, cg_ref[...])) * mm(rows_in, cu_ref[...])).astype(
        jnp.bfloat16
    )
    for j in range(4):
        shared[j] = mm(hidden, cd_ref[:, j * columns : (j + 1) * columns]).astype(jnp.bfloat16)

    def shared_cross(turn):
        there = 2 * lax.rem(group + turn, 2) + other
        return remote(
            shared.at[there],
            shared_half.at[turn],
            sh_send.at[turn],
            sh_recv.at[turn],
            {"tp": partner},
        )

    for turn in (1, 0):
        shared_cross(turn).start()

    def take_in(batch):
        for bits in batch:
            if not isinstance(bits, int) or bits:
                dispatch(bits).wait_recv()
                forward(bits).start()

    for turn in (1, 0):
        shared_cross(turn).wait_recv()
        shared_sum[turn] = shared[tp_of(turn)].astype(jnp.float32) + shared_half[turn].astype(
            jnp.float32
        )
    shared_last[0] = shared_sum[1].astype(jnp.bfloat16)
    shared_tail = remote(
        shared_last.at[0], shared_last.at[1], tail_send.at[0], tail_recv.at[0], {"tp": across}
    )
    shared_tail.start()
    for n in (5, 8):
        loads[n].wait()
    scale_ref[...] = hgain_ref[...] * jax.nn.sigmoid(gate_ref[...].astype(jnp.float32))
    take_in(first_batch)

    @pl.when(outer == 1)
    def _():
        for bits in order[2 * quarter :]:
            dispatch(bits).start()

    def wait_far(batch):
        for bits in batch:
            if not isinstance(bits, int) or bits:
                forward(bits).wait_recv()

    def cross(batch_index, turn, span):
        return remote(
            crossing.at[turn, span],
            halves.at[turn, span],
            cross_send.at[batch_index, turn],
            cross_recv.at[batch_index, turn],
            {"tp": partner},
        )

    def home(turn, bits):
        return remote(
            final.at[turn, rows_of(bits)],
            back.at[group, rows_of(bits)],
            home_send.at[turn, bits],
            home_recv.at[turn, bits],
            {"ep": peer(bits), "tp": tp_of(turn)},
        )

    def span_of(batch):
        if isinstance(batch[0], int):
            return slice(0, len(batch) * capacity)
        size = quarter * capacity
        return pl.ds(pl.multiple_of(batch[0] * capacity, size), size)

    def feed(batch_index, batch):
        span = span_of(batch)
        near, away = arrived[0, span, :], arrived[1, span, :]
        gate = mm(near, wg_ref[:fold, :]) + mm(away, wg_ref[fold:, :])
        upper = mm(near, wu_ref[:fold, :]) + mm(away, wu_ref[fold:, :])
        routed_hidden = (jax.nn.silu(gate) * upper).astype(jnp.bfloat16)

        def part(index):
            lanes = pl.ds(pl.multiple_of(index * columns, columns), columns)
            return mm(routed_hidden, wd_ref[:, lanes])

        for turn in (1, 0):
            crossing[turn, span, :] = part(2 * lax.rem(group + turn, 2) + other).astype(
                jnp.bfloat16
            )
            cross(batch_index, turn, span).start()
        for turn in (1, 0):
            own_ref[turn, span, :] = part(2 * lax.rem(group + turn, 2) + half)

    def send_home(batch_index, batch):
        span = span_of(batch)
        for turn in (1, 0):
            cross(batch_index, turn, span).wait_recv()
            final[turn, span, :] = (
                own_ref[turn, span, :] + halves[turn, span, :].astype(jnp.float32)
            ).astype(jnp.bfloat16)
            for bits in batch:
                if not isinstance(bits, int) or bits or turn:
                    home(turn, bits).start()
                else:
                    back[group, rows_of(0), :] = final[0, rows_of(0), :]

    for n in (15, 16, 17):
        loads[n].wait()
    wait_far(first_batch)
    feed(0, first_batch)
    def moved_by(block, p, current):
        through = block[p, :, :wide]
        high, low = pair_parts(current, masks)
        return mm(
            jnp.concatenate([through, through], axis=1), jnp.concatenate([high, low], axis=0)
        ) + block[p, :, wide:].astype(jnp.float32)

    def above(turn):
        return remote(
            next_state,
            base_state,
            base_send.at[turn],
            base_recv.at[0],
            {"ep": lax.rem(4 * (level + 1) + 2 * turn + member % 2, ep_count)},
        )

    hands_on = (member >= 2) & (level + 1 < levels)

    def settle():
        for p in range(pairs):
            state[p] = base_state[p].astype(jnp.float32)
        for source in range(3):

            @pl.when(source < member)
            def _():
                taken(source).wait_recv()
                for p in range(pairs):
                    state[p] = moved_by(held.at[source], p, state[p])

        @pl.when(member == 2)
        def _():
            taken(3).wait_recv()

        @pl.when(hands_on)
        def _():
            for p in range(pairs):
                once = moved_by(own_map, p, state[p])
                twice = moved_by(held.at[3], p, once)
                next_state[p] = jnp.where(member == 2, twice, once).astype(jnp.bfloat16)
            for turn in range(2):
                above(turn).start()

    @pl.when(level == 0)
    def _():
        base_state[...] = jnp.zeros_like(base_state)
        settle()

    for n in (9, 10):
        loads[n].wait()

    def mix_cross(turn):
        there = 2 * lax.rem(group + turn, 2) + other
        return remote(
            mix.at[there],
            mix_half.at[turn],
            mx_send.at[turn],
            mx_recv.at[turn],
            {"tp": partner},
        )

    def project(turn):
        there = lax.rem(group + turn, 2)
        rows_there = pl.ds(pl.multiple_of(there * 2 * block_rows, 2 * block_rows), 2 * block_rows)
        rows_made = heads_ref[rows_there, :]
        for j in range(4):
            span = slice(j * columns, (j + 1) * columns)
            made = mm(rows_made, wout_ref[:, span]).astype(jnp.bfloat16)
            for b in range(2):
                mix[2 * there + b, :, span] = made[b * block_rows : (b + 1) * block_rows]

    def attend():
        ones_head = head_ones()
        for p in range(pairs):
            lanes = slice(p * wide, (p + 1) * wide)
            value = value_ref[:, lanes] + pair_dot(
                carry_ref[:, lanes], pair_parts(state[p], masks)
            )
            centred = value - head_sum(value, ones_head) * (1.0 / HEAD_CHANNELS)
            spread = head_sum(centred * centred, ones_head) * (1.0 / HEAD_CHANNELS)
            heads_ref[:, lanes] = (
                centred
                * lax.rsqrt(spread + GROUP_EPSILON)
                * scale_ref[:, lanes]
            ).astype(jnp.bfloat16)
        for turn in (1, 0):
            project(turn)
            mix_cross(turn).start()

    mix_tail = remote(
        mix_last.at[0], mix_last.at[1], tail_send.at[1], tail_recv.at[1], {"tp": across}
    )

    def pass_mix():
        mix_cross(1).wait_recv()
        mix_last[0] = (
            mix[across].astype(jnp.float32) + mix_half[1].astype(jnp.float32)
        ).astype(jnp.bfloat16)
        mix_tail.start()

    @pl.when(level == 0)
    def _():
        attend()

    send_home(0, first_batch)
    take_in(near_batch)
    @pl.when(level == 0)
    def _():
        pass_mix()

    wait_far(near_batch)
    feed(1, near_batch)
    take_in(second_batch)
    send_home(1, near_batch)

    last_first = (level > 0) & (outer == 1)

    def feed_last():
        wait_far(second_batch)
        feed(2, second_batch)
        send_home(2, second_batch)

    @pl.when(last_first)
    def _():
        feed_last()

    @pl.when(level > 0)
    def _():
        above(0).wait_recv()
        settle()

    @pl.when(level > 0)
    def _():
        attend()

    @pl.when(level > 0)
    def _():
        pass_mix()

    @pl.when(jnp.logical_not(last_first))
    def _():
        feed_last()

    mix_cross(0).wait_recv()
    mix_sum[...] = mix[place].astype(jnp.float32) + mix_half[0].astype(jnp.float32)

    all_slots = 2 * slots
    slot = lax.broadcasted_iota(jnp.int32, (experts, all_slots), 1)
    which = lax.broadcasted_iota(jnp.int32, (experts, all_slots), 0)
    there = flipped_rows(me, (slot % slots) // capacity, ep_count)
    holder = jnp.where(which == 2 * there + slot // slots, 1.0, 0.0).astype(jnp.bfloat16)
    slot_rank = (
        lax.broadcasted_iota(jnp.int32, (tok_rows, all_slots), 1) % capacity
    ).astype(jnp.float32)
    hit = mm(rank, holder, TN) == slot_rank
    weight_high, weight_low = split_parts(weight_of)
    picks = [
        jnp.where(hit, mm(w, holder, TN), 0.0).astype(jnp.bfloat16)
        for w in (weight_high, weight_low)
    ]
    shared_tail.wait_recv()
    base = shared_sum[0] + shared_last[1].astype(jnp.float32)
    for turn in range(2):
        for bits in first_batch:
            home(turn, bits).wait_recv()
    for turn in range(2):
        for bits in near_batch:
            if bits or turn:
                home(turn, bits).wait_recv()
    for turn in range(2):
        for bits in second_batch:
            home(turn, bits).wait_recv()
    returned = back[...].reshape(all_slots, columns)
    routed = mm(
        jnp.concatenate(picks, axis=1), jnp.concatenate([returned, returned], axis=0)
    )
    expert_out[...] = (routed + base).astype(jnp.bfloat16)

    mix_tail.wait_recv()
    total = mix_sum[...] + mix_last[1].astype(jnp.float32)
    attn_out[...] = rms_scale(total, pgain_ref[...]).astype(jnp.bfloat16)

    for bits in order:
        dispatch(bits).wait_send()
        forward(bits).wait_send()
    for there in (3, 2, 1):

        @pl.when(gives(there))
        def _():
            give(there).wait_send()

    @pl.when(hands_on)
    def _():
        for turn in range(2):
            above(turn).wait_send()

    for turn in range(2):
        shared_cross(turn).wait_send()
        mix_cross(turn).wait_send()
        for n, batch in enumerate((first_batch, near_batch, second_batch)):
            cross(n, turn, span_of(batch)).wait_send()
        for bits in range(ep_count):
            if bits or turn:
                home(turn, bits).wait_send()
    shared_tail.wait_send()
    mix_tail.wait_send()


def mega(
    receptance, head_key_input, head_value_input, decay_input_part, learning_rate_input,
    output_gate_input, decay_channel_offset, spike_log_decay, head_norm_gain, head_output_weight,
    projection_norm_gain, expert_input_rows, expert_norm_gain, selected_expert_index,
    selected_expert_weight, routed_gate_weight, routed_up_weight, routed_down_weight,
    common_gate_weight, common_up_weight, common_down_weight,
):
    ep_count = lax.axis_size("ep")
    rows, width = receptance.shape
    tok_rows, model_width = expert_input_rows.shape
    chosen = selected_expert_index.shape[1]
    capacity = tok_rows * chosen // ep_count
    slots = ep_count * capacity
    columns = model_width // 4
    wide = 2 * HEAD_CHANNELS
    pairs = width // wide
    operands = (
        receptance, head_key_input, head_value_input, decay_input_part, learning_rate_input,
        output_gate_input, decay_channel_offset[None, :], spike_log_decay, head_norm_gain[None, :],
        head_output_weight, projection_norm_gain[None, :], expert_input_rows,
        expert_norm_gain[None, :], selected_expert_index.T, selected_expert_weight.T,
        routed_gate_weight[0], routed_up_weight[0], routed_down_weight[0], common_gate_weight,
        common_up_weight, common_down_weight,
    )
    bf16, f32 = jnp.bfloat16, jnp.float32
    dma = pltpu.SemaphoreType.DMA
    scratch = [pltpu.VMEM(o.shape, o.dtype) for o in operands] + [
        pltpu.VMEM((tok_rows, model_width), bf16),
        pltpu.VMEM((slots, model_width // 2), bf16),
        pltpu.VMEM((2, slots, model_width // 2), bf16),
        pltpu.VMEM((rows, width), f32),
        pltpu.VMEM((rows, width), f32),
        pltpu.VMEM((pairs, HEAD_CHANNELS, 2 * wide), bf16),
        pltpu.VMEM((4, pairs, HEAD_CHANNELS, 2 * wide), bf16),
        pltpu.VMEM((pairs, HEAD_CHANNELS, wide), bf16),
        pltpu.VMEM((pairs, HEAD_CHANNELS, wide), f32),
        pltpu.VMEM((pairs, HEAD_CHANNELS, wide), bf16),
        pltpu.VMEM((4, tok_rows, columns), bf16),
        pltpu.VMEM((2, tok_rows, columns), bf16),
        pltpu.VMEM((2, tok_rows, columns), f32),
        pltpu.VMEM((2, tok_rows, columns), bf16),
        pltpu.VMEM((2, slots, columns), bf16),
        pltpu.VMEM((2, slots, columns), bf16),
        pltpu.VMEM((2, slots, columns), f32),
        pltpu.VMEM((2, slots, columns), bf16),
        pltpu.VMEM((2, slots, columns), bf16),
        pltpu.VMEM((rows, width), bf16),
        pltpu.VMEM((rows, width), f32),
        pltpu.VMEM((4, rows // 4, model_width), bf16),
        pltpu.VMEM((2, rows // 4, model_width), bf16),
        pltpu.VMEM((rows // 4, model_width), f32),
        pltpu.VMEM((2, rows // 4, model_width), bf16),
        dma((len(operands),)),
    ]
    scratch += [dma((ep_count,))] * 4
    scratch += [dma((4,))] * 2
    scratch += [dma((2,))] * 4
    scratch += [dma((3, 2))] * 2
    scratch += [dma((2, ep_count))] * 2
    scratch += [dma((2,))] * 4
    full = pl.BlockSpec(memory_space=pltpu.VMEM)
    return pl.pallas_call(
        functools.partial(mega_kernel, ep_count),
        out_shape=(
            pltpu.VMEM((rows // 4, model_width), bf16),
            pltpu.VMEM((tok_rows, columns), bf16),
        ),
        in_specs=[pl.BlockSpec(memory_space=pl.ANY)] * len(operands),
        out_specs=(full, full),
        scratch_shapes=scratch,
        compiler_params=pltpu.CompilerParams(collective_id=0, has_side_effects=True),
    )(*operands)


def fits_mega(receptance, expert_input_rows, selected_expert_index):
    ep_count = lax.axis_size("ep")
    rows, width = receptance.shape
    tok_rows, model_width = expert_input_rows.shape
    assigned = tok_rows * selected_expert_index.shape[1]
    return (
        lax.axis_size("tp") == 4
        and ep_count >= 4
        and ep_count & (ep_count - 1) == 0
        and width % (2 * HEAD_CHANNELS) == 0
        and rows % (4 * BLOCK) == 0
        and assigned % (16 * ep_count) == 0
        and tok_rows % 128 == 0
        and tok_rows <= 256
        and model_width % 512 == 0
    )


def body(
    receptance,
    head_key_input,
    head_value_input,
    decay_input_part,
    learning_rate_input,
    output_gate_input,
    decay_channel_offset,
    spike_log_decay,
    head_norm_gain,
    head_output_weight,
    projection_norm_gain,
    expert_input_rows,
    expert_norm_gain,
    selected_expert_index,
    selected_expert_weight,
    routed_gate_weight,
    routed_up_weight,
    routed_down_weight,
    common_gate_weight,
    common_up_weight,
    common_down_weight,
):
    if fits_mega(receptance, expert_input_rows, selected_expert_index):
        return mega(
            receptance, head_key_input, head_value_input, decay_input_part, learning_rate_input,
            output_gate_input, decay_channel_offset, spike_log_decay, head_norm_gain,
            head_output_weight, projection_norm_gain, expert_input_rows, expert_norm_gain,
            selected_expert_index, selected_expert_weight, routed_gate_weight, routed_up_weight,
            routed_down_weight, common_gate_weight, common_up_weight, common_down_weight,
        )
    attention_output = attention_mixer(
        receptance,
        head_key_input,
        head_value_input,
        decay_input_part,
        learning_rate_input,
        output_gate_input,
        decay_channel_offset,
        spike_log_decay,
        head_norm_gain,
        head_output_weight,
        projection_norm_gain,
    )
    expert_output = expert_half(
        expert_input_rows,
        expert_norm_gain,
        selected_expert_index,
        selected_expert_weight,
        routed_gate_weight,
        routed_up_weight,
        routed_down_weight,
        common_gate_weight,
        common_up_weight,
        common_down_weight,
    )
    return (attention_output, expert_output)


def solution(mesh):
    placed = (
        P("ep", "tp"),
        P("ep", "tp"),
        P("ep", "tp"),
        P("ep", "tp"),
        P("ep", "tp"),
        P("ep", "tp"),
        P("tp"),
        P("ep", "tp"),
        P("tp"),
        P("tp", None),
        P(),
        P("ep", None),
        P(),
        P("ep", None),
        P("ep", None),
        P(("ep", "tp"), None, None),
        P(("ep", "tp"), None, None),
        P(("ep", "tp"), None, None),
        P(None, "tp"),
        P(None, "tp"),
        P("tp", None),
    )
    return jax.shard_map(
        body,
        mesh=mesh,
        in_specs=placed,
        out_specs=(P(("ep", "tp"), None), P("ep", "tp")),
        check_vma=False,
    )
```
